128 devices in a mesh: sp: 32 (over z, y, core), tp: 4 (over x).
Axes of the slice: x: 4, y: 4, z: 4, core: 2. Of those that a mesh axis runs over, the one named last changes fastest.
Arguments:
- resid: bfloat16 [8192, 2048], P(('sp', 'tp')), may hold values from -6 to 6
- query_a: bfloat16 [8192, 4, 128], P('sp', 'tp')
- key_a: bfloat16 [8192, 4, 128], P('sp', 'tp')
- value_a: bfloat16 [8192, 4, 128], P('sp', 'tp'), may hold values from -6 to 6
- query_b: bfloat16 [8192, 4, 256], P('sp', 'tp')
- key_b: bfloat16 [8192, 4, 256], P('sp', 'tp')
- value_b: bfloat16 [8192, 4, 128], P('sp', 'tp'), may hold values from -6 to 6
- lambda_a: float32 [4], P('tp'), may hold values from 0.3 to 0.8
- lambda_b: float32 [4], P('tp'), may hold values from 0.3 to 0.8
- head_gain: float32 [128], replicated, may hold values from 0.1 to 1.9
- out_weight: bfloat16 [1024, 2048], replicated, may hold values from -0.1875 to 0.1875
- norm_gain: float32 [2048], replicated, may hold values from 0.1 to 1.9
- expert_ids: int32 [8192, 4], P(('sp', 'tp')), may hold values from 0 to 127, all different within a row; in each aligned block of 64 rows (0 to 63, 64 to 127, ...) at most 4 rows name the same one
- expert_mix: float32 [8192, 4], P(('sp', 'tp')), may hold values from 0.2 to 1
- gate_experts: bfloat16 [128, 2048, 1024], P(('sp', 'tp')), may hold values from -0.125 to 0.125
- up_experts: bfloat16 [128, 2048, 1024], P(('sp', 'tp')), may hold values from -0.125 to 0.125
- down_experts: bfloat16 [128, 1024, 2048], P(('sp', 'tp')), may hold values from -0.1875 to 0.1875
- shared_gate: bfloat16 [2048, 512], replicated, may hold values from -0.125 to 0.125
- shared_up: bfloat16 [2048, 512], replicated, may hold values from -0.125 to 0.125
- shared_down: bfloat16 [512, 2048], replicated, may hold values from -0.25 to 0.25
Outputs:
- layer_out: bfloat16 [8192, 2048], P(('sp', 'tp'))
The draws below stay inside these ranges and needn't reach their ends.
Inputs may be any that keep to these rules, and one draw needn't show every extreme that they name: `expert_ids`: in each aligned block of 64 rows (the rows of one device) no expert is named more than 4 times, a bound that some block reaches.
All inputs are finite; a program needn't handle non-finite values.
Results may differ from the reference program's by a relative error of at most 0.017.
Values may be sent and summed in bfloat16 or wider, within the bound.
A program may use at most 128 MiB of HBM per device.

```python
import math
import jax
import jax.numpy as jnp
import numpy as np
from jax import lax

D = 2048
HA = 4
HB = 4
DA = 64
DB = 128
DV = 128
EFF = 1024
SFF = 512
TOPK = 4
TOK_DEV = 64
TOKENS = 8192
EXPERTS = 128
CAP = 4
N_SP = 32
N_TP = 4


def drawn_pair(key, tag, head_count, width):
    base = jax.random.fold_in(key, tag)
    query_key, key_key = jax.random.split(base)
    queries = 1.3 * jax.random.normal(query_key, (TOKENS, head_count, width), jnp.float32)
    keys = 1.3 * jax.random.normal(key_key, (TOKENS, head_count, width), jnp.float32)
    return (queries.astype(jnp.bfloat16), keys.astype(jnp.bfloat16))


def draw_query_a(key, part):
    return drawn_pair(key, 11, HA, 2 * DA)[0]


def draw_key_a(key, part):
    return drawn_pair(key, 11, HA, 2 * DA)[1]


def draw_query_b(key, part):
    return drawn_pair(key, 23, HB, 2 * DB)[0]


def draw_key_b(key, part):
    return drawn_pair(key, 23, HB, 2 * DB)[1]


def steps_of(rng, extent, pieces, smallest, high):
    def one(axis_at, parts):
        heights = jax.random.uniform(jax.random.fold_in(jax.random.fold_in(rng, 6), axis_at), (parts,), jnp.float32, smallest / len(pieces), high / len(pieces))
        return jnp.repeat(jnp.exp(heights), extent[axis_at] // parts).reshape((-1,) + (1,) * (len(extent) - axis_at - 1))

    gain = one(*pieces[0])
    for cut in pieces[1:]:
        gain = gain * one(*cut)
    return gain


def shared_out(own_key, own, number, rows, amount, top, reach, slope):
    order = jax.random.permutation(own_key, amount)
    packed, usual = load_shares(amount, rows * top, reach, slope, True), load_shares(amount, rows * top, reach, slope, False)
    places = jnp.arange(amount)

    def named(sizes, turn):
        used = int((sizes > 0).sum())
        fixed = max(1, used // 4)
        passed = fixed + (places - fixed + turn * (used - fixed)) % max(1, amount - fixed)
        return jnp.zeros((amount,), jnp.int32).at[order[jnp.where(places < fixed, places, passed)]].set(jnp.asarray(sizes, jnp.int32))

    sizes = jnp.where(number % 4 == 0, named(packed, number // 4), named(usual, number - number // 4 - 1))
    mixed = jax.random.permutation(jax.random.fold_in(own, 3), amount)
    giver, sink = mixed[0:amount // 2 * 2:2], mixed[1:amount // 2 * 2:2]
    slack = jnp.minimum(sizes[giver] - 1, reach - sizes[sink]) // 2
    slack = jnp.where((giver == order[0]) | (sink == order[0]) | (sizes[sink] == 0), 0, jnp.maximum(slack, 0))
    passed = jax.random.randint(jax.random.fold_in(own, 4), (amount // 2,), 0, 1 << 20) % (slack + 1)
    sizes = sizes.at[giver].add(-passed).at[sink].add(passed)
    items = jnp.searchsorted(jnp.cumsum(sizes), jnp.arange(rows * top), side="right").astype(jnp.int32)
    grid = items.reshape(top, rows).T
    grid = grid[jax.random.permutation(jax.random.fold_in(own, 1), rows)]
    turn = jax.random.randint(jax.random.fold_in(own, 2), (rows, 1), 0, top)
    return jnp.take_along_axis(grid, (jnp.arange(top)[None, :] + turn) % top, axis=1)


def load_shares(number_of, total, limit, skew, full):
    portions = [(1 << 20) // math.isqrt(grade ** skew) + 1 for grade in range(1, number_of + 1)]
    largest = limit if full else min(limit, max(-(-total // number_of), total * portions[0] // sum(portions)))
    least = 1 if total - largest >= number_of - 1 else 0
    counts, rest = [largest] + [least] * (number_of - 1), total - largest - least * (number_of - 1)
    while rest > 0:
        free = [i for i in range(1, number_of) if counts[i] < largest] or [i for i in range(1, number_of) if counts[i] < limit]
        whole, remaining = sum([portions[i] for i in free]), rest
        for i in free:
            addition = min(limit - counts[i], max(1, remaining * portions[i] // whole), rest)
            counts[i] = counts[i] + addition
            rest = rest - addition
    return np.array(counts)


def noise(stream_key, extent, scale, reach, pieces=(), kind=jnp.bfloat16):
    values = jax.random.normal(stream_key, extent, jnp.float32) * scale
    if len(pieces) > 0:
        values = steps_of(stream_key, extent, pieces, -0.22, 0.18) * values
    return jnp.clip(values, min=-reach, max=reach).astype(kind)


def setup_inputs(seed: int = 0) -> dict:
    seeds = jax.random.split(jax.random.key(seed), 21)
    resid = noise(seeds[0], (TOKENS, D), 1.0, 6.0, ((0, 128),))
    query_a = draw_query_a(jax.random.fold_in(seeds[20], 71), 0)
    key_a = draw_key_a(jax.random.fold_in(seeds[20], 71), 0)
    value_a = noise(seeds[3], (TOKENS, HA, DV), 1.0, 6.0, ((0, 32), (1, 4)))
    query_b = draw_query_b(jax.random.fold_in(seeds[20], 71), 0)
    key_b = draw_key_b(jax.random.fold_in(seeds[20], 71), 0)
    value_b = noise(seeds[6], (TOKENS, HB, DV), 1.0, 6.0, ((0, 32), (1, 4)))
    lambda_a = jnp.clip(0.3 + 0.5 * jax.random.uniform(seeds[7], (HA,), jnp.float32) ** steps_of(seeds[7], (HA,), ((0, 4),), -0.2, 0.2), 0.3, 0.8)
    lambda_b = jnp.clip(0.3 + 0.5 * jax.random.uniform(seeds[8], (HB,), jnp.float32) ** steps_of(seeds[8], (HB,), ((0, 4),), -0.2, 0.2), 0.3, 0.8)
    head_gain = jnp.clip(1.0 + 0.18 * jax.random.normal(seeds[9], (DV,), jnp.float32), 0.1, 1.9)
    out_weight = noise(seeds[10], ((HA + HB) * DV, D), ((HA + HB) * DV) ** -0.5, 0.1875)
    norm_gain = jnp.clip(1.0 + 0.18 * jax.random.normal(seeds[11], (D,), jnp.float32), 0.1, 1.9)
    expert_ids_keys = jax.random.split(jax.random.fold_in(seeds[12], 1), TOKENS // TOK_DEV)
    expert_ids_turns = jax.random.permutation(jax.random.fold_in(seeds[12], 3), TOKENS // TOK_DEV)
    expert_ids = jax.vmap(lambda own, number: shared_out(jax.random.fold_in(seeds[12], 2), own, number, TOK_DEV, EXPERTS, TOPK, CAP, 2))(expert_ids_keys, expert_ids_turns).reshape((TOKENS, TOPK))
    expert_mix = jnp.clip(jnp.exp(math.log(1.0) - 1.609438 * jax.random.uniform(seeds[13], (TOKENS, TOPK), jnp.float32) ** steps_of(seeds[13], (TOKENS, TOPK), ((0, 128),), -0.2, 0.2)), 0.2, 1.0)
    gate_experts = noise(seeds[14], (EXPERTS, D, EFF), D ** -0.5, 0.125, ((0, 128),))
    up_experts = noise(seeds[15], (EXPERTS, D, EFF), D ** -0.5, 0.125, ((0, 128),))
    down_experts = noise(seeds[16], (EXPERTS, EFF, D), EFF ** -0.5, 0.1875, ((0, 128),))
    shared_gate = noise(seeds[17], (D, SFF), D ** -0.5, 0.125)
    shared_up = noise(seeds[18], (D, SFF), D ** -0.5, 0.125)
    shared_down = noise(seeds[19], (SFF, D), SFF ** -0.5, 0.25)
    return dict(resid=resid, query_a=query_a, key_a=key_a, value_a=value_a, query_b=query_b, key_b=key_b, value_b=value_b, lambda_a=lambda_a, lambda_b=lambda_b, head_gain=head_gain, out_weight=out_weight, norm_gain=norm_gain, expert_ids=expert_ids, expert_mix=expert_mix, gate_experts=gate_experts, up_experts=up_experts, down_experts=down_experts, shared_gate=shared_gate, shared_up=shared_up, shared_down=shared_down)


NEG_FILL = -1e+30
EPSILON = 1e-05
HEAD_SCALE = 0.8

def group_attention(queries, keys, values, lambdas, head_gain):
    seq_total = queries.shape[0]
    map_width = queries.shape[2] // 2
    head_count = queries.shape[1]
    value_width = values.shape[2]
    block_rows = min(512, seq_total)
    key_float = keys.astype(jnp.float32)
    value_float = values.astype(jnp.float32)
    key_pos = jnp.arange(seq_total, dtype=jnp.int32)
    scaling = map_width ** (-0.5)

    def one_block(begin_row):
        query_block = lax.dynamic_slice_in_dim(queries, begin_row, block_rows, 0).astype(jnp.float32)
        query_pos = begin_row + jnp.arange(block_rows, dtype=jnp.int32)
        causal = (key_pos[None, :] <= query_pos[:, None])[None]
        results = []
        for map_index in range(2):
            low_col = map_index * map_width
            scores = jnp.einsum('qhd,khd->hqk', query_block[:, :, low_col:low_col + map_width], key_float[:, :, low_col:low_col + map_width]) * scaling
            scores = jnp.where(causal, scores, NEG_FILL)
            row_top = lax.optimization_barrier(jnp.max(scores, axis=2, keepdims=True))
            exponent = jnp.where(causal, jnp.exp(scores - row_top), 0.0)
            denoms = lax.optimization_barrier(jnp.sum(exponent, axis=2))
            rounded = lax.optimization_barrier(exponent.astype(jnp.bfloat16)).astype(jnp.float32)
            numerator = jnp.einsum('hqk,khe->qhe', rounded, value_float)
            results.append(numerator / jnp.transpose(denoms)[:, :, None])
        differ = results[0] - lambdas[None, :, None] * results[1]
        scale_rms = lax.rsqrt(lax.optimization_barrier(jnp.mean(differ * differ, axis=2, keepdims=True)) + EPSILON)
        return (differ * scale_rms * head_gain[None, None, :] * HEAD_SCALE).astype(jnp.bfloat16)
    starts = jnp.arange(seq_total // block_rows, dtype=jnp.int32) * block_rows
    outputs = lax.map(one_block, starts)
    return outputs.reshape(seq_total, head_count, value_width)

def swiglu_rows(row_set, w_gate, w_up, w_down):
    gate_val = jnp.dot(row_set, w_gate, preferred_element_type=jnp.float32)
    up_val = jnp.dot(row_set, w_up, preferred_element_type=jnp.float32)
    hidden = (jax.nn.silu(gate_val) * up_val).astype(jnp.bfloat16)
    return jnp.dot(hidden, w_down, preferred_element_type=jnp.float32)

def reference(resid, query_a, key_a, value_a, query_b, key_b, value_b, lambda_a, lambda_b, head_gain, out_weight, norm_gain, expert_ids, expert_mix, gate_experts, up_experts, down_experts, shared_gate, shared_up, shared_down):
    seq_total = resid.shape[0]
    heads_a = group_attention(query_a, key_a, value_a, lambda_a, head_gain)
    heads_b = group_attention(query_b, key_b, value_b, lambda_b, head_gain)
    joined = jnp.concatenate([heads_a.reshape(seq_total, -1), heads_b.reshape(seq_total, -1)], axis=1)
    project = jnp.dot(joined, out_weight, preferred_element_type=jnp.float32)
    middle = (resid.astype(jnp.float32) + project).astype(jnp.bfloat16)
    middle_f = middle.astype(jnp.float32)
    normed = (middle_f * lax.rsqrt(lax.optimization_barrier(jnp.mean(middle_f * middle_f, axis=1, keepdims=True)) + EPSILON) * norm_gain[None, :]).astype(jnp.bfloat16)
    shared = swiglu_rows(normed, shared_gate, shared_up, shared_down)
    top_count = expert_ids.shape[1]
    flat_ids = expert_ids.reshape(-1).astype(jnp.int32)
    flat_mix = expert_mix.reshape(-1)
    expert_count = gate_experts.shape[0]
    sorted_pairs = jnp.argsort(flat_ids, stable=True).astype(jnp.int32)
    load_counts = lax.optimization_barrier(jnp.sum((flat_ids[:, None] == jnp.arange(expert_count, dtype=jnp.int32)[None, :]).astype(jnp.int32), axis=0))
    offsets = (jnp.cumsum(load_counts) - load_counts).astype(jnp.int32)
    most_rows = N_SP * N_TP * CAP
    padded_pairs = jnp.concatenate([sorted_pairs, jnp.zeros((most_rows,), jnp.int32)])

    def one_expert(routed, inputs):
        expert_index, w_gate, w_up, w_down = inputs
        picked = lax.dynamic_slice_in_dim(padded_pairs, offsets[expert_index], most_rows, 0)
        is_valid = jnp.arange(most_rows, dtype=jnp.int32) < load_counts[expert_index]
        token_rows = (picked // top_count).astype(jnp.int32)
        result = swiglu_rows(normed[token_rows], w_gate, w_up, w_down)
        result = lax.optimization_barrier(result.astype(jnp.bfloat16)).astype(jnp.float32)
        weights = jnp.where(is_valid, flat_mix[picked], 0.0)
        return (routed.at[token_rows].add(result * weights[:, None]), None)
    routed = lax.scan(one_expert, jnp.zeros((seq_total, D), jnp.float32), (jnp.arange(expert_count, dtype=jnp.int32), gate_experts, up_experts, down_experts))[0]
    return (middle_f + shared + routed).astype(jnp.bfloat16)
```

```python
import functools
import math

import jax
import jax.numpy as jnp
from jax import lax
from jax.experimental import pallas as pl
from jax.experimental.pallas import tpu as pltpu
from jax.sharding import PartitionSpec as P

EPSILON = 1e-05
HEAD_SCALE = 0.8
LOG2E = 1.4426950408889634
NEG = -1e30
BF16 = jnp.bfloat16
F32 = jnp.float32


def dot_nt(a, b):
    return lax.dot_general(a, b, (((1,), (1,)), ((), ())), preferred_element_type=F32)


def attention_kernel(q_ref, kv_ref, lam_ref, gain_ref, out_ref, acc, top):
    me = lax.axis_index("sp")
    chip = me // 2
    rows = q_ref.shape[0]
    ones = jnp.ones((8, 2 * rows), BF16)
    scale_a = LOG2E * 64**-0.5
    scale_b = LOG2E * 128**-0.5

    def chunk(c, masked, first):
        piece = [kv_ref.at[2 * c], kv_ref.at[2 * c + 1]]
        if masked:
            key_pos = lax.broadcasted_iota(jnp.int32, (2 * rows, rows), 0)
            query_pos = lax.broadcasted_iota(jnp.int32, (2 * rows, rows), 1) + (me % 2) * rows
            keep = key_pos <= query_pos
        for head in range(2):
            vt = jnp.concatenate(
                [p[head * 128 : head * 128 + 128, 384:640] for p in piece], axis=1
            )
            vt = jnp.concatenate([vt, ones], axis=0)
            for m in range(2):
                h = head * 2 + m
                lo = [0, 0, 128, 256][h]
                keys = jnp.concatenate([p[:, lo : lo + 128] for p in piece], axis=0)
                s = dot_nt(keys, q_ref[:, h * 128 : h * 128 + 128])
                s = s * (scale_a if head == 0 else scale_b)
                if masked:
                    s = jnp.where(keep, s, NEG)
                best = jnp.max(s, axis=0, keepdims=True)
                if not first:
                    old = top[h : h + 1, :]
                    best = jnp.maximum(best, old)
                p = jnp.exp2(s - best).astype(BF16)
                add = jnp.dot(vt, p, preferred_element_type=F32)
                if first:
                    acc[h] = add
                else:
                    acc[h] = acc[h] * jnp.exp2(old - best) + add
                top[h : h + 1, :] = best

    chunk(chip, True, True)

    def body(c, carry):
        chunk(c, False, False)
        return carry

    lax.fori_loop(0, chip, body, 0)
    for head in range(2):
        first = acc[2 * head]
        second = acc[2 * head + 1]
        one = first[0:128] / first[128:129]
        two = second[0:128] / second[128:129]
        differ = one - lam_ref[head] * two
        scale = lax.rsqrt(jnp.mean(differ * differ, axis=0, keepdims=True) + EPSILON)
        heads = differ * scale
        out_ref[:, head * 128 : head * 128 + 128] = (
            heads.T * gain_ref[...] * HEAD_SCALE
        ).astype(BF16)


def attention(q, kv, lam, gain):
    rows = q.shape[0]
    return pl.pallas_call(
        attention_kernel,
        out_shape=jax.ShapeDtypeStruct((rows, 256), BF16),
        in_specs=[
            pl.BlockSpec(memory_space=pltpu.VMEM),
            pl.BlockSpec(memory_space=pltpu.VMEM),
            pl.BlockSpec(memory_space=pltpu.SMEM),
            pl.BlockSpec(memory_space=pltpu.VMEM),
        ],
        out_specs=pl.BlockSpec(memory_space=pltpu.VMEM),
        scratch_shapes=[
            pltpu.VMEM((4, 136, rows), F32),
            pltpu.VMEM((8, rows), F32),
        ],
        compiler_params=pltpu.CompilerParams(vmem_limit_bytes=48 * 1024 * 1024),
    )(q, kv, lam, gain)


def swiglu_rows(row_set, w_gate, w_up, w_down):
    gate_val = jnp.dot(row_set, w_gate, preferred_element_type=F32)
    up_val = jnp.dot(row_set, w_up, preferred_element_type=F32)
    hidden = (jax.nn.silu(gate_val) * up_val).astype(BF16)
    return jnp.dot(hidden, w_down, preferred_element_type=F32)


def slot_matrices(expert_ids, expert_mix, experts, capacity):
    tokens, top_count = expert_ids.shape
    named = jnp.sum(
        (expert_ids[:, :, None] == jnp.arange(experts, dtype=jnp.int32)).astype(F32), axis=1
    )
    mix = jnp.sum(
        jnp.where(
            expert_ids[:, :, None] == jnp.arange(experts, dtype=jnp.int32),
            expert_mix[:, :, None],
            0.0,
        ),
        axis=1,
    )
    before = jnp.tril(jnp.ones((tokens, tokens), F32), -1)
    rank = jnp.dot(before, named, preferred_element_type=F32)
    slot = jnp.arange(capacity, dtype=F32)
    hit = (rank[:, :, None] == slot) & (named[:, :, None] > 0)
    fill = hit.astype(BF16).reshape(tokens, experts * capacity)
    weight = jnp.where(hit, mix[:, :, None], 0.0).reshape(tokens, experts * capacity)
    return fill, weight


def per_device(
    resid,
    query_a,
    key_a,
    value_a,
    query_b,
    key_b,
    value_b,
    lambda_a,
    lambda_b,
    head_gain,
    out_weight,
    norm_gain,
    expert_ids,
    expert_mix,
    gate_experts,
    up_experts,
    down_experts,
    shared_gate,
    shared_up,
    shared_down,
):
    rows = query_a.shape[0]
    sp_count = lax.axis_size("sp")
    tp_count = lax.axis_size("tp")
    experts = sp_count * tp_count
    tok_dev, width = resid.shape
    capacity = 4
    qa = query_a[:, 0]
    zero = jnp.zeros((rows, 64), BF16)
    q = jnp.concatenate([qa[:, :64], zero, zero, qa[:, 64:], query_b[:, 0]], axis=1)
    piece = jnp.concatenate(
        [
            key_a[:, 0],
            key_b[:, 0],
            jnp.concatenate([value_a[:, 0].T, value_b[:, 0].T], axis=0),
        ],
        axis=1,
    )
    kv = lax.all_gather(piece, "sp", axis=0, tiled=False)
    lam = jnp.concatenate([lambda_a, lambda_b])
    heads = attention(q, kv, lam, head_gain[None, :])
    back = lax.all_to_all(
        heads.reshape(tp_count, tok_dev, 256), "tp", split_axis=0, concat_axis=0, tiled=True
    )
    joined = jnp.concatenate(
        [back[:, :, :128].transpose(1, 0, 2).reshape(tok_dev, -1),
         back[:, :, 128:].transpose(1, 0, 2).reshape(tok_dev, -1)], axis=1)
    project = jnp.dot(joined, out_weight, preferred_element_type=F32)
    middle = (resid.astype(F32) + project).astype(BF16)
    middle_f = middle.astype(F32)
    normed = (
        middle_f
        * lax.rsqrt(jnp.mean(middle_f * middle_f, axis=1, keepdims=True) + EPSILON)
        * norm_gain[None, :]
    ).astype(BF16)
    shared = swiglu_rows(normed, shared_gate, shared_up, shared_down)
    fill, weight = slot_matrices(expert_ids, expert_mix, experts, capacity)
    send = jnp.dot(fill.T, normed, preferred_element_type=F32).astype(BF16)
    arrived = lax.all_to_all(send, ("sp", "tp"), split_axis=0, concat_axis=0, tiled=True)
    result = swiglu_rows(arrived, gate_experts[0], up_experts[0], down_experts[0]).astype(BF16)
    returned = lax.all_to_all(result, ("sp", "tp"), split_axis=0, concat_axis=0, tiled=True)
    high = weight.astype(BF16)
    low = (weight - high.astype(F32)).astype(BF16)
    routed = jnp.dot(high, returned, preferred_element_type=F32) + jnp.dot(
        low, returned, preferred_element_type=F32
    )
    return (middle_f + shared + routed).astype(BF16)


def solution(mesh):
    in_specs = (
        P(("sp", "tp"), None),
        P("sp", "tp", None),
        P("sp", "tp", None),
        P("sp", "tp", None),
        P("sp", "tp", None),
        P("sp", "tp", None),
        P("sp", "tp", None),
        P("tp"),
        P("tp"),
        P(),
        P(),
        P(),
        P(("sp", "tp"), None),
        P(("sp", "tp"), None),
        P(("sp", "tp"), None, None),
        P(("sp", "tp"), None, None),
        P(("sp", "tp"), None, None),
        P(),
        P(),
        P(),
    )
    return jax.shard_map(
        per_device,
        mesh=mesh,
        in_specs=in_specs,
        out_specs=P(("sp", "tp"), None),
        check_vma=False,
    )
```

```python
import functools
import math

import jax
import jax.numpy as jnp
from jax import lax
from jax.experimental import pallas as pl
from jax.experimental.pallas import tpu as pltpu
from jax.sharding import PartitionSpec as P

EPSILON = 1e-05
HEAD_SCALE = 0.8
LOG2E = 1.4426950408889634
NEG = -1e30
BF16 = jnp.bfloat16
F32 = jnp.float32


def dot_nt(a, b):
    return lax.dot_general(a, b, (((1,), (1,)), ((), ())), preferred_element_type=F32)


MESH = pl.DeviceIdType.MESH
SIDE = 4


def attention_kernel(
    q_ref, own_ref, lam_ref, gain_ref, out_ref, kv, heads, acc, top, send_sem, half_sem, pair_sem, tp_send, tp_recv
):
    sp = lax.axis_index("sp")
    tp = lax.axis_index("tp")
    core = sp % 2
    chip = sp // 2
    z = chip // SIDE
    y = chip % SIDE
    rows = q_ref.shape[0]
    half = rows // 2
    ones = jnp.ones((8, 2 * rows), BF16)
    scale_a = LOG2E * 64**-0.5
    scale_b = LOG2E * 128**-0.5

    def at(zz, yy, cc):
        return ((zz % SIDE) * SIDE + yy % SIDE) * 2 + cc

    def neighbour(dim, step):
        return (at(z + step, y, core), tp) if dim == 0 else (at(z, y + step, core), tp)

    partner = (at(z, y, 1 - core), tp)
    barrier = pltpu.get_barrier_semaphore()
    peers = [neighbour(d, s) for d in (0, 1) for s in (1, 3)] + [partner]
    peers += [(sp, (tp + k) % 4) for k in (1, 2, 3)]
    for peer in peers:
        pl.semaphore_signal(barrier, inc=1, device_id=peer, device_id_type=MESH)
    pl.semaphore_wait(barrier, len(peers))

    started = []

    def dims(h):
        return (1, 0) if h == 0 else (0, 1)

    def piece_of(h, o1, o2):
        return at(z - o2, y - o1, core) if h == 0 else at(z - o1, y - o2, core)

    def half_send(h, o1, o2, along, step, part=None):
        dim = dims(h)[along]
        new = [o1, o2]
        new[along] = (new[along] + step) % SIDE
        lo, size = (h * half, half) if part is None else (h * half + part * half // 2, half // 2)
        p = piece_of(h, o1, o2)
        own = o1 == 0 and o2 == 0
        source = own_ref.at[pl.ds(lo, size)] if own else kv.at[p, pl.ds(lo, size)]
        copy = pltpu.make_async_remote_copy(
            src_ref=source,
            dst_ref=kv.at[p, pl.ds(lo, size)],
            send_sem=send_sem.at[len(started)],
            recv_sem=half_sem.at[h * 16 + new[0] * 4 + new[1]],
            device_id=neighbour(dim, step),
            device_id_type=MESH,
        )
        copy.start()
        started.append(copy)

    def half_wait(h, o1, o2):
        p = piece_of(h, o1, o2)
        pltpu.make_async_copy(
            kv.at[p, pl.ds(h * half, half)],
            kv.at[p, pl.ds(h * half, half)],
            half_sem.at[h * 16 + o1 * 4 + o2],
        ).wait()

    def spread(h, o1, o2, along):
        o = (o1, o2)[along]
        if o == 0:
            half_send(h, o1, o2, along, 1)
            half_send(h, o1, o2, along, 3)
        elif o == 1:
            half_send(h, o1, o2, along, 1, 0)
        elif o == 3:
            half_send(h, o1, o2, along, 3, 1)

    def arrive(h, o1, o2):
        half_wait(h, o1, o2)
        if o2 == 0:
            spread(h, o1, o2, 0)
        spread(h, o1, o2, 1)

    def pair_send(a, b):
        p = at(z - a, y - b, core)
        copy = pltpu.make_async_remote_copy(
            src_ref=own_ref if (a, b) == (0, 0) else kv.at[p],
            dst_ref=kv.at[p],
            send_sem=send_sem.at[len(started)],
            recv_sem=pair_sem.at[a * 4 + b],
            device_id=partner,
            device_id_type=MESH,
        )
        copy.start()
        started.append(copy)

    def chunk(c, masked, first):
        piece = [kv.at[2 * c], kv.at[2 * c + 1]]
        if masked:
            key_pos = lax.broadcasted_iota(jnp.int32, (2 * rows, rows), 0)
            query_pos = lax.broadcasted_iota(jnp.int32, (2 * rows, rows), 1) + core * rows
            keep = key_pos <= query_pos
        for head in range(2):
            vt = jnp.concatenate(
                [p[head * 128 : head * 128 + 128, 384:640] for p in piece], axis=1
            )
            vt = jnp.concatenate([vt, ones], axis=0)
            for m in range(2):
                h = head * 2 + m
                lo = [0, 0, 128, 256][h]
                keys = jnp.concatenate([p[:, lo : lo + 128] for p in piece], axis=0)
                s = dot_nt(keys, q_ref[:, h * 128 : h * 128 + 128])
                s = s * (scale_a if head == 0 else scale_b)
                if masked:
                    s = jnp.where(keep, s, NEG)
                best = jnp.max(s, axis=0, keepdims=True)
                if not first:
                    old = top[h : h + 1, :]
                    best = jnp.maximum(best, old)
                p = jnp.exp2(s - best).astype(BF16)
                add = jnp.dot(vt, p, preferred_element_type=F32)
                if first:
                    acc[h] = add
                else:
                    acc[h] = acc[h] * jnp.exp2(old - best) + add
                top[h : h + 1, :] = best

    def chunks(offsets):
        code = 0
        for k, (a, b) in enumerate(offsets):
            code += (a * 4 + b) * 16**k

        def body(k, left):
            o = left % 16
            a = o // 4
            b = o % 4
            p = at(z - a, y - b, 1 - core)
            pltpu.make_async_copy(kv.at[p], kv.at[p], pair_sem.at[o]).wait()
            c = p // 2

            @pl.when(c < chip)
            def _():
                chunk(c, False, False)

            return left // 16

        lax.fori_loop(0, len(offsets), body, jnp.int32(code))

    for h in range(2):
        spread(h, 0, 0, 0)
    pair_send(0, 0)
    for h in range(2):
        spread(h, 0, 0, 1)
    kv[sp] = own_ref[...]
    pltpu.make_async_copy(kv.at[sp], kv.at[sp], pair_sem.at[0]).wait()
    chunk(chip, True, True)

    for o1 in (1, 3):
        for h in range(2):
            arrive(h, o1, 0)
    for o2 in (1, 3):
        for h in range(2):
            arrive(h, 0, o2)
    near = [(0, 1), (0, 3), (1, 0), (3, 0)]
    for a, b in near:
        pair_send(a, b)
    chunks(near)
    for h in range(2):
        arrive(h, 2, 0)
    for o1 in (1, 3):
        for o2 in (1, 3):
            for h in range(2):
                arrive(h, o1, o2)
    for h in range(2):
        arrive(h, 0, 2)
    second = [(0, 2), (2, 0), (1, 1), (1, 3), (3, 1), (3, 3)]
    for a, b in second:
        pair_send(a, b)
    chunks(second[:3])
    for o2 in (1, 3):
        for h in range(2):
            arrive(h, 2, o2)
    for o1 in (1, 3):
        for h in range(2):
            arrive(h, o1, 2)
    third = [(1, 2), (3, 2), (2, 1), (2, 3)]
    for a, b in third:
        pair_send(a, b)
    chunks(second[3:])
    for h in range(2):
        arrive(h, 2, 2)
    pair_send(2, 2)
    chunks(third + [(2, 2)])

    for head in range(2):
        first = acc[2 * head]
        second = acc[2 * head + 1]
        one = first[0:128] / first[128:129]
        two = second[0:128] / second[128:129]
        differ = one - lam_ref[head] * two
        scale = lax.rsqrt(jnp.mean(differ * differ, axis=0, keepdims=True) + EPSILON)
        done = (differ * scale).T * gain_ref[...] * HEAD_SCALE
        heads[:, :, head * 128 : head * 128 + 128] = done.astype(BF16).reshape(4, rows // 4, 128)
    sends = []
    for k in (1, 2, 3):
        to = (tp + k) % 4
        copy = pltpu.make_async_remote_copy(
            src_ref=heads.at[to],
            dst_ref=out_ref.at[tp],
            send_sem=tp_send.at[k],
            recv_sem=tp_recv.at[k],
            device_id=(sp, to),
            device_id_type=MESH,
        )
        copy.start()
        sends.append(copy)
    out_ref[tp] = heads[tp]
    for copy in started:
        copy.wait_send()
    for k in (1, 2, 3):
        sends[k - 1].wait_send()
        source = (tp + 4 - k) % 4
        pltpu.make_async_copy(out_ref.at[source], out_ref.at[source], tp_recv.at[k]).wait()


def attention(q, piece, lam, gain):
    rows = q.shape[0]
    return pl.pallas_call(
        attention_kernel,
        out_shape=jax.ShapeDtypeStruct((4, rows // 4, 256), BF16),
        in_specs=[
            pl.BlockSpec(memory_space=pltpu.VMEM),
            pl.BlockSpec(memory_space=pltpu.VMEM),
            pl.BlockSpec(memory_space=pltpu.SMEM),
            pl.BlockSpec(memory_space=pltpu.VMEM),
        ],
        out_specs=pl.BlockSpec(memory_space=pltpu.VMEM),
        scratch_shapes=[
            pltpu.VMEM((32, rows, 640), BF16),
            pltpu.VMEM((4, rows // 4, 256), BF16),
            pltpu.VMEM((4, 136, rows), F32),
            pltpu.VMEM((8, rows), F32),
            pltpu.SemaphoreType.DMA((64,)),
            pltpu.SemaphoreType.DMA((32,)),
            pltpu.SemaphoreType.DMA((16,)),
            pltpu.SemaphoreType.DMA((4,)),
            pltpu.SemaphoreType.DMA((4,)),
        ],
        compiler_params=pltpu.CompilerParams(
            vmem_limit_bytes=48 * 1024 * 1024, collective_id=0, has_side_effects=True
        ),
    )(q, piece, lam, gain)


def swiglu_rows(row_set, w_gate, w_up, w_down):
    gate_val = jnp.dot(row_set, w_gate, preferred_element_type=F32)
    up_val = jnp.dot(row_set, w_up, preferred_element_type=F32)
    hidden = (jax.nn.silu(gate_val) * up_val).astype(BF16)
    return jnp.dot(hidden, w_down, preferred_element_type=F32)


def slot_matrices(expert_ids, expert_mix, experts, capacity):
    tokens, top_count = expert_ids.shape
    named = jnp.sum(
        (expert_ids[:, :, None] == jnp.arange(experts, dtype=jnp.int32)).astype(F32), axis=1
    )
    mix = jnp.sum(
        jnp.where(
            expert_ids[:, :, None] == jnp.arange(experts, dtype=jnp.int32),
            expert_mix[:, :, None],
            0.0,
        ),
        axis=1,
    )
    before = jnp.tril(jnp.ones((tokens, tokens), F32), -1)
    rank = jnp.dot(before, named, preferred_element_type=F32)
    slot = jnp.arange(capacity, dtype=F32)
    hit = (rank[:, :, None] == slot) & (named[:, :, None] > 0)
    fill = hit.astype(BF16).reshape(tokens, experts * capacity)
    weight = jnp.where(hit, mix[:, :, None], 0.0).reshape(tokens, experts * capacity)
    return fill, weight


def per_device(
    resid,
    query_a,
    key_a,
    value_a,
    query_b,
    key_b,
    value_b,
    lambda_a,
    lambda_b,
    head_gain,
    out_weight,
    norm_gain,
    expert_ids,
    expert_mix,
    gate_experts,
    up_experts,
    down_experts,
    shared_gate,
    shared_up,
    shared_down,
):
    rows = query_a.shape[0]
    sp_count = lax.axis_size("sp")
    tp_count = lax.axis_size("tp")
    experts = sp_count * tp_count
    tok_dev, width = resid.shape
    capacity = 4
    qa = query_a[:, 0]
    zero = jnp.zeros((rows, 64), BF16)
    q = jnp.concatenate([qa[:, :64], zero, zero, qa[:, 64:], query_b[:, 0]], axis=1)
    piece = jnp.concatenate(
        [
            key_a[:, 0],
            key_b[:, 0],
            jnp.concatenate([value_a[:, 0].T, value_b[:, 0].T], axis=0),
        ],
        axis=1,
    )
    lam = jnp.concatenate([lambda_a, lambda_b])
    back = attention(q, piece, lam, head_gain[None, :])
    joined = jnp.concatenate(
        [back[:, :, :128].transpose(1, 0, 2).reshape(tok_dev, -1),
         back[:, :, 128:].transpose(1, 0, 2).reshape(tok_dev, -1)], axis=1)
    project = jnp.dot(joined, out_weight, preferred_element_type=F32)
    middle = (resid.astype(F32) + project).astype(BF16)
    middle_f = middle.astype(F32)
    normed = (
        middle_f
        * lax.rsqrt(jnp.mean(middle_f * middle_f, axis=1, keepdims=True) + EPSILON)
        * norm_gain[None, :]
    ).astype(BF16)
    shared = swiglu_rows(normed, shared_gate, shared_up, shared_down)
    fill, weight = slot_matrices(expert_ids, expert_mix, experts, capacity)
    send = jnp.dot(fill.T, normed, preferred_element_type=F32).astype(BF16)
    arrived = lax.all_to_all(send, ("sp", "tp"), split_axis=0, concat_axis=0, tiled=True)
    result = swiglu_rows(arrived, gate_experts[0], up_experts[0], down_experts[0]).astype(BF16)
    returned = lax.all_to_all(result, ("sp", "tp"), split_axis=0, concat_axis=0, tiled=True)
    high = weight.astype(BF16)
    low = (weight - high.astype(F32)).astype(BF16)
    routed = jnp.dot(high, returned, preferred_element_type=F32) + jnp.dot(
        low, returned, preferred_element_type=F32
    )
    return (middle_f + shared + routed).astype(BF16)


def solution(mesh):
    in_specs = (
        P(("sp", "tp"), None),
        P("sp", "tp", None),
        P("sp", "tp", None),
        P("sp", "tp", None),
        P("sp", "tp", None),
        P("sp", "tp", None),
        P("sp", "tp", None),
        P("tp"),
        P("tp"),
        P(),
        P(),
        P(),
        P(("sp", "tp"), None),
        P(("sp", "tp"), None),
        P(("sp", "tp"), None, None),
        P(("sp", "tp"), None, None),
        P(("sp", "tp"), None, None),
        P(),
        P(),
        P(),
    )
    return jax.shard_map(
        per_device,
        mesh=mesh,
        in_specs=in_specs,
        out_specs=P(("sp", "tp"), None),
        check_vma=False,
    )
```

```python
import itertools

import jax
import jax.numpy as jnp
import numpy as np
from jax import lax
from jax.experimental import pallas as pl
from jax.experimental.pallas import tpu as pltpu
from jax.sharding import PartitionSpec as P

EPSILON = 1e-05
HEAD_SCALE = 0.8
LOG2E = 1.4426950408889634
NEG = -1e30
BF16 = jnp.bfloat16
F32 = jnp.float32


def dot_nt(a, b):
    return lax.dot_general(a, b, (((1,), (1,)), ((), ())), preferred_element_type=F32)


MESH = pl.DeviceIdType.MESH
SIDE = 4


def flows():
    every = [(a, b, c) for a in range(SIDE) for b in range(SIDE) for c in range(SIDE)]
    order, groups = [], []
    for mask in itertools.product((0, 1), repeat=3):
        if any(mask):
            members = [o for o in every if tuple(int(v == 2) for v in o) == mask]
            groups.append((mask, len(order), len(order) + len(members)))
            order += [o + (1,) for o in members]
    far = [o for o in every if 2 in o]
    near = [o for o in every if 2 not in o]
    order += [o + (1,) for o in near]
    order += [o + (0,) for o in far]
    order += [o + (0,) for o in near if any(o)] + [(0, 0, 0, 0)]
    return order, groups


ORDER, GROUPS = flows()
RELAYED = GROUPS[-1][2]
FAR_END = 64 + RELAYED


def layer_kernel(
    q_ref,
    own_ref,
    lam_ref,
    gain_ref,
    resid_ref,
    norm_ref,
    ids_ref,
    mix_ref,
    table_ref,
    wo_hbm,
    wg_hbm,
    wu_hbm,
    wd_hbm,
    sg_hbm,
    su_hbm,
    sd_hbm,
    out_ref,
    kv,
    heads,
    back,
    acc,
    top,
    wo,
    wg,
    wu,
    wd,
    sg,
    su,
    sd,
    fill,
    combine,
    perm,
    middle,
    shared,
    send,
    recv,
    res,
    ret,
    relay_out,
    relay_back,
    xs,
    hs,
    rs,
    routed,
    send_sem,
    half_sem,
    pair_sem,
    tp_send,
    tp_recv,
    load_sem,
    a2a_send,
    a2a_recv,
    relay_recv,
):
    sp = lax.axis_index("sp")
    tp = lax.axis_index("tp")
    core = sp % 2
    chip = sp // 2
    z = chip // SIDE
    y = chip % SIDE
    rows = q_ref.shape[0]
    half = rows // 2
    ones = jnp.ones((8, 2 * rows), BF16)
    scale_a = LOG2E * 64**-0.5
    scale_b = LOG2E * 128**-0.5

    def at(zz, yy, cc):
        return ((zz % SIDE) * SIDE + yy % SIDE) * 2 + cc

    def neighbour(dim, step):
        return (at(z + step, y, core), tp) if dim == 0 else (at(z, y + step, core), tp)

    partner = (at(z, y, 1 - core), tp)
    loads = [
        pltpu.make_async_copy(source, target, load_sem.at[k])
        for k, (source, target) in enumerate(
            [(wo_hbm, wo), (sg_hbm, sg), (su_hbm, su), (sd_hbm, sd), (wg_hbm, wg), (wu_hbm, wu), (wd_hbm, wd)]
        )
    ]
    for load in loads:
        load.start()
    me = sp * 4 + tp
    barrier = pltpu.get_barrier_semaphore()

    def greet(k, carry):
        other = (me + k) % 128
        pl.semaphore_signal(
            barrier, inc=1, device_id=(other // 4, other % 4), device_id_type=MESH
        )
        return carry

    lax.fori_loop(1, 128, greet, 0)
    pl.semaphore_wait(barrier, 127)

    started = []

    def dims(h):
        return (1, 0) if h == 0 else (0, 1)

    def piece_of(h, o1, o2):
        return at(z - o2, y - o1, core) if h == 0 else at(z - o1, y - o2, core)

    def half_send(h, o1, o2, along, step, part=None):
        dim = dims(h)[along]
        new = [o1, o2]
        new[along] = (new[along] + step) % SIDE
        lo, size = (h * half, half) if part is None else (h * half + part * half // 2, half // 2)
        p = piece_of(h, o1, o2)
        own = o1 == 0 and o2 == 0
        source = own_ref.at[pl.ds(lo, size)] if own else kv.at[p, pl.ds(lo, size)]
        copy = pltpu.make_async_remote_copy(
            src_ref=source,
            dst_ref=kv.at[p, pl.ds(lo, size)],
            send_sem=send_sem.at[len(started)],
            recv_sem=half_sem.at[h * 16 + new[0] * 4 + new[1]],
            device_id=neighbour(dim, step),
            device_id_type=MESH,
        )
        copy.start()
        started.append(copy)

    def half_wait(h, o1, o2):
        p = piece_of(h, o1, o2)
        pltpu.make_async_copy(
            kv.at[p, pl.ds(h * half, half)],
            kv.at[p, pl.ds(h * half, half)],
            half_sem.at[h * 16 + o1 * 4 + o2],
        ).wait()

    def spread(h, o1, o2, along):
        o = (o1, o2)[along]
        if o == 0:
            half_send(h, o1, o2, along, 1)
            half_send(h, o1, o2, along, 3)
        elif o == 1:
            half_send(h, o1, o2, along, 1, 0)
        elif o == 3:
            half_send(h, o1, o2, along, 3, 1)

    def arrive(h, o1, o2):
        half_wait(h, o1, o2)
        if o2 == 0:
            spread(h, o1, o2, 0)
        spread(h, o1, o2, 1)

    def pair_send(a, b):
        p = at(z - a, y - b, core)
        copy = pltpu.make_async_remote_copy(
            src_ref=own_ref if (a, b) == (0, 0) else kv.at[p],
            dst_ref=kv.at[p],
            send_sem=send_sem.at[len(started)],
            recv_sem=pair_sem.at[a * 4 + b],
            device_id=partner,
            device_id_type=MESH,
        )
        copy.start()
        started.append(copy)

    def chunk(c, masked, first):
        piece = [kv.at[2 * c], kv.at[2 * c + 1]]
        if masked:
            key_pos = lax.broadcasted_iota(jnp.int32, (2 * rows, rows), 0)
            query_pos = lax.broadcasted_iota(jnp.int32, (2 * rows, rows), 1) + core * rows
            keep = key_pos <= query_pos
        for head in range(2):
            vt = jnp.concatenate(
                [p[head * 128 : head * 128 + 128, 384:640] for p in piece], axis=1
            )
            vt = jnp.concatenate([vt, ones], axis=0)
            for m in range(2):
                h = head * 2 + m
                lo = [0, 0, 128, 256][h]
                keys = jnp.concatenate([p[:, lo : lo + 128] for p in piece], axis=0)
                s = dot_nt(keys, q_ref[:, h * 128 : h * 128 + 128])
                s = s * (scale_a if head == 0 else scale_b)
                if masked:
                    s = jnp.where(keep, s, NEG)
                best = jnp.max(s, axis=0, keepdims=True)
                if not first:
                    old = top[h : h + 1, :]
                    best = jnp.maximum(best, old)
                p = jnp.exp2(s - best).astype(BF16)
                add = jnp.dot(vt, p, preferred_element_type=F32)
                if first:
                    acc[h] = add
                else:
                    acc[h] = acc[h] * jnp.exp2(old - best) + add
                top[h : h + 1, :] = best

    def chunks(offsets):
        code = 0
        for k, (a, b) in enumerate(offsets):
            code += (a * 4 + b) * 16**k

        def body(k, left):
            o = left % 16
            a = o // 4
            b = o % 4
            p = at(z - a, y - b, 1 - core)
            pltpu.make_async_copy(kv.at[p], kv.at[p], pair_sem.at[o]).wait()
            c = p // 2

            @pl.when(c < chip)
            def _():
                chunk(c, False, False)

            return left // 16

        lax.fori_loop(0, len(offsets), body, jnp.int32(code))

    def slot_matrices():
        lane = lax.broadcasted_iota(jnp.int32, (64, 2048), 1)
        quarter = (lane // 4) % 4
        oz, oy, ox, oc = (table_ref[k : k + 1, :] for k in range(4))
        expert = at(z + oz, y + oy, (core + oc) % 2) * 4 + (tp + ox) % 4
        named = jnp.zeros((64, 2048), F32)
        mixed = jnp.zeros((64, 2048), F32)
        for k in range(4):
            same = ids_ref[:, k : k + 1] == expert
            named = named + jnp.where(same, 1.0, 0.0)
            mixed = mixed + jnp.where(same, mix_ref[:, k : k + 1], 0.0)
        before = jnp.where(
            lax.broadcasted_iota(jnp.int32, (64, 64), 1) < lax.broadcasted_iota(jnp.int32, (64, 64), 0),
            1.0,
            0.0,
        ).astype(BF16)
        rank = jnp.dot(before, named.astype(BF16), preferred_element_type=F32)
        hit = (named > 0.5) & (jnp.abs(rank - (lane % 4).astype(F32)) < 0.5)
        placed = jnp.where(hit, 1.0, 0.0)
        mixed = jnp.where(hit, mixed, 0.0)
        high = mixed.astype(BF16).astype(F32)
        low = mixed - high
        for j in range(4):
            keep = quarter == j
            combine[j * 64 : j * 64 + 64] = jnp.where(keep, high, 0.0).astype(BF16)
            combine[256 + j * 64 : 256 + j * 64 + 64] = jnp.where(keep, low, 0.0).astype(BF16)
        for k in range(8):
            cols = slice(k * 256, k * 256 + 256)
            block = jnp.concatenate(
                [jnp.where(quarter[:, cols] == j, placed[:, cols], 0.0) for j in range(4)], axis=0
            )
            fill[cols] = block.T.astype(BF16)
        a = lax.broadcasted_iota(jnp.int32, (256, 256), 0)
        b = lax.broadcasted_iota(jnp.int32, (256, 256), 1)
        perm[0] = jnp.where(b == ((a // 4) % 16) * 16 + (a // 64) * 4 + a % 4, 1.0, 0.0).astype(BF16)
        perm[1] = jnp.where(a == ((b // 4) % 16) * 16 + (b // 64) * 4 + b % 4, 1.0, 0.0).astype(BF16)

    for h in range(2):
        spread(h, 0, 0, 0)
    pair_send(0, 0)
    for h in range(2):
        spread(h, 0, 0, 1)
    kv[sp] = own_ref[...]
    pltpu.make_async_copy(kv.at[sp], kv.at[sp], pair_sem.at[0]).wait()
    chunk(chip, True, True)

    slot_matrices()

    for o1 in (1, 3):
        for h in range(2):
            arrive(h, o1, 0)
    for o2 in (1, 3):
        for h in range(2):
            arrive(h, 0, o2)
    near = [(0, 1), (0, 3), (1, 0), (3, 0)]
    for a, b in near:
        pair_send(a, b)
    chunks(near)
    for h in range(2):
        arrive(h, 2, 0)
    for o1 in (1, 3):
        for o2 in (1, 3):
            for h in range(2):
                arrive(h, o1, o2)
    for h in range(2):
        arrive(h, 0, 2)
    second = [(0, 2), (2, 0), (1, 1), (1, 3), (3, 1), (3, 3)]
    for a, b in second:
        pair_send(a, b)
    chunks(second[:3])
    for o2 in (1, 3):
        for h in range(2):
            arrive(h, 2, o2)
    for o1 in (1, 3):
        for h in range(2):
            arrive(h, o1, 2)
    third = [(1, 2), (3, 2), (2, 1), (2, 3)]
    for a, b in third:
        pair_send(a, b)
    chunks(second[3:])
    for h in range(2):
        arrive(h, 2, 2)
    pair_send(2, 2)
    chunks(third + [(2, 2)])

    for head in range(2):
        first = acc[2 * head]
        second = acc[2 * head + 1]
        one = first[0:128] / first[128:129]
        two = second[0:128] / second[128:129]
        differ = one - lam_ref[head] * two
        scale = lax.rsqrt(jnp.mean(differ * differ, axis=0, keepdims=True) + EPSILON)
        done = (differ * scale).T * gain_ref[...] * HEAD_SCALE
        heads[:, :, head * 128 : head * 128 + 128] = done.astype(BF16).reshape(4, rows // 4, 128)
    sends = []
    for k in (1, 2, 3):
        to = (tp + k) % 4
        copy = pltpu.make_async_remote_copy(
            src_ref=heads.at[to],
            dst_ref=back.at[tp],
            send_sem=tp_send.at[k],
            recv_sem=tp_recv.at[k],
            device_id=(sp, to),
            device_id_type=MESH,
        )
        copy.start()
        sends.append(copy)
    back[tp] = heads[tp]
    for load in loads:
        load.wait()
    for k in (1, 2, 3):
        source = (tp + 4 - k) % 4
        pltpu.make_async_copy(back.at[source], back.at[source], tp_recv.at[k]).wait()

    joined = jnp.concatenate(
        [back[p, :, :128] for p in range(4)] + [back[p, :, 128:] for p in range(4)], axis=1
    )

    def project(n, total):
        cols = pl.ds(pl.multiple_of(n * 256, 256), 256)
        part = jnp.dot(joined, wo[:, cols], preferred_element_type=F32)
        rounded = (resid_ref[:, cols].astype(F32) + part).astype(BF16)
        middle[:, cols] = rounded
        wide = rounded.astype(F32)
        return total + jnp.sum(wide * wide, axis=1, keepdims=True)

    total = lax.fori_loop(0, 8, project, jnp.zeros((64, 1), F32))
    scale = lax.rsqrt(total / 2048.0 + EPSILON)
    normed = (middle[...].astype(F32) * scale * norm_ref[...]).astype(BF16)
    stack = jnp.concatenate([normed[:, j * 512 : j * 512 + 512] for j in range(4)], axis=0)

    def device(o, other):
        return (at(z + o[0], y + o[1], (core + other) % 2), (tp + o[2]) % 4)

    def move(source, target, sem_out, sem_in, o, other):
        pltpu.make_async_remote_copy(
            src_ref=source,
            dst_ref=target,
            send_sem=sem_out,
            recv_sem=sem_in,
            device_id=device(o, other),
            device_id_type=MESH,
        ).start()

    def to_relays(way, source, relay):
        for g, (mask, lo, hi) in enumerate(GROUPS):
            move(
                source.at[pl.ds(lo, hi - lo)],
                relay.at[pl.ds(lo, hi - lo)],
                a2a_send.at[way * 4],
                relay_recv.at[way * 8 + g],
                [-v for v in mask],
                0,
            )

    def from_relays(way, relay, target):
        sign = 1 - 2 * way
        for g, (mask, lo, hi) in enumerate(GROUPS):
            there = relay.at[pl.ds(lo, hi - lo)]
            pltpu.make_async_copy(there, there, relay_recv.at[way * 8 + g]).wait()
            for k in range(lo, hi):
                o = [sign * v + m for v, m in zip(ORDER[k][:3], mask)]
                move(relay.at[k], target.at[k], a2a_send.at[way * 4 + 1], a2a_recv.at[way * 2], o, 1)

    def direct(way, source, target, lo, hi):
        sign = 1 - 2 * way
        for k in range(lo, hi):
            g = int(k >= 64)
            move(
                source.at[k],
                target.at[k],
                a2a_send.at[way * 4 + 2 + g],
                a2a_recv.at[way * 2 + g],
                [sign * v for v in ORDER[k][:3]],
                ORDER[k][3],
            )

    def arrived(way, target, g):
        part = target.at[pl.ds(g * 64, 64 - g)]
        pltpu.make_async_copy(part, part, a2a_recv.at[way * 2 + g]).wait()

    def fill_units(lo, hi):
        for u in range(lo, hi):
            rows_u = jnp.dot(fill[u * 256 : u * 256 + 256], stack, preferred_element_type=F32)
            send[u * 16 : u * 16 + 16] = rows_u.astype(BF16).reshape(16, 16, 512)

    fill_units(0, 4)
    to_relays(0, send, relay_out)
    direct(0, send, recv, RELAYED, 64)
    fill_units(4, 8)
    direct(0, send, recv, 64, FAR_END)
    recv[127] = send[127]

    def shared_hidden(n, carry):
        cols = pl.ds(pl.multiple_of(n * 256, 256), 256)
        gate = jnp.dot(normed, sg[:, cols], preferred_element_type=F32)
        up = jnp.dot(normed, su[:, cols], preferred_element_type=F32)
        hs[0:64, cols] = (gate * jax.nn.sigmoid(gate) * up).astype(BF16)
        return carry

    lax.fori_loop(0, 2, shared_hidden, 0)
    from_relays(0, relay_out, recv)
    direct(0, send, recv, FAR_END, 127)

    def shared_down(n, carry):
        cols = pl.ds(pl.multiple_of(n * 256, 256), 256)
        shared[:, cols] = jnp.dot(hs[0:64, 0:512], sd[:, cols], preferred_element_type=F32)
        return carry

    lax.fori_loop(0, 8, shared_down, 0)

    def expert(g):
        for u in range(4):
            s0 = (g * 4 + u) * 16
            rows_u = jnp.dot(
                perm[0], recv[s0 : s0 + 16].reshape(256, 512), preferred_element_type=F32
            ).astype(BF16)
            for j in range(4):
                xs[u * 64 : u * 64 + 64, j * 512 : j * 512 + 512] = rows_u[j * 64 : j * 64 + 64]

        def hidden(n, carry):
            cols = pl.ds(pl.multiple_of(n * 256, 256), 256)
            gate = jnp.dot(xs[...], wg[:, cols], preferred_element_type=F32)
            up = jnp.dot(xs[...], wu[:, cols], preferred_element_type=F32)
            hs[:, cols] = (gate * jax.nn.sigmoid(gate) * up).astype(BF16)
            return carry

        lax.fori_loop(0, 4, hidden, 0)

        def down(n, carry):
            cols = pl.ds(pl.multiple_of(n * 256, 256), 256)
            rs[:, cols] = jnp.dot(hs[...], wd[:, cols], preferred_element_type=F32).astype(BF16)
            return carry

        lax.fori_loop(0, 8, down, 0)
        for u in range(4):
            s0 = (g * 4 + u) * 16
            block = jnp.concatenate(
                [rs[u * 64 : u * 64 + 64, j * 512 : j * 512 + 512] for j in range(4)], axis=0
            )
            rows_u = jnp.dot(perm[1], block, preferred_element_type=F32)
            res[s0 : s0 + 16] = rows_u.astype(BF16).reshape(16, 16, 512)

    arrived(0, recv, 0)
    expert(0)
    to_relays(1, res, relay_back)
    direct(1, res, ret, RELAYED, 64)
    arrived(0, recv, 1)
    expert(1)
    ret[127] = res[127]
    direct(1, res, ret, 64, 127)
    from_relays(1, relay_back, ret)

    for g in range(2):
        arrived(1, ret, g)
        for half_cols in range(2):
            cols = slice(half_cols * 256, half_cols * 256 + 256)
            part = jnp.dot(
                combine[:, g * 1024 : g * 1024 + 1024],
                ret[g * 64 : g * 64 + 64].reshape(1024, 512)[:, cols],
                preferred_element_type=F32,
            )
            if g == 0:
                routed[:, cols] = part
            else:
                routed[:, cols] = routed[:, cols] + part
    for j in range(4):
        cols = slice(j * 512, j * 512 + 512)
        rows_j = routed[j * 64 : j * 64 + 64] + routed[256 + j * 64 : 256 + j * 64 + 64]
        out_ref[:, cols] = (middle[:, cols].astype(F32) + shared[:, cols] + rows_j).astype(BF16)

    for copy in started + sends:
        copy.wait_send()
    for way, (buffer, relay) in enumerate(((send, relay_out), (res, relay_back))):
        for k, part in enumerate(
            (
                relay.at[pl.ds(0, RELAYED)],
                relay.at[pl.ds(0, RELAYED)],
                buffer.at[pl.ds(RELAYED, 64 - RELAYED)],
                buffer.at[pl.ds(64, 63)],
            )
        ):
            pltpu.make_async_copy(part, part, a2a_send.at[way * 4 + k]).wait()


def layer(q, piece, lam, gain, resid, norm, ids, mix, weights):
    rows = q.shape[0]
    tokens, width = resid.shape
    table = np.zeros((8, 2048), np.int32)
    table[:4] = np.repeat(np.array(ORDER, np.int32).T, 16, axis=1)
    vmem = pl.BlockSpec(memory_space=pltpu.VMEM)
    smem = pl.BlockSpec(memory_space=pltpu.SMEM)
    slots = pltpu.VMEM((128, 16, 512), BF16)
    relays = pltpu.VMEM((RELAYED, 16, 512), BF16)
    return pl.pallas_call(
        layer_kernel,
        out_shape=jax.ShapeDtypeStruct((tokens, width), BF16),
        in_specs=[vmem, vmem, smem] + [vmem] * 6 + [pl.BlockSpec(memory_space=pl.ANY)] * 7,
        out_specs=vmem,
        scratch_shapes=[
            pltpu.VMEM((32, rows, 640), BF16),
            pltpu.VMEM((4, rows // 4, 256), BF16),
            pltpu.VMEM((4, rows // 4, 256), BF16),
            pltpu.VMEM((4, 136, rows), F32),
            pltpu.VMEM((8, rows), F32),
        ]
        + [pltpu.VMEM(weights[k].shape, BF16) for k in (0, 1, 2, 3, 4, 5, 6)]
        + [
            pltpu.VMEM((2048, 256), BF16),
            pltpu.VMEM((512, 2048), BF16),
            pltpu.VMEM((2, 256, 256), BF16),
            pltpu.VMEM((tokens, width), BF16),
            pltpu.VMEM((tokens, width), F32),
            slots,
            slots,
            slots,
            slots,
            relays,
            relays,
            pltpu.VMEM((256, width), BF16),
            pltpu.VMEM((256, 1024), BF16),
            pltpu.VMEM((256, width), BF16),
            pltpu.VMEM((512, 512), F32),
            pltpu.SemaphoreType.DMA((64,)),
            pltpu.SemaphoreType.DMA((32,)),
            pltpu.SemaphoreType.DMA((16,)),
            pltpu.SemaphoreType.DMA((4,)),
            pltpu.SemaphoreType.DMA((4,)),
            pltpu.SemaphoreType.DMA((7,)),
            pltpu.SemaphoreType.DMA((8,)),
            pltpu.SemaphoreType.DMA((4,)),
            pltpu.SemaphoreType.DMA((16,)),
        ],
        compiler_params=pltpu.CompilerParams(
            vmem_limit_bytes=63 * 1024 * 1024, collective_id=0, has_side_effects=True
        ),
    )(q, piece, lam, gain, resid, norm, ids, mix, jnp.asarray(table), *weights)


def per_device(
    resid,
    query_a,
    key_a,
    value_a,
    query_b,
    key_b,
    value_b,
    lambda_a,
    lambda_b,
    head_gain,
    out_weight,
    norm_gain,
    expert_ids,
    expert_mix,
    gate_experts,
    up_experts,
    down_experts,
    shared_gate,
    shared_up,
    shared_down,
):
    rows = query_a.shape[0]
    qa = query_a[:, 0]
    zero = jnp.zeros((rows, 64), BF16)
    q = jnp.concatenate([qa[:, :64], zero, zero, qa[:, 64:], query_b[:, 0]], axis=1)
    piece = jnp.concatenate(
        [
            key_a[:, 0],
            key_b[:, 0],
            jnp.concatenate([value_a[:, 0].T, value_b[:, 0].T], axis=0),
        ],
        axis=1,
    )
    lam = jnp.concatenate([lambda_a, lambda_b])
    weights = (
        out_weight,
        gate_experts[0],
        up_experts[0],
        down_experts[0],
        shared_gate,
        shared_up,
        shared_down,
    )
    return layer(
        q,
        piece,
        lam,
        head_gain[None, :],
        resid,
        norm_gain[None, :],
        expert_ids,
        expert_mix,
        weights,
    )


def solution(mesh):
    in_specs = (
        P(("sp", "tp"), None),
        P("sp", "tp", None),
        P("sp", "tp", None),
        P("sp", "tp", None),
        P("sp", "tp", None),
        P("sp", "tp", None),
        P("sp", "tp", None),
        P("tp"),
        P("tp"),
        P(),
        P(),
        P(),
        P(("sp", "tp"), None),
        P(("sp", "tp"), None),
        P(("sp", "tp"), None, None),
        P(("sp", "tp"), None, None),
        P(("sp", "tp"), None, None),
        P(),
        P(),
        P(),
    )
    return jax.shard_map(
        per_device,
        mesh=mesh,
        in_specs=in_specs,
        out_specs=P(("sp", "tp"), None),
        check_vma=False,
    )
```

```python
import itertools

import jax
import jax.numpy as jnp
import numpy as np
from jax import lax
from jax.experimental import pallas as pl
from jax.experimental.pallas import tpu as pltpu
from jax.sharding import PartitionSpec as P

EPSILON = 1e-05
HEAD_SCALE = 0.8
LOG2E = 1.4426950408889634
NEG = -1e30
BF16 = jnp.bfloat16
F32 = jnp.float32


MESH = pl.DeviceIdType.MESH
SIDE = 4


def flows():
    every = [(a, b, c) for a in range(SIDE) for b in range(SIDE) for c in range(SIDE)]
    order = [o + (1,) for o in every] + [o + (0,) for o in every if any(o)]
    return order + [(0, 0, 0, 0)]


ORDER = flows()


def layer_kernel(
    qa_ref,
    ka_ref,
    va_ref,
    qb_ref,
    kb_ref,
    vb_ref,
    la_ref,
    lb_ref,
    gain_ref,
    resid_ref,
    norm_ref,
    ids_ref,
    mix_ref,
    table_ref,
    wo_hbm,
    wg_hbm,
    wu_hbm,
    wd_hbm,
    sg_hbm,
    su_hbm,
    sd_hbm,
    out_ref,
    qt,
    kv,
    heads,
    back,
    acc,
    top,
    wo,
    wg,
    wu,
    wd,
    sg,
    su,
    sd,
    fill,
    combine,
    perm,
    middle,
    shared,
    send,
    recv,
    res,
    ret,
    xs,
    hs,
    rs,
    routed,
    send_sem,
    half_sem,
    pair_sem,
    tp_send,
    tp_recv,
    load_sem,
    a2a_send,
    a2a_recv,
):
    sp = lax.axis_index("sp")
    tp = lax.axis_index("tp")
    core = sp % 2
    chip = sp // 2
    z = chip // SIDE
    y = chip % SIDE
    rows = qa_ref.shape[0]
    half = rows // 2
    ones = jnp.ones((8, 2 * rows), BF16)
    scale_a = LOG2E * 64**-0.5
    scale_b = LOG2E * 128**-0.5

    def at(zz, yy, cc):
        return ((zz % SIDE) * SIDE + yy % SIDE) * 2 + cc

    def neighbour(dim, step):
        return (at(z + step, y, core), tp) if dim == 0 else (at(z, y + step, core), tp)

    partner = (at(z, y, 1 - core), tp)
    loads = [
        pltpu.make_async_copy(source, target, load_sem.at[k])
        for k, (source, target) in enumerate(
            [(wo_hbm, wo), (sg_hbm, sg), (su_hbm, su), (sd_hbm, sd), (wg_hbm, wg), (wu_hbm, wu), (wd_hbm, wd)]
        )
    ]
    for load in loads:
        load.start()
    me = sp * 4 + tp
    barrier = pltpu.get_barrier_semaphore()

    def greet(k, carry):
        other = (me + k) % 128
        pl.semaphore_signal(
            barrier, inc=1, device_id=(other // 4, other % 4), device_id_type=MESH
        )
        return carry

    lax.fori_loop(1, 128, greet, 0)

    turned = qa_ref[...].astype(F32).T.astype(BF16)
    nothing = jnp.zeros((64, rows), BF16)
    qt[0] = jnp.concatenate([turned[:64], nothing], axis=0)
    qt[1] = jnp.concatenate([nothing, turned[64:]], axis=0)
    qt[2] = qb_ref[:, :128].astype(F32).T.astype(BF16)
    qt[3] = qb_ref[:, 128:].astype(F32).T.astype(BF16)
    kv[sp, :, 0:128] = ka_ref[...]
    kv[sp, :, 128:384] = kb_ref[...]
    kv[sp, 0:128, 384:640] = va_ref[...].astype(F32).T.astype(BF16)
    kv[sp, 128:256, 384:640] = vb_ref[...].astype(F32).T.astype(BF16)
    pl.semaphore_wait(barrier, 127)

    started = []

    def dims(h):
        return (1, 0) if h == 0 else (0, 1)

    def piece_of(h, o1, o2):
        return at(z - o2, y - o1, core) if h == 0 else at(z - o1, y - o2, core)

    def half_send(h, o1, o2, along, step, part=None):
        dim = dims(h)[along]
        new = [o1, o2]
        new[along] = (new[along] + step) % SIDE
        lo, size = (h * half, half) if part is None else (h * half + part * half // 2, half // 2)
        p = piece_of(h, o1, o2)
        copy = pltpu.make_async_remote_copy(
            src_ref=kv.at[p, pl.ds(lo, size)],
            dst_ref=kv.at[p, pl.ds(lo, size)],
            send_sem=send_sem.at[len(started)],
            recv_sem=half_sem.at[h * 16 + new[0] * 4 + new[1]],
            device_id=neighbour(dim, step),
            device_id_type=MESH,
        )
        copy.start()
        started.append(copy)

    def half_wait(h, o1, o2):
        p = piece_of(h, o1, o2)
        pltpu.make_async_copy(
            kv.at[p, pl.ds(h * half, half)],
            kv.at[p, pl.ds(h * half, half)],
            half_sem.at[h * 16 + o1 * 4 + o2],
        ).wait()

    def spread(h, o1, o2, along):
        o = (o1, o2)[along]
        if o == 0:
            half_send(h, o1, o2, along, 1)
            half_send(h, o1, o2, along, 3)
        elif o == 1:
            half_send(h, o1, o2, along, 1, 0)
        elif o == 3:
            half_send(h, o1, o2, along, 3, 1)

    def arrive(h, o1, o2):
        half_wait(h, o1, o2)
        if o2 == 0:
            spread(h, o1, o2, 0)
        spread(h, o1, o2, 1)

    def pair_send(a, b):
        p = at(z - a, y - b, core)
        copy = pltpu.make_async_remote_copy(
            src_ref=kv.at[p],
            dst_ref=kv.at[p],
            send_sem=send_sem.at[len(started)],
            recv_sem=pair_sem.at[a * 4 + b],
            device_id=partner,
            device_id_type=MESH,
        )
        copy.start()
        started.append(copy)

    def chunk(c, masked, first):
        piece = [kv.at[2 * c], kv.at[2 * c + 1]]
        if masked:
            key_pos = lax.broadcasted_iota(jnp.int32, (2 * rows, rows), 0)
            query_pos = lax.broadcasted_iota(jnp.int32, (2 * rows, rows), 1) + core * rows
            keep = key_pos <= query_pos
        for head in range(2):
            vt = jnp.concatenate(
                [p[head * 128 : head * 128 + 128, 384:640] for p in piece], axis=1
            )
            vt = jnp.concatenate([vt, ones], axis=0)
            for m in range(2):
                h = head * 2 + m
                lo = [0, 0, 128, 256][h]
                keys = jnp.concatenate([p[:, lo : lo + 128] for p in piece], axis=0)
                s = jnp.dot(keys, qt[h], preferred_element_type=F32)
                s = s * (scale_a if head == 0 else scale_b)
                if masked:
                    s = jnp.where(keep, s, NEG)
                best = jnp.max(s, axis=0, keepdims=True)
                if not first:
                    old = top[h : h + 1, :]
                    best = jnp.maximum(best, old)
                p = jnp.exp2(s - best).astype(BF16)
                add = jnp.dot(vt, p, preferred_element_type=F32)
                if first:
                    acc[h] = add
                else:
                    acc[h] = acc[h] * jnp.exp2(old - best) + add
                top[h : h + 1, :] = best

    def chunks(offsets):
        code = 0
        for k, (a, b) in enumerate(offsets):
            code += (a * 4 + b) * 16**k

        def body(k, left):
            o = left % 16
            a = o // 4
            b = o % 4
            p = at(z - a, y - b, 1 - core)
            pltpu.make_async_copy(kv.at[p], kv.at[p], pair_sem.at[o]).wait()
            c = p // 2

            @pl.when(c < chip)
            def _():
                chunk(c, False, False)

            return left // 16

        lax.fori_loop(0, len(offsets), body, jnp.int32(code))

    def slot_matrices():
        lane = lax.broadcasted_iota(jnp.int32, (64, 2048), 1)
        quarter = (lane // 4) % 4
        oz, oy, ox, oc = (table_ref[k : k + 1, :] for k in range(4))
        expert = at(z + oz, y + oy, (core + oc) % 2) * 4 + (tp + ox) % 4
        named = jnp.zeros((64, 2048), F32)
        mixed = jnp.zeros((64, 2048), F32)
        down = lax.broadcasted_iota(jnp.int32, (64, 64), 0)
        across = lax.broadcasted_iota(jnp.int32, (64, 64), 1)

        def column(row):
            return jnp.sum(jnp.where(down == across, row, jnp.zeros_like(row)), axis=1, keepdims=True)

        for k in range(4):
            same = column(ids_ref[k : k + 1, :]) == expert
            named = named + jnp.where(same, 1.0, 0.0)
            mixed = mixed + jnp.where(same, column(mix_ref[k : k + 1, :]), 0.0)
        before = jnp.where(across < down, 1.0, 0.0).astype(BF16)
        rank = jnp.dot(before, named.astype(BF16), preferred_element_type=F32)
        hit = (named > 0.5) & (jnp.abs(rank - (lane % 4).astype(F32)) < 0.5)
        placed = jnp.where(hit, 1.0, 0.0)
        mixed = jnp.where(hit, mixed, 0.0)
        high = mixed.astype(BF16).astype(F32)
        low = mixed - high
        for j in range(4):
            keep = quarter == j
            combine[j * 64 : j * 64 + 64] = jnp.where(keep, high, 0.0).astype(BF16)
            combine[256 + j * 64 : 256 + j * 64 + 64] = jnp.where(keep, low, 0.0).astype(BF16)
        for k in range(8):
            cols = slice(k * 256, k * 256 + 256)
            block = jnp.concatenate(
                [jnp.where(quarter[:, cols] == j, placed[:, cols], 0.0) for j in range(4)], axis=0
            )
            fill[cols] = block.T.astype(BF16)
        a = lax.broadcasted_iota(jnp.int32, (256, 256), 0)
        b = lax.broadcasted_iota(jnp.int32, (256, 256), 1)
        perm[0] = jnp.where(b == ((a // 4) % 16) * 16 + (a // 64) * 4 + a % 4, 1.0, 0.0).astype(BF16)
        perm[1] = jnp.where(a == ((b // 4) % 16) * 16 + (b // 64) * 4 + b % 4, 1.0, 0.0).astype(BF16)

    for h in range(2):
        spread(h, 0, 0, 0)
    pair_send(0, 0)
    for h in range(2):
        spread(h, 0, 0, 1)
    pltpu.make_async_copy(kv.at[sp], kv.at[sp], pair_sem.at[0]).wait()
    chunk(chip, True, True)

    slot_matrices()

    for o1 in (1, 3):
        for h in range(2):
            arrive(h, o1, 0)
    for o2 in (1, 3):
        for h in range(2):
            arrive(h, 0, o2)
    near = [(0, 1), (0, 3), (1, 0), (3, 0)]
    for a, b in near:
        pair_send(a, b)
    chunks(near)
    for h in range(2):
        arrive(h, 2, 0)
    for o1 in (1, 3):
        for o2 in (1, 3):
            for h in range(2):
                arrive(h, o1, o2)
    for h in range(2):
        arrive(h, 0, 2)
    second = [(0, 2), (2, 0), (1, 1), (1, 3), (3, 1), (3, 3)]
    for a, b in second:
        pair_send(a, b)
    chunks(second[:3])
    for o2 in (1, 3):
        for h in range(2):
            arrive(h, 2, o2)
    for o1 in (1, 3):
        for h in range(2):
            arrive(h, o1, 2)
    third = [(1, 2), (3, 2), (2, 1), (2, 3)]
    for a, b in third:
        pair_send(a, b)
    chunks(second[3:])
    for h in range(2):
        arrive(h, 2, 2)
    pair_send(2, 2)
    chunks(third + [(2, 2)])

    for head in range(2):
        first = acc[2 * head]
        second = acc[2 * head + 1]
        one = first[0:128] / first[128:129]
        two = second[0:128] / second[128:129]
        differ = one - (la_ref, lb_ref)[head][...] * two
        scale = lax.rsqrt(jnp.mean(differ * differ, axis=0, keepdims=True) + EPSILON)
        done = (differ * scale).T * gain_ref[...] * HEAD_SCALE
        heads[:, :, head * 128 : head * 128 + 128] = done.astype(BF16).reshape(4, rows // 4, 128)
    sends = []
    for k in (1, 2, 3):
        to = (tp + k) % 4
        copy = pltpu.make_async_remote_copy(
            src_ref=heads.at[to],
            dst_ref=back.at[tp],
            send_sem=tp_send.at[k],
            recv_sem=tp_recv.at[k],
            device_id=(sp, to),
            device_id_type=MESH,
        )
        copy.start()
        sends.append(copy)
    back[tp] = heads[tp]
    for load in loads:
        load.wait()
    for k in (1, 2, 3):
        source = (tp + 4 - k) % 4
        pltpu.make_async_copy(back.at[source], back.at[source], tp_recv.at[k]).wait()

    joined = jnp.concatenate(
        [back[p, :, :128] for p in range(4)] + [back[p, :, 128:] for p in range(4)], axis=1
    )

    def project(n, total):
        cols = pl.ds(pl.multiple_of(n * 256, 256), 256)
        part = jnp.dot(joined, wo[:, cols], preferred_element_type=F32)
        rounded = (resid_ref[:, cols].astype(F32) + part).astype(BF16)
        middle[:, cols] = rounded
        wide = rounded.astype(F32)
        return total + jnp.sum(wide * wide, axis=1, keepdims=True)

    total = lax.fori_loop(0, 8, project, jnp.zeros((64, 1), F32))
    scale = lax.rsqrt(total / 2048.0 + EPSILON)
    normed = (middle[...].astype(F32) * scale * norm_ref[...]).astype(BF16)
    stack = jnp.concatenate([normed[:, j * 512 : j * 512 + 512] for j in range(4)], axis=0)

    def device(o, other):
        return (at(z + o[0], y + o[1], (core + other) % 2), (tp + o[2]) % 4)

    def move(source, target, sem_out, sem_in, o, other):
        pltpu.make_async_remote_copy(
            src_ref=source,
            dst_ref=target,
            send_sem=sem_out,
            recv_sem=sem_in,
            device_id=device(o, other),
            device_id_type=MESH,
        ).start()

    def direct(way, source, target, lo, hi):
        sign = 1 - 2 * way
        for k in range(lo, hi):
            g = int(k >= 64)
            move(
                source.at[k],
                target.at[k],
                a2a_send.at[way * 2 + g],
                a2a_recv.at[way * 2 + g],
                [sign * v for v in ORDER[k][:3]],
                ORDER[k][3],
            )

    def arrived(way, target, g):
        part = target.at[pl.ds(g * 64, 64 - g)]
        pltpu.make_async_copy(part, part, a2a_recv.at[way * 2 + g]).wait()

    def fill_units(lo, hi):
        for u in range(lo, hi):
            rows_u = jnp.dot(fill[u * 256 : u * 256 + 256], stack, preferred_element_type=F32)
            send[u * 16 : u * 16 + 16] = rows_u.astype(BF16).reshape(16, 16, 512)

    for u in range(8):
        fill_units(u, u + 1)
        if u > 0:
            direct(0, send, recv, u * 16 - 16, u * 16)
    direct(0, send, recv, 112, 127)
    recv[127] = send[127]

    def shared_hidden(n, carry):
        cols = pl.ds(pl.multiple_of(n * 256, 256), 256)
        gate = jnp.dot(normed, sg[:, cols], preferred_element_type=F32)
        up = jnp.dot(normed, su[:, cols], preferred_element_type=F32)
        hs[0:64, cols] = (gate * jax.nn.sigmoid(gate) * up).astype(BF16)
        return carry

    lax.fori_loop(0, 2, shared_hidden, 0)

    def shared_down(n, carry):
        cols = pl.ds(pl.multiple_of(n * 256, 256), 256)
        shared[:, cols] = jnp.dot(hs[0:64, 0:512], sd[:, cols], preferred_element_type=F32)
        return carry

    lax.fori_loop(0, 8, shared_down, 0)

    def expert(g):
        for u in range(4):
            s0 = (g * 4 + u) * 16
            rows_u = jnp.dot(
                perm[0], recv[s0 : s0 + 16].reshape(256, 512), preferred_element_type=F32
            ).astype(BF16)
            for j in range(4):
                xs[u * 64 : u * 64 + 64, j * 512 : j * 512 + 512] = rows_u[j * 64 : j * 64 + 64]

        def hidden(n, carry):
            cols = pl.ds(pl.multiple_of(n * 256, 256), 256)
            gate = jnp.dot(xs[...], wg[:, cols], preferred_element_type=F32)
            up = jnp.dot(xs[...], wu[:, cols], preferred_element_type=F32)
            hs[:, cols] = (gate * jax.nn.sigmoid(gate) * up).astype(BF16)
            return carry

        lax.fori_loop(0, 4, hidden, 0)

        def down(n, carry):
            cols = pl.ds(pl.multiple_of(n * 256, 256), 256)
            rs[:, cols] = jnp.dot(hs[...], wd[:, cols], preferred_element_type=F32).astype(BF16)
            return carry

        lax.fori_loop(0, 8, down, 0)
        for u in range(4):
            s0 = (g * 4 + u) * 16
            block = jnp.concatenate(
                [rs[u * 64 : u * 64 + 64, j * 512 : j * 512 + 512] for j in range(4)], axis=0
            )
            rows_u = jnp.dot(perm[1], block, preferred_element_type=F32)
            res[s0 : s0 + 16] = rows_u.astype(BF16).reshape(16, 16, 512)

    arrived(0, recv, 0)
    expert(0)
    direct(1, res, ret, 0, 64)
    arrived(0, recv, 1)
    expert(1)
    ret[127] = res[127]
    direct(1, res, ret, 64, 127)

    for g in range(2):
        arrived(1, ret, g)
        for half_cols in range(2):
            cols = slice(half_cols * 256, half_cols * 256 + 256)
            part = jnp.dot(
                combine[:, g * 1024 : g * 1024 + 1024],
                ret[g * 64 : g * 64 + 64].reshape(1024, 512)[:, cols],
                preferred_element_type=F32,
            )
            if g == 0:
                routed[:, cols] = part
            else:
                routed[:, cols] = routed[:, cols] + part
    for j in range(4):
        cols = slice(j * 512, j * 512 + 512)
        rows_j = routed[j * 64 : j * 64 + 64] + routed[256 + j * 64 : 256 + j * 64 + 64]
        out_ref[:, cols] = (middle[:, cols].astype(F32) + shared[:, cols] + rows_j).astype(BF16)

    for copy in started + sends:
        copy.wait_send()
    for way, buffer in enumerate((send, res)):
        for g in range(2):
            part = buffer.at[pl.ds(g * 64, 64 - g)]
            pltpu.make_async_copy(part, part, a2a_send.at[way * 2 + g]).wait()


def layer(qkv, lambdas, gain, resid, norm, ids, mix, weights):
    rows = qkv[0].shape[0]
    tokens, width = resid.shape
    table = np.zeros((8, 2048), np.int32)
    table[:4] = np.repeat(np.array(ORDER, np.int32).T, 16, axis=1)
    vmem = pl.BlockSpec(memory_space=pltpu.VMEM)
    slots = pltpu.VMEM((128, 16, 512), BF16)
    return pl.pallas_call(
        layer_kernel,
        out_shape=jax.ShapeDtypeStruct((tokens, width), BF16),
        in_specs=[vmem] * 14 + [pl.BlockSpec(memory_space=pl.ANY)] * 7,
        out_specs=vmem,
        scratch_shapes=[
            pltpu.VMEM((4, 128, rows), BF16),
            pltpu.VMEM((32, rows, 640), BF16),
            pltpu.VMEM((4, rows // 4, 256), BF16),
            pltpu.VMEM((4, rows // 4, 256), BF16),
            pltpu.VMEM((4, 136, rows), F32),
            pltpu.VMEM((8, rows), F32),
        ]
        + [pltpu.VMEM(weights[k].shape, BF16) for k in (0, 1, 2, 3, 4, 5, 6)]
        + [
            pltpu.VMEM((2048, 256), BF16),
            pltpu.VMEM((512, 2048), BF16),
            pltpu.VMEM((2, 256, 256), BF16),
            pltpu.VMEM((tokens, width), BF16),
            pltpu.VMEM((tokens, width), F32),
            slots,
            slots,
            slots,
            slots,
            pltpu.VMEM((256, width), BF16),
            pltpu.VMEM((256, 1024), BF16),
            pltpu.VMEM((256, width), BF16),
            pltpu.VMEM((512, 512), F32),
            pltpu.SemaphoreType.DMA((64,)),
            pltpu.SemaphoreType.DMA((32,)),
            pltpu.SemaphoreType.DMA((16,)),
            pltpu.SemaphoreType.DMA((4,)),
            pltpu.SemaphoreType.DMA((4,)),
            pltpu.SemaphoreType.DMA((7,)),
            pltpu.SemaphoreType.DMA((4,)),
            pltpu.SemaphoreType.DMA((4,)),
        ],
        compiler_params=pltpu.CompilerParams(
            vmem_limit_bytes=63 * 1024 * 1024, collective_id=0, has_side_effects=True
        ),
    )(*qkv, *lambdas, gain, resid, norm, ids, mix, jnp.asarray(table), *weights)


def per_device(
    resid,
    query_a,
    key_a,
    value_a,
    query_b,
    key_b,
    value_b,
    lambda_a,
    lambda_b,
    head_gain,
    out_weight,
    norm_gain,
    expert_ids,
    expert_mix,
    gate_experts,
    up_experts,
    down_experts,
    shared_gate,
    shared_up,
    shared_down,
):
    weights = (
        out_weight,
        gate_experts[0],
        up_experts[0],
        down_experts[0],
        shared_gate,
        shared_up,
        shared_down,
    )
    qkv = [a[:, 0] for a in (query_a, key_a, value_a, query_b, key_b, value_b)]
    return layer(
        qkv,
        (lambda_a[None, :], lambda_b[None, :]),
        head_gain[None, :],
        resid,
        norm_gain[None, :],
        expert_ids.T,
        expert_mix.T,
        weights,
    )


def solution(mesh):
    in_specs = (
        P(("sp", "tp"), None),
        P("sp", "tp", None),
        P("sp", "tp", None),
        P("sp", "tp", None),
        P("sp", "tp", None),
        P("sp", "tp", None),
        P("sp", "tp", None),
        P("tp"),
        P("tp"),
        P(),
        P(),
        P(),
        P(("sp", "tp"), None),
        P(("sp", "tp"), None),
        P(("sp", "tp"), None, None),
        P(("sp", "tp"), None, None),
        P(("sp", "tp"), None, None),
        P(),
        P(),
        P(),
    )
    return jax.shard_map(
        per_device,
        mesh=mesh,
        in_specs=in_specs,
        out_specs=P(("sp", "tp"), None),
        check_vma=False,
    )
```

```python
import itertools

import jax
import jax.numpy as jnp
import numpy as np
from jax import lax
from jax.experimental import pallas as pl
from jax.experimental.pallas import tpu as pltpu
from jax.sharding import PartitionSpec as P

EPSILON = 1e-05
HEAD_SCALE = 0.8
NEG = -1e30
BF16 = jnp.bfloat16
F32 = jnp.float32


MESH = pl.DeviceIdType.MESH
SIDE = 4


def flows():
    every = np.array([o for o in itertools.product(range(SIDE), range(SIDE), range(SIDE), (0, 1)) if any(o)])
    mixed = every[np.random.RandomState(1).permutation(len(every))]
    hops = np.minimum(mixed[:, :3], SIDE - mixed[:, :3]).sum(axis=1)
    mixed = mixed[np.argsort(-hops, kind="stable")]
    for part in (mixed[:64], mixed[64:]):
        part[:] = part[np.random.RandomState(2).permutation(len(part))]
    return [tuple(int(v) for v in o) for o in mixed] + [(0, 0, 0, 0)]


ORDER = flows()


def layer_kernel(
    qa_ref,
    ka_ref,
    va_ref,
    qb_ref,
    kb_ref,
    vb_ref,
    la_ref,
    lb_ref,
    gain_ref,
    resid_ref,
    norm_ref,
    ids_ref,
    mix_ref,
    table_ref,
    wo_hbm,
    wg_hbm,
    wu_hbm,
    wd_hbm,
    sg_hbm,
    su_hbm,
    sd_hbm,
    out_ref,
    qt,
    kv,
    heads,
    back,
    acc,
    top,
    wo,
    wg,
    wu,
    wd,
    sg,
    su,
    sd,
    fill,
    combine,
    perm,
    middle,
    shared,
    send,
    recv,
    res,
    ret,
    xs,
    hs,
    rs,
    routed,
    send_sem,
    half_sem,
    pair_sem,
    tp_send,
    tp_recv,
    load_sem,
    a2a_send,
    a2a_recv,
):
    sp = lax.axis_index("sp")
    tp = lax.axis_index("tp")
    core = sp % 2
    chip = sp // 2
    z = chip // SIDE
    y = chip % SIDE
    rows = qa_ref.shape[0]
    half = rows // 2
    ones = jnp.ones((8, 2 * rows), BF16)

    def at(zz, yy, cc):
        return ((zz % SIDE) * SIDE + yy % SIDE) * 2 + cc

    def neighbour(dim, step):
        return (at(z + step, y, core), tp) if dim == 0 else (at(z, y + step, core), tp)

    partner = (at(z, y, 1 - core), tp)
    loads = [
        pltpu.make_async_copy(source, target, load_sem.at[k])
        for k, (source, target) in enumerate(
            [(wo_hbm, wo), (sg_hbm, sg), (su_hbm, su), (sd_hbm, sd), (wg_hbm, wg), (wu_hbm, wu), (wd_hbm, wd)]
        )
    ]
    for load in loads:
        load.start()
    me = sp * 4 + tp
    barrier = pltpu.get_barrier_semaphore()

    def greet(k, carry):
        other = (me + k) % 128
        pl.semaphore_signal(
            barrier, inc=1, device_id=(other // 4, other % 4), device_id_type=MESH
        )
        return carry

    lax.fori_loop(1, 128, greet, 0)

    turned = qa_ref[...].astype(F32).T.astype(BF16)
    nothing = jnp.zeros((64, rows), BF16)
    qt[0] = jnp.concatenate([turned[:64], nothing], axis=0)
    qt[1] = jnp.concatenate([nothing, turned[64:]], axis=0)
    qt[2] = qb_ref[:, :128].astype(F32).T.astype(BF16)
    qt[3] = qb_ref[:, 128:].astype(F32).T.astype(BF16)
    kv[sp, :, 0:128] = ka_ref[...]
    kv[sp, :, 128:384] = kb_ref[...]
    kv[sp, 0:128, 384:640] = va_ref[...].astype(F32).T.astype(BF16)
    kv[sp, 128:256, 384:640] = vb_ref[...].astype(F32).T.astype(BF16)
    pl.semaphore_wait(barrier, 127)

    started = []

    def dims(h):
        return (1, 0) if h == 0 else (0, 1)

    def piece_of(h, o1, o2):
        return at(z - o2, y - o1, core) if h == 0 else at(z - o1, y - o2, core)

    def half_send(h, o1, o2, along, step, part=None):
        dim = dims(h)[along]
        new = [o1, o2]
        new[along] = (new[along] + step) % SIDE
        lo, size = (h * half, half) if part is None else (h * half + part * half // 2, half // 2)
        p = piece_of(h, o1, o2)
        copy = pltpu.make_async_remote_copy(
            src_ref=kv.at[p, pl.ds(lo, size)],
            dst_ref=kv.at[p, pl.ds(lo, size)],
            send_sem=send_sem.at[len(started)],
            recv_sem=half_sem.at[h * 16 + new[0] * 4 + new[1]],
            device_id=neighbour(dim, step),
            device_id_type=MESH,
        )
        copy.start()
        started.append(copy)

    def half_wait(h, o1, o2):
        p = piece_of(h, o1, o2)
        pltpu.make_async_copy(
            kv.at[p, pl.ds(h * half, half)],
            kv.at[p, pl.ds(h * half, half)],
            half_sem.at[h * 16 + o1 * 4 + o2],
        ).wait()

    def spread(h, o1, o2, along):
        o = (o1, o2)[along]
        if o == 0:
            half_send(h, o1, o2, along, 1)
            half_send(h, o1, o2, along, 3)
        elif o == 1:
            half_send(h, o1, o2, along, 1, 0)
        elif o == 3:
            half_send(h, o1, o2, along, 3, 1)

    def arrive(h, o1, o2):
        half_wait(h, o1, o2)
        if o2 == 0:
            spread(h, o1, o2, 0)
        spread(h, o1, o2, 1)

    def pair_send(a, b):
        p = at(z - a, y - b, core)
        copy = pltpu.make_async_remote_copy(
            src_ref=kv.at[p],
            dst_ref=kv.at[p],
            send_sem=send_sem.at[len(started)],
            recv_sem=pair_sem.at[a * 4 + b],
            device_id=partner,
            device_id_type=MESH,
        )
        copy.start()
        started.append(copy)

    def chunk(c, masked, first):
        piece = [kv.at[2 * c], kv.at[2 * c + 1]]
        if masked:
            key_pos = lax.broadcasted_iota(jnp.int32, (2 * rows, rows), 0)
            query_pos = lax.broadcasted_iota(jnp.int32, (2 * rows, rows), 1) + core * rows
            keep = key_pos <= query_pos
        values = [
            jnp.concatenate(
                [
                    jnp.concatenate(
                        [p[head * 128 : head * 128 + 128, 384:640] for p in piece], axis=1
                    ),
                    ones,
                ],
                axis=0,
            )
            for head in range(2)
        ]

        def scores(h):
            lo = (0, 0, 128, 256)[h]
            keys = jnp.concatenate([p[:, lo : lo + 128] for p in piece], axis=0)
            s = jnp.dot(keys, qt[h], preferred_element_type=F32)
            return jnp.where(keep, s, NEG) if masked else s

        ready = scores(0)
        for h in range(4):
            s = ready
            if h < 3:
                ready = scores(h + 1)
            scale = (64**-0.5, 64**-0.5, 128**-0.5, 128**-0.5)[h]
            best = jnp.max(s, axis=0, keepdims=True)
            if not first:
                old = top[h : h + 1, :]
                best = jnp.maximum(best, old)
            p = jnp.exp((s - best) * scale).astype(BF16)
            add = jnp.dot(values[h // 2], p, preferred_element_type=F32)
            if first:
                acc[h] = add
            else:
                acc[h] = acc[h] * jnp.exp((old - best) * scale) + add
            top[h : h + 1, :] = best

    def chunks(offsets):
        code = 0
        for k, (a, b) in enumerate(offsets):
            code += (a * 4 + b) * 16**k

        def body(k, left):
            o = left % 16
            a = o // 4
            b = o % 4
            p = at(z - a, y - b, 1 - core)
            pltpu.make_async_copy(kv.at[p], kv.at[p], pair_sem.at[o]).wait()
            c = p // 2

            @pl.when(c < chip)
            def _():
                chunk(c, False, False)

            return left // 16

        lax.fori_loop(0, len(offsets), body, jnp.int32(code))

    def slot_matrices():
        lane = lax.broadcasted_iota(jnp.int32, (64, 2048), 1)
        quarter = (lane // 4) % 4
        oz, oy, ox, oc = (table_ref[k : k + 1, :] for k in range(4))
        expert = at(z + oz, y + oy, (core + oc) % 2) * 4 + (tp + ox) % 4
        named = jnp.zeros((64, 2048), F32)
        mixed = jnp.zeros((64, 2048), F32)
        down = lax.broadcasted_iota(jnp.int32, (64, 64), 0)
        across = lax.broadcasted_iota(jnp.int32, (64, 64), 1)

        def column(row):
            return jnp.sum(jnp.where(down == across, row, jnp.zeros_like(row)), axis=1, keepdims=True)

        for k in range(4):
            same = column(ids_ref[k : k + 1, :]) == expert
            named = named + jnp.where(same, 1.0, 0.0)
            mixed = mixed + jnp.where(same, column(mix_ref[k : k + 1, :]), 0.0)
        before = jnp.where(across < down, 1.0, 0.0).astype(BF16)
        rank = jnp.dot(before, named.astype(BF16), preferred_element_type=F32)
        hit = (named > 0.5) & (jnp.abs(rank - (lane % 4).astype(F32)) < 0.5)
        placed = jnp.where(hit, 1.0, 0.0)
        mixed = jnp.where(hit, mixed, 0.0)
        high = mixed.astype(BF16).astype(F32)
        low = mixed - high
        for j in range(4):
            keep = quarter == j
            combine[j * 64 : j * 64 + 64] = jnp.where(keep, high, 0.0).astype(BF16)
            combine[256 + j * 64 : 256 + j * 64 + 64] = jnp.where(keep, low, 0.0).astype(BF16)
        for k in range(8):
            cols = slice(k * 256, k * 256 + 256)
            block = jnp.concatenate(
                [jnp.where(quarter[:, cols] == j, placed[:, cols], 0.0) for j in range(4)], axis=0
            )
            fill[cols] = block.T.astype(BF16)
        a = lax.broadcasted_iota(jnp.int32, (256, 256), 0)
        b = lax.broadcasted_iota(jnp.int32, (256, 256), 1)
        perm[0] = jnp.where(b == ((a // 4) % 16) * 16 + (a // 64) * 4 + a % 4, 1.0, 0.0).astype(BF16)
        perm[1] = jnp.where(a == ((b // 4) % 16) * 16 + (b // 64) * 4 + b % 4, 1.0, 0.0).astype(BF16)

    for h in range(2):
        spread(h, 0, 0, 0)
    pair_send(0, 0)
    for h in range(2):
        spread(h, 0, 0, 1)
    pltpu.make_async_copy(kv.at[sp], kv.at[sp], pair_sem.at[0]).wait()
    chunk(chip, True, True)

    slot_matrices()

    for o1 in (1, 3):
        for h in range(2):
            arrive(h, o1, 0)
    for o2 in (1, 3):
        for h in range(2):
            arrive(h, 0, o2)
    near = [(0, 1), (0, 3), (1, 0), (3, 0)]
    for a, b in near:
        pair_send(a, b)
    chunks(near)
    for h in range(2):
        arrive(h, 2, 0)
    for o1 in (1, 3):
        for o2 in (1, 3):
            for h in range(2):
                arrive(h, o1, o2)
    for h in range(2):
        arrive(h, 0, 2)
    second = [(0, 2), (2, 0), (1, 1), (1, 3), (3, 1), (3, 3)]
    for a, b in second:
        pair_send(a, b)
    chunks(second[:3])
    for o2 in (1, 3):
        for h in range(2):
            arrive(h, 2, o2)
    for o1 in (1, 3):
        for h in range(2):
            arrive(h, o1, 2)
    third = [(1, 2), (3, 2), (2, 1), (2, 3)]
    for a, b in third:
        pair_send(a, b)
    chunks(second[3:])
    for h in range(2):
        arrive(h, 2, 2)
    pair_send(2, 2)
    chunks(third + [(2, 2)])

    for head in range(2):
        first = acc[2 * head]
        second = acc[2 * head + 1]
        one = first[0:128] / first[128:129]
        two = second[0:128] / second[128:129]
        differ = one - (la_ref, lb_ref)[head][...] * two
        scale = lax.rsqrt(jnp.mean(differ * differ, axis=0, keepdims=True) + EPSILON)
        done = (differ * scale).T * gain_ref[...] * HEAD_SCALE
        heads[:, :, head * 128 : head * 128 + 128] = done.astype(BF16).reshape(4, rows // 4, 128)
    sends = []
    for k in (1, 2, 3):
        to = (tp + k) % 4
        copy = pltpu.make_async_remote_copy(
            src_ref=heads.at[to],
            dst_ref=back.at[tp],
            send_sem=tp_send.at[k],
            recv_sem=tp_recv.at[k],
            device_id=(sp, to),
            device_id_type=MESH,
        )
        copy.start()
        sends.append(copy)
    back[tp] = heads[tp]
    for load in loads:
        load.wait()
    for k in (1, 2, 3):
        source = (tp + 4 - k) % 4
        pltpu.make_async_copy(back.at[source], back.at[source], tp_recv.at[k]).wait()

    joined = jnp.concatenate(
        [back[p, :, :128] for p in range(4)] + [back[p, :, 128:] for p in range(4)], axis=1
    )

    def project(n, total):
        cols = pl.ds(pl.multiple_of(n * 256, 256), 256)
        part = jnp.dot(joined, wo[:, cols], preferred_element_type=F32)
        rounded = (resid_ref[:, cols].astype(F32) + part).astype(BF16)
        middle[:, cols] = rounded
        wide = rounded.astype(F32)
        return total + jnp.sum(wide * wide, axis=1, keepdims=True)

    total = lax.fori_loop(0, 8, project, jnp.zeros((64, 1), F32))
    scale = lax.rsqrt(total / 2048.0 + EPSILON)
    normed = (middle[...].astype(F32) * scale * norm_ref[...]).astype(BF16)
    stack = jnp.concatenate([normed[:, j * 512 : j * 512 + 512] for j in range(4)], axis=0)

    def device(o, other):
        return (at(z + o[0], y + o[1], (core + other) % 2), (tp + o[2]) % 4)

    def move(source, target, sem_out, sem_in, o, other):
        pltpu.make_async_remote_copy(
            src_ref=source,
            dst_ref=target,
            send_sem=sem_out,
            recv_sem=sem_in,
            device_id=device(o, other),
            device_id_type=MESH,
        ).start()

    def direct(way, source, target, lo, hi):
        sign = 1 - 2 * way
        for k in range(lo, hi):
            g = int(k >= 64)
            move(
                source.at[k],
                target.at[k],
                a2a_send.at[way * 2 + g],
                a2a_recv.at[way * 2 + g],
                [sign * v for v in ORDER[k][:3]],
                ORDER[k][3],
            )

    def arrived(way, target, g):
        part = target.at[pl.ds(g * 64, 64 - g)]
        pltpu.make_async_copy(part, part, a2a_recv.at[way * 2 + g]).wait()

    def fill_units(lo, hi):
        for u in range(lo, hi):
            rows_u = jnp.dot(fill[u * 256 : u * 256 + 256], stack, preferred_element_type=F32)
            send[u * 16 : u * 16 + 16] = rows_u.astype(BF16).reshape(16, 16, 512)

    for u in range(8):
        fill_units(u, u + 1)
        if u > 0:
            direct(0, send, recv, u * 16 - 16, u * 16)
    direct(0, send, recv, 112, 127)
    recv[127] = send[127]

    def shared_hidden(n, carry):
        cols = pl.ds(pl.multiple_of(n * 256, 256), 256)
        gate = jnp.dot(normed, sg[:, cols], preferred_element_type=F32)
        up = jnp.dot(normed, su[:, cols], preferred_element_type=F32)
        hs[0:64, cols] = (gate * jax.nn.sigmoid(gate) * up).astype(BF16)
        return carry

    lax.fori_loop(0, 2, shared_hidden, 0)

    def shared_down(n, carry):
        cols = pl.ds(pl.multiple_of(n * 256, 256), 256)
        shared[:, cols] = jnp.dot(hs[0:64, 0:512], sd[:, cols], preferred_element_type=F32)
        return carry

    lax.fori_loop(0, 8, shared_down, 0)

    def expert(g):
        for u in range(4):
            s0 = (g * 4 + u) * 16
            rows_u = jnp.dot(
                perm[0], recv[s0 : s0 + 16].reshape(256, 512), preferred_element_type=F32
            ).astype(BF16)
            for j in range(4):
                xs[u * 64 : u * 64 + 64, j * 512 : j * 512 + 512] = rows_u[j * 64 : j * 64 + 64]

        def hidden(n, carry):
            cols = pl.ds(pl.multiple_of(n * 256, 256), 256)
            gate = jnp.dot(xs[...], wg[:, cols], preferred_element_type=F32)
            up = jnp.dot(xs[...], wu[:, cols], preferred_element_type=F32)
            hs[:, cols] = (gate * jax.nn.sigmoid(gate) * up).astype(BF16)
            return carry

        lax.fori_loop(0, 4, hidden, 0)

        def down(n, carry):
            cols = pl.ds(pl.multiple_of(n * 256, 256), 256)
            rs[:, cols] = jnp.dot(hs[...], wd[:, cols], preferred_element_type=F32).astype(BF16)
            return carry

        lax.fori_loop(0, 8, down, 0)
        for u in range(4):
            s0 = (g * 4 + u) * 16
            block = jnp.concatenate(
                [rs[u * 64 : u * 64 + 64, j * 512 : j * 512 + 512] for j in range(4)], axis=0
            )
            rows_u = jnp.dot(perm[1], block, preferred_element_type=F32)
            res[s0 : s0 + 16] = rows_u.astype(BF16).reshape(16, 16, 512)

    arrived(0, recv, 0)
    expert(0)
    direct(1, res, ret, 0, 64)
    arrived(0, recv, 1)
    expert(1)
    ret[127] = res[127]
    direct(1, res, ret, 64, 127)

    for g in range(2):
        arrived(1, ret, g)
        for half_cols in range(2):
            cols = slice(half_cols * 256, half_cols * 256 + 256)
            part = jnp.dot(
                combine[:, g * 1024 : g * 1024 + 1024],
                ret[g * 64 : g * 64 + 64].reshape(1024, 512)[:, cols],
                preferred_element_type=F32,
            )
            if g == 0:
                routed[:, cols] = part
            else:
                routed[:, cols] = routed[:, cols] + part
    for j in range(4):
        cols = slice(j * 512, j * 512 + 512)
        rows_j = routed[j * 64 : j * 64 + 64] + routed[256 + j * 64 : 256 + j * 64 + 64]
        out_ref[:, cols] = (middle[:, cols].astype(F32) + shared[:, cols] + rows_j).astype(BF16)

    for copy in started + sends:
        copy.wait_send()
    for way, buffer in enumerate((send, res)):
        for g in range(2):
            part = buffer.at[pl.ds(g * 64, 64 - g)]
            pltpu.make_async_copy(part, part, a2a_send.at[way * 2 + g]).wait()


def layer(qkv, lambdas, gain, resid, norm, ids, mix, weights):
    rows = qkv[0].shape[0]
    tokens, width = resid.shape
    table = np.zeros((8, 2048), np.int32)
    table[:4] = np.repeat(np.array(ORDER, np.int32).T, 16, axis=1)
    vmem = pl.BlockSpec(memory_space=pltpu.VMEM)
    slots = pltpu.VMEM((128, 16, 512), BF16)
    return pl.pallas_call(
        layer_kernel,
        out_shape=jax.ShapeDtypeStruct((tokens, width), BF16),
        in_specs=[vmem] * 14 + [pl.BlockSpec(memory_space=pl.ANY)] * 7,
        out_specs=vmem,
        scratch_shapes=[
            pltpu.VMEM((4, 128, rows), BF16),
            pltpu.VMEM((32, rows, 640), BF16),
            pltpu.VMEM((4, rows // 4, 256), BF16),
            pltpu.VMEM((4, rows // 4, 256), BF16),
            pltpu.VMEM((4, 136, rows), F32),
            pltpu.VMEM((8, rows), F32),
        ]
        + [pltpu.VMEM(weights[k].shape, BF16) for k in (0, 1, 2, 3, 4, 5, 6)]
        + [
            pltpu.VMEM((2048, 256), BF16),
            pltpu.VMEM((512, 2048), BF16),
            pltpu.VMEM((2, 256, 256), BF16),
            pltpu.VMEM((tokens, width), BF16),
            pltpu.VMEM((tokens, width), F32),
            slots,
            slots,
            slots,
            slots,
            pltpu.VMEM((256, width), BF16),
            pltpu.VMEM((256, 1024), BF16),
            pltpu.VMEM((256, width), BF16),
            pltpu.VMEM((512, 512), F32),
            pltpu.SemaphoreType.DMA((64,)),
            pltpu.SemaphoreType.DMA((32,)),
            pltpu.SemaphoreType.DMA((16,)),
            pltpu.SemaphoreType.DMA((4,)),
            pltpu.SemaphoreType.DMA((4,)),
            pltpu.SemaphoreType.DMA((7,)),
            pltpu.SemaphoreType.DMA((4,)),
            pltpu.SemaphoreType.DMA((4,)),
        ],
        compiler_params=pltpu.CompilerParams(
            vmem_limit_bytes=63 * 1024 * 1024, collective_id=0, has_side_effects=True
        ),
    )(*qkv, *lambdas, gain, resid, norm, ids, mix, jnp.asarray(table), *weights)


def per_device(
    resid,
    query_a,
    key_a,
    value_a,
    query_b,
    key_b,
    value_b,
    lambda_a,
    lambda_b,
    head_gain,
    out_weight,
    norm_gain,
    expert_ids,
    expert_mix,
    gate_experts,
    up_experts,
    down_experts,
    shared_gate,
    shared_up,
    shared_down,
):
    weights = (
        out_weight,
        gate_experts[0],
        up_experts[0],
        down_experts[0],
        shared_gate,
        shared_up,
        shared_down,
    )
    qkv = [a[:, 0] for a in (query_a, key_a, value_a, query_b, key_b, value_b)]
    return layer(
        qkv,
        (lambda_a[None, :], lambda_b[None, :]),
        head_gain[None, :],
        resid,
        norm_gain[None, :],
        expert_ids.T,
        expert_mix.T,
        weights,
    )


def solution(mesh):
    in_specs = (
        P(("sp", "tp"), None),
        P("sp", "tp", None),
        P("sp", "tp", None),
        P("sp", "tp", None),
        P("sp", "tp", None),
        P("sp", "tp", None),
        P("sp", "tp", None),
        P("tp"),
        P("tp"),
        P(),
        P(),
        P(),
        P(("sp", "tp"), None),
        P(("sp", "tp"), None),
        P(("sp", "tp"), None, None),
        P(("sp", "tp"), None, None),
        P(("sp", "tp"), None, None),
        P(),
        P(),
        P(),
    )
    return jax.shard_map(
        per_device,
        mesh=mesh,
        in_specs=in_specs,
        out_specs=P(("sp", "tp"), None),
        check_vma=False,
    )
```

```python
import itertools

import jax
import jax.numpy as jnp
import numpy as np
from jax import lax
from jax.experimental import pallas as pl
from jax.experimental.pallas import tpu as pltpu
from jax.sharding import PartitionSpec as P

EPSILON = 1e-05
HEAD_SCALE = 0.8
NEG = -1e30
BF16 = jnp.bfloat16
F32 = jnp.float32


MESH = pl.DeviceIdType.MESH
SIDE = 4


def flows():
    every = np.array([o for o in itertools.product(range(SIDE), range(SIDE), range(SIDE), (0, 1)) if any(o)])
    mixed = every[np.random.RandomState(1).permutation(len(every))]
    hops = np.minimum(mixed[:, :3], SIDE - mixed[:, :3]).sum(axis=1)
    mixed = mixed[np.argsort(-hops, kind="stable")]
    for part in (mixed[:64], mixed[64:]):
        part[:] = part[np.random.RandomState(2).permutation(len(part))]
    return [tuple(int(v) for v in o) for o in mixed] + [(0, 0, 0, 0)]


ORDER = flows()


def layer_kernel(
    qa_ref,
    ka_ref,
    va_ref,
    qb_ref,
    kb_ref,
    vb_ref,
    la_ref,
    lb_ref,
    gain_ref,
    resid_ref,
    norm_ref,
    ids_ref,
    mix_ref,
    table_ref,
    wo_hbm,
    wg_hbm,
    wu_hbm,
    wd_hbm,
    sg_hbm,
    su_hbm,
    sd_hbm,
    out_ref,
    qt,
    kv,
    heads,
    back,
    acc,
    top,
    wo,
    wg,
    wu,
    wd,
    sg,
    su,
    sd,
    fill,
    combine,
    perm,
    middle,
    shared,
    send,
    recv,
    res,
    ret,
    xs,
    hs,
    rs,
    routed,
    send_sem,
    half_sem,
    pair_sem,
    tp_send,
    tp_recv,
    load_sem,
    a2a_send,
    a2a_recv,
):
    sp = lax.axis_index("sp")
    tp = lax.axis_index("tp")
    core = sp % 2
    chip = sp // 2
    z = chip // SIDE
    y = chip % SIDE
    rows = qa_ref.shape[0]
    half = rows // 2
    ones = jnp.ones((8, 2 * rows), BF16)

    z_at = [lax.rem(z + k, SIDE) * (SIDE * 2) for k in range(SIDE)]
    y_at = [lax.rem(y + k, SIDE) * 2 for k in range(SIDE)]
    core_at = [core, 1 - core]
    tp_at = [lax.rem(tp + k, SIDE) for k in range(SIDE)]

    def at(dz, dy, other):
        return z_at[dz % SIDE] + y_at[dy % SIDE] + core_at[other]

    def device(o, other):
        return (at(o[0], o[1], other), tp_at[o[2] % SIDE])

    def neighbour(dim, step):
        return (at(step, 0, 0), tp) if dim == 0 else (at(0, step, 0), tp)

    partner = (at(0, 0, 1), tp)
    loads = [
        pltpu.make_async_copy(source, target, load_sem.at[k])
        for k, (source, target) in enumerate(
            [(wo_hbm, wo), (sg_hbm, sg), (su_hbm, su), (sd_hbm, sd), (wg_hbm, wg), (wu_hbm, wu), (wd_hbm, wd)]
        )
    ]
    for load in loads:
        load.start()
    barrier = pltpu.get_barrier_semaphore()
    peers = [neighbour(d, k) for d in (0, 1) for k in (1, 3)] + [partner]
    peers += [(sp, tp_at[k]) for k in (1, 2, 3)]
    for peer in peers:
        pl.semaphore_signal(barrier, inc=1, device_id=peer, device_id_type=MESH)

    turned = qa_ref[...].astype(F32).T.astype(BF16)
    nothing = jnp.zeros((64, rows), BF16)
    qt[0] = jnp.concatenate([turned[:64], nothing], axis=0)
    qt[1] = jnp.concatenate([nothing, turned[64:]], axis=0)
    qt[2] = qb_ref[:, :128].astype(F32).T.astype(BF16)
    qt[3] = qb_ref[:, 128:].astype(F32).T.astype(BF16)
    kv[sp, :, 0:128] = ka_ref[...]
    kv[sp, :, 128:384] = kb_ref[...]
    kv[sp, 0:128, 384:640] = va_ref[...].astype(F32).T.astype(BF16)
    kv[sp, 128:256, 384:640] = vb_ref[...].astype(F32).T.astype(BF16)
    pl.semaphore_wait(barrier, len(peers))

    started = []

    def dims(h):
        return (1, 0) if h == 0 else (0, 1)

    def piece_of(h, o1, o2):
        return at(-o2, -o1, 0) if h == 0 else at(-o1, -o2, 0)

    def half_send(h, o1, o2, along, step, part=None):
        dim = dims(h)[along]
        new = [o1, o2]
        new[along] = (new[along] + step) % SIDE
        lo, size = (h * half, half) if part is None else (h * half + part * half // 2, half // 2)
        p = piece_of(h, o1, o2)
        copy = pltpu.make_async_remote_copy(
            src_ref=kv.at[p, pl.ds(lo, size)],
            dst_ref=kv.at[p, pl.ds(lo, size)],
            send_sem=send_sem.at[len(started)],
            recv_sem=half_sem.at[h * 16 + new[0] * 4 + new[1]],
            device_id=neighbour(dim, step),
            device_id_type=MESH,
        )
        copy.start()
        started.append(copy)

    def half_wait(h, o1, o2):
        p = piece_of(h, o1, o2)
        pltpu.make_async_copy(
            kv.at[p, pl.ds(h * half, half)],
            kv.at[p, pl.ds(h * half, half)],
            half_sem.at[h * 16 + o1 * 4 + o2],
        ).wait()

    def spread(h, o1, o2, along):
        o = (o1, o2)[along]
        if o == 0:
            half_send(h, o1, o2, along, 1)
            half_send(h, o1, o2, along, 3)
        elif o == 1:
            half_send(h, o1, o2, along, 1, 0)
        elif o == 3:
            half_send(h, o1, o2, along, 3, 1)

    def arrive(h, o1, o2):
        half_wait(h, o1, o2)
        if o2 == 0:
            spread(h, o1, o2, 0)
        spread(h, o1, o2, 1)

    def pair_send(a, b):
        p = at(-a, -b, 0)
        copy = pltpu.make_async_remote_copy(
            src_ref=kv.at[p],
            dst_ref=kv.at[p],
            send_sem=send_sem.at[len(started)],
            recv_sem=pair_sem.at[a * 4 + b],
            device_id=partner,
            device_id_type=MESH,
        )
        copy.start()
        started.append(copy)

    def chunk(c, masked, first):
        piece = [kv.at[2 * c], kv.at[2 * c + 1]]
        if masked:
            key_pos = lax.broadcasted_iota(jnp.int32, (2 * rows, rows), 0)
            query_pos = lax.broadcasted_iota(jnp.int32, (2 * rows, rows), 1) + core * rows
            keep = key_pos <= query_pos
        values = [
            jnp.concatenate(
                [
                    jnp.concatenate(
                        [p[head * 128 : head * 128 + 128, 384:640] for p in piece], axis=1
                    ),
                    ones,
                ],
                axis=0,
            )
            for head in range(2)
        ]

        def scores(h):
            lo = (0, 0, 128, 256)[h]
            keys = jnp.concatenate([p[:, lo : lo + 128] for p in piece], axis=0)
            s = jnp.dot(keys, qt[h], preferred_element_type=F32)
            return jnp.where(keep, s, NEG) if masked else s

        ready = scores(0)
        for h in range(4):
            s = ready
            if h < 3:
                ready = scores(h + 1)
            scale = (64**-0.5, 64**-0.5, 128**-0.5, 128**-0.5)[h]
            best = jnp.max(s, axis=0, keepdims=True)
            if not first:
                old = top[h : h + 1, :]
                best = jnp.maximum(best, old)
            p = jnp.exp((s - best) * scale).astype(BF16)
            add = jnp.dot(values[h // 2], p, preferred_element_type=F32)
            if first:
                acc[h] = add
            else:
                acc[h] = acc[h] * jnp.exp((old - best) * scale) + add
            top[h : h + 1, :] = best

    def chunks(offsets):
        code = 0
        for k, (a, b) in enumerate(offsets):
            code += (a * 4 + b) * 16**k

        def body(k, left):
            o = lax.rem(left, 16)
            a = o // 4
            b = lax.rem(o, 4)
            p = lax.rem(z + 4 - a, 4) * 8 + lax.rem(y + 4 - b, 4) * 2 + 1 - core
            pltpu.make_async_copy(kv.at[p], kv.at[p], pair_sem.at[o]).wait()
            c = p // 2

            @pl.when(c < chip)
            def _():
                chunk(c, False, False)

            return left // 16

        lax.fori_loop(0, len(offsets), body, jnp.int32(code))

    def slot_matrices():
        lane = lax.broadcasted_iota(jnp.int32, (64, 2048), 1)
        quarter = (lane // 4) % 4
        oz, oy, ox, oc = (table_ref[k : k + 1, :] for k in range(4))
        expert = (((z + oz) % 4) * 8 + ((y + oy) % 4) * 2 + (core + oc) % 2) * 4 + (tp + ox) % 4
        named = jnp.zeros((64, 2048), F32)
        mixed = jnp.zeros((64, 2048), F32)
        down = lax.broadcasted_iota(jnp.int32, (64, 64), 0)
        across = lax.broadcasted_iota(jnp.int32, (64, 64), 1)

        def column(row):
            return jnp.sum(jnp.where(down == across, row, jnp.zeros_like(row)), axis=1, keepdims=True)

        for k in range(4):
            same = column(ids_ref[k : k + 1, :]) == expert
            named = named + jnp.where(same, 1.0, 0.0)
            mixed = mixed + jnp.where(same, column(mix_ref[k : k + 1, :]), 0.0)
        before = jnp.where(across < down, 1.0, 0.0).astype(BF16)
        rank = jnp.dot(before, named.astype(BF16), preferred_element_type=F32)
        hit = (named > 0.5) & (jnp.abs(rank - (lane % 4).astype(F32)) < 0.5)
        placed = jnp.where(hit, 1.0, 0.0)
        mixed = jnp.where(hit, mixed, 0.0)
        high = mixed.astype(BF16).astype(F32)
        low = mixed - high
        for j in range(4):
            keep = quarter == j
            combine[j * 64 : j * 64 + 64] = jnp.where(keep, high, 0.0).astype(BF16)
            combine[256 + j * 64 : 256 + j * 64 + 64] = jnp.where(keep, low, 0.0).astype(BF16)
        for k in range(8):
            cols = slice(k * 256, k * 256 + 256)
            block = jnp.concatenate(
                [jnp.where(quarter[:, cols] == j, placed[:, cols], 0.0) for j in range(4)], axis=0
            )
            fill[cols] = block.T.astype(BF16)
        a = lax.broadcasted_iota(jnp.int32, (256, 256), 0)
        b = lax.broadcasted_iota(jnp.int32, (256, 256), 1)
        perm[0] = jnp.where(b == ((a // 4) % 16) * 16 + (a // 64) * 4 + a % 4, 1.0, 0.0).astype(BF16)
        perm[1] = jnp.where(a == ((b // 4) % 16) * 16 + (b // 64) * 4 + b % 4, 1.0, 0.0).astype(BF16)

    for h in range(2):
        spread(h, 0, 0, 0)
    pair_send(0, 0)
    for h in range(2):
        spread(h, 0, 0, 1)
    pltpu.make_async_copy(kv.at[sp], kv.at[sp], pair_sem.at[0]).wait()
    chunk(chip, True, True)

    slot_matrices()

    for o1 in (1, 3):
        for h in range(2):
            arrive(h, o1, 0)
    for o2 in (1, 3):
        for h in range(2):
            arrive(h, 0, o2)
    near = [(0, 1), (0, 3), (1, 0), (3, 0)]
    for a, b in near:
        pair_send(a, b)
    chunks(near)
    for h in range(2):
        arrive(h, 2, 0)
    for o1 in (1, 3):
        for o2 in (1, 3):
            for h in range(2):
                arrive(h, o1, o2)
    for h in range(2):
        arrive(h, 0, 2)
    second = [(0, 2), (2, 0), (1, 1), (1, 3), (3, 1), (3, 3)]
    for a, b in second:
        pair_send(a, b)
    chunks(second[:3])
    for o2 in (1, 3):
        for h in range(2):
            arrive(h, 2, o2)
    for o1 in (1, 3):
        for h in range(2):
            arrive(h, o1, 2)
    third = [(1, 2), (3, 2), (2, 1), (2, 3)]
    for a, b in third:
        pair_send(a, b)
    chunks(second[3:])
    for h in range(2):
        arrive(h, 2, 2)
    pair_send(2, 2)
    chunks(third + [(2, 2)])

    for head in range(2):
        first = acc[2 * head]
        second = acc[2 * head + 1]
        one = first[0:128] / first[128:129]
        two = second[0:128] / second[128:129]
        differ = one - (la_ref, lb_ref)[head][...] * two
        scale = lax.rsqrt(jnp.mean(differ * differ, axis=0, keepdims=True) + EPSILON)
        done = (differ * scale).T * gain_ref[...] * HEAD_SCALE
        heads[:, :, head * 128 : head * 128 + 128] = done.astype(BF16).reshape(4, rows // 4, 128)
    sends = []
    for k in (1, 2, 3):
        to = tp_at[k]
        copy = pltpu.make_async_remote_copy(
            src_ref=heads.at[to],
            dst_ref=back.at[tp],
            send_sem=tp_send.at[k],
            recv_sem=tp_recv.at[k],
            device_id=(sp, to),
            device_id_type=MESH,
        )
        copy.start()
        sends.append(copy)
    back[tp] = heads[tp]
    for load in loads:
        load.wait()
    for k in (1, 2, 3):
        source = tp_at[4 - k]
        pltpu.make_async_copy(back.at[source], back.at[source], tp_recv.at[k]).wait()

    joined = jnp.concatenate(
        [back[p, :, :128] for p in range(4)] + [back[p, :, 128:] for p in range(4)], axis=1
    )

    def project(n, total):
        cols = pl.ds(pl.multiple_of(n * 512, 512), 512)
        part = jnp.dot(joined, wo[:, cols], preferred_element_type=F32)
        rounded = (resid_ref[:, cols].astype(F32) + part).astype(BF16)
        middle[:, cols] = rounded
        wide = rounded.astype(F32)
        return total + jnp.sum(wide * wide, axis=1, keepdims=True)

    total = lax.fori_loop(0, 4, project, jnp.zeros((64, 1), F32), unroll=True)
    scale = lax.rsqrt(total / 2048.0 + EPSILON)
    normed = (middle[...].astype(F32) * scale * norm_ref[...]).astype(BF16)
    stack = jnp.concatenate([normed[:, j * 512 : j * 512 + 512] for j in range(4)], axis=0)

    def move(source, target, sem_out, sem_in, o, other):
        pltpu.make_async_remote_copy(
            src_ref=source,
            dst_ref=target,
            send_sem=sem_out,
            recv_sem=sem_in,
            device_id=device(o, other),
            device_id_type=MESH,
        ).start()

    def direct(way, source, target, lo, hi):
        sign = 1 - 2 * way
        for k in range(lo, hi):
            g = int(k >= 64)
            move(
                source.at[k],
                target.at[k],
                a2a_send.at[way * 2 + g],
                a2a_recv.at[way * 2 + g],
                [sign * v for v in ORDER[k][:3]],
                ORDER[k][3],
            )

    def arrived(way, target, g):
        part = target.at[pl.ds(g * 64, 64 - g)]
        pltpu.make_async_copy(part, part, a2a_recv.at[way * 2 + g]).wait()

    def fill_units(lo, hi):
        for u in range(lo, hi):
            rows_u = jnp.dot(fill[u * 256 : u * 256 + 256], stack, preferred_element_type=F32)
            send[u * 16 : u * 16 + 16] = rows_u.astype(BF16).reshape(16, 16, 512)

    for u in range(8):
        fill_units(u, u + 1)
        if u > 0:
            direct(0, send, recv, u * 16 - 16, u * 16)
    direct(0, send, recv, 112, 127)
    recv[127] = send[127]

    def shared_hidden(n, carry):
        cols = pl.ds(pl.multiple_of(n * 256, 256), 256)
        gate = jnp.dot(normed, sg[:, cols], preferred_element_type=F32)
        up = jnp.dot(normed, su[:, cols], preferred_element_type=F32)
        hs[0:64, cols] = (gate * jax.nn.sigmoid(gate) * up).astype(BF16)
        return carry

    lax.fori_loop(0, 2, shared_hidden, 0)

    def shared_down(n, carry):
        cols = pl.ds(pl.multiple_of(n * 256, 256), 256)
        shared[:, cols] = jnp.dot(hs[0:64, 0:512], sd[:, cols], preferred_element_type=F32)
        return carry

    lax.fori_loop(0, 8, shared_down, 0)

    def expert(g):
        for u in range(4):
            s0 = (g * 4 + u) * 16
            rows_u = jnp.dot(
                perm[0], recv[s0 : s0 + 16].reshape(256, 512), preferred_element_type=F32
            ).astype(BF16)
            for j in range(4):
                xs[u * 64 : u * 64 + 64, j * 512 : j * 512 + 512] = rows_u[j * 64 : j * 64 + 64]

        def hidden(n, carry):
            cols = pl.ds(pl.multiple_of(n * 256, 256), 256)
            gate = jnp.dot(xs[...], wg[:, cols], preferred_element_type=F32)
            up = jnp.dot(xs[...], wu[:, cols], preferred_element_type=F32)
            hs[:, cols] = (gate * jax.nn.sigmoid(gate) * up).astype(BF16)
            return carry

        lax.fori_loop(0, 4, hidden, 0)

        def down(n, carry):
            cols = pl.ds(pl.multiple_of(n * 256, 256), 256)
            rs[:, cols] = jnp.dot(hs[...], wd[:, cols], preferred_element_type=F32).astype(BF16)
            return carry

        lax.fori_loop(0, 8, down, 0)
        for u in range(4):
            s0 = (g * 4 + u) * 16
            block = jnp.concatenate(
                [rs[u * 64 : u * 64 + 64, j * 512 : j * 512 + 512] for j in range(4)], axis=0
            )
            rows_u = jnp.dot(perm[1], block, preferred_element_type=F32)
            res[s0 : s0 + 16] = rows_u.astype(BF16).reshape(16, 16, 512)
            if u > 0:
                direct(1, res, ret, s0 - 16, s0)
        direct(1, res, ret, g * 64 + 48, g * 64 + 64 - g)

    arrived(0, recv, 0)
    expert(0)
    arrived(0, recv, 1)
    expert(1)
    ret[127] = res[127]

    for g in range(2):
        arrived(1, ret, g)
        for half_cols in range(2):
            cols = slice(half_cols * 256, half_cols * 256 + 256)
            part = jnp.dot(
                combine[:, g * 1024 : g * 1024 + 1024],
                ret[g * 64 : g * 64 + 64].reshape(1024, 512)[:, cols],
                preferred_element_type=F32,
            )
            if g == 0:
                routed[:, cols] = part
            else:
                routed[:, cols] = routed[:, cols] + part
    for j in range(4):
        cols = slice(j * 512, j * 512 + 512)
        rows_j = routed[j * 64 : j * 64 + 64] + routed[256 + j * 64 : 256 + j * 64 + 64]
        out_ref[:, cols] = (middle[:, cols].astype(F32) + shared[:, cols] + rows_j).astype(BF16)

    for copy in started + sends:
        copy.wait_send()
    for way, buffer in enumerate((send, res)):
        for g in range(2):
            part = buffer.at[pl.ds(g * 64, 64 - g)]
            pltpu.make_async_copy(part, part, a2a_send.at[way * 2 + g]).wait()


def layer(qkv, lambdas, gain, resid, norm, ids, mix, weights):
    rows = qkv[0].shape[0]
    tokens, width = resid.shape
    table = np.zeros((8, 2048), np.int32)
    table[:4] = np.repeat(np.array(ORDER, np.int32).T, 16, axis=1)
    vmem = pl.BlockSpec(memory_space=pltpu.VMEM)
    slots = pltpu.VMEM((128, 16, 512), BF16)
    return pl.pallas_call(
        layer_kernel,
        out_shape=jax.ShapeDtypeStruct((tokens, width), BF16),
        in_specs=[vmem] * 14 + [pl.BlockSpec(memory_space=pl.ANY)] * 7,
        out_specs=vmem,
        scratch_shapes=[
            pltpu.VMEM((4, 128, rows), BF16),
            pltpu.VMEM((32, rows, 640), BF16),
            pltpu.VMEM((4, rows // 4, 256), BF16),
            pltpu.VMEM((4, rows // 4, 256), BF16),
            pltpu.VMEM((4, 136, rows), F32),
            pltpu.VMEM((8, rows), F32),
        ]
        + [pltpu.VMEM(weights[k].shape, BF16) for k in (0, 1, 2, 3, 4, 5, 6)]
        + [
            pltpu.VMEM((2048, 256), BF16),
            pltpu.VMEM((512, 2048), BF16),
            pltpu.VMEM((2, 256, 256), BF16),
            pltpu.VMEM((tokens, width), BF16),
            pltpu.VMEM((tokens, width), F32),
            slots,
            slots,
            slots,
            slots,
            pltpu.VMEM((256, width), BF16),
            pltpu.VMEM((256, 1024), BF16),
            pltpu.VMEM((256, width), BF16),
            pltpu.VMEM((512, 512), F32),
            pltpu.SemaphoreType.DMA((64,)),
            pltpu.SemaphoreType.DMA((32,)),
            pltpu.SemaphoreType.DMA((16,)),
            pltpu.SemaphoreType.DMA((4,)),
            pltpu.SemaphoreType.DMA((4,)),
            pltpu.SemaphoreType.DMA((7,)),
            pltpu.SemaphoreType.DMA((4,)),
            pltpu.SemaphoreType.DMA((4,)),
        ],
        compiler_params=pltpu.CompilerParams(
            vmem_limit_bytes=63 * 1024 * 1024, collective_id=0, has_side_effects=True
        ),
    )(*qkv, *lambdas, gain, resid, norm, ids, mix, jnp.asarray(table), *weights)


def per_device(
    resid,
    query_a,
    key_a,
    value_a,
    query_b,
    key_b,
    value_b,
    lambda_a,
    lambda_b,
    head_gain,
    out_weight,
    norm_gain,
    expert_ids,
    expert_mix,
    gate_experts,
    up_experts,
    down_experts,
    shared_gate,
    shared_up,
    shared_down,
):
    weights = (
        out_weight,
        gate_experts[0],
        up_experts[0],
        down_experts[0],
        shared_gate,
        shared_up,
        shared_down,
    )
    qkv = [a[:, 0] for a in (query_a, key_a, value_a, query_b, key_b, value_b)]
    return layer(
        qkv,
        (lambda_a[None, :], lambda_b[None, :]),
        head_gain[None, :],
        resid,
        norm_gain[None, :],
        expert_ids.T,
        expert_mix.T,
        weights,
    )


def solution(mesh):
    in_specs = (
        P(("sp", "tp"), None),
        P("sp", "tp", None),
        P("sp", "tp", None),
        P("sp", "tp", None),
        P("sp", "tp", None),
        P("sp", "tp", None),
        P("sp", "tp", None),
        P("tp"),
        P("tp"),
        P(),
        P(),
        P(),
        P(("sp", "tp"), None),
        P(("sp", "tp"), None),
        P(("sp", "tp"), None, None),
        P(("sp", "tp"), None, None),
        P(("sp", "tp"), None, None),
        P(),
        P(),
        P(),
    )
    return jax.shard_map(
        per_device,
        mesh=mesh,
        in_specs=in_specs,
        out_specs=P(("sp", "tp"), None),
        check_vma=False,
    )
```

```python
import itertools

import jax
import jax.numpy as jnp
import numpy as np
from jax import lax
from jax.experimental import pallas as pl
from jax.experimental.pallas import tpu as pltpu
from jax.sharding import PartitionSpec as P

EPSILON = 1e-05
HEAD_SCALE = 0.8
NEG = -1e30
BF16 = jnp.bfloat16
F32 = jnp.float32


MESH = pl.DeviceIdType.MESH
SIDE = 4


def flows():
    every = np.array([o for o in itertools.product(range(SIDE), range(SIDE), range(SIDE), (0, 1)) if any(o)])
    mixed = every[np.random.RandomState(1).permutation(len(every))]
    hops = np.minimum(mixed[:, :3], SIDE - mixed[:, :3]).sum(axis=1)
    mixed = mixed[np.argsort(-hops, kind="stable")]
    for part in (mixed[:64], mixed[64:]):
        part[:] = part[np.random.RandomState(2).permutation(len(part))]
    return [tuple(int(v) for v in o) for o in mixed] + [(0, 0, 0, 0)]


ORDER = flows()


STEPS = (
    ("a", [(1, 1, 0), (1, 3, 0), (0, 3, 0), (0, 0, 1), (0, 0, 3)]),
    ("c", [(3, 0), (1, 0)]),
    ("a", [(1, 0, 3), (0, 1, 0), (1, 0, 1), (0, 3, 3), (0, 0, 2), (1, 1, 3), (1, 1, 1), (0, 3, 1), (1, 2, 0)]),
    ("c", [(0, 1), (0, 3)]),
    ("a", [(0, 2, 0), (1, 3, 3)]),
    ("c", [(2, 0)]),
    ("a", [(0, 1, 3), (1, 0, 2), (0, 1, 1), (1, 3, 1)]),
    ("c", [(1, 3), (3, 3), (0, 2), (1, 1)]),
    ("a", [(1, 1, 2), (0, 2, 1), (1, 2, 1), (0, 3, 2), (1, 2, 3), (0, 2, 3)]),
    ("c", [(3, 1)]),
    ("a", [(1, 3, 2), (0, 1, 2)]),
    ("c", [(1, 2), (2, 3)]),
    ("a", [(1, 2, 2), (0, 2, 2)]),
    ("c", [(2, 1), (3, 2), (2, 2)]),
)


def layer_kernel(
    qa_ref,
    ka_ref,
    va_ref,
    qb_ref,
    kb_ref,
    vb_ref,
    la_ref,
    lb_ref,
    gain_ref,
    resid_ref,
    norm_ref,
    ids_ref,
    mix_ref,
    table_ref,
    wo_hbm,
    wg_hbm,
    wu_hbm,
    wd_hbm,
    sg_hbm,
    su_hbm,
    sd_hbm,
    out_ref,
    qt,
    kv,
    heads,
    back,
    acc,
    top,
    wo,
    wg,
    wu,
    wd,
    sg,
    su,
    sd,
    fill,
    combine,
    perm,
    middle,
    shared,
    send,
    recv,
    res,
    ret,
    xs,
    hs,
    rs,
    routed,
    send_sem,
    half_sem,
    pair_sem,
    tp_send,
    tp_recv,
    load_sem,
    a2a_send,
    a2a_recv,
):
    sp = lax.axis_index("sp")
    tp = lax.axis_index("tp")
    core = sp % 2
    chip = sp // 2
    z = chip // SIDE
    y = chip % SIDE
    rows = qa_ref.shape[0]
    half = rows // 2
    ones = jnp.ones((8, 2 * rows), BF16)

    z_at = [lax.rem(z + k, SIDE) * (SIDE * 2) for k in range(SIDE)]
    y_at = [lax.rem(y + k, SIDE) * 2 for k in range(SIDE)]
    core_at = [core, 1 - core]
    tp_at = [lax.rem(tp + k, SIDE) for k in range(SIDE)]

    def at(dz, dy, other):
        return z_at[dz % SIDE] + y_at[dy % SIDE] + core_at[other]

    def device(o, other):
        return (at(o[0], o[1], other), tp_at[o[2] % SIDE])

    def neighbour(dim, step):
        return (at(step, 0, 0), tp) if dim == 0 else (at(0, step, 0), tp)

    partner = (at(0, 0, 1), tp)
    loads = [
        pltpu.make_async_copy(source, target, load_sem.at[k])
        for k, (source, target) in enumerate(
            [(wo_hbm, wo), (sg_hbm, sg), (su_hbm, su), (sd_hbm, sd), (wg_hbm, wg), (wu_hbm, wu), (wd_hbm, wd)]
        )
    ]
    for load in loads:
        load.start()
    barrier = pltpu.get_barrier_semaphore()
    peers = [neighbour(d, k) for d in (0, 1) for k in (1, 3)] + [partner]
    peers += [(sp, tp_at[k]) for k in (1, 2, 3)]
    for peer in peers:
        pl.semaphore_signal(barrier, inc=1, device_id=peer, device_id_type=MESH)

    turned = qa_ref[...].astype(F32).T.astype(BF16)
    nothing = jnp.zeros((64, rows), BF16)
    qt[0] = jnp.concatenate([turned[:64], nothing], axis=0)
    qt[1] = jnp.concatenate([nothing, turned[64:]], axis=0)
    qt[2] = qb_ref[:, :128].astype(F32).T.astype(BF16)
    qt[3] = qb_ref[:, 128:].astype(F32).T.astype(BF16)
    kv[sp, :, 0:128] = ka_ref[...]
    kv[sp, :, 128:384] = kb_ref[...]
    kv[sp, 0:128, 384:640] = va_ref[...].astype(F32).T.astype(BF16)
    kv[sp, 128:256, 384:640] = vb_ref[...].astype(F32).T.astype(BF16)
    pl.semaphore_wait(barrier, len(peers))

    started = []

    def dims(h):
        return (1, 0) if h == 0 else (0, 1)

    def piece_of(h, o1, o2):
        return at(-o2, -o1, 0) if h == 0 else at(-o1, -o2, 0)

    def half_send(h, o1, o2, along, step, part=None):
        dim = dims(h)[along]
        new = [o1, o2]
        new[along] = (new[along] + step) % SIDE
        lo, size = (h * half, half) if part is None else (h * half + part * half // 2, half // 2)
        p = piece_of(h, o1, o2)
        copy = pltpu.make_async_remote_copy(
            src_ref=kv.at[p, pl.ds(lo, size)],
            dst_ref=kv.at[p, pl.ds(lo, size)],
            send_sem=send_sem.at[len(started)],
            recv_sem=half_sem.at[h * 16 + new[0] * 4 + new[1]],
            device_id=neighbour(dim, step),
            device_id_type=MESH,
        )
        copy.start()
        started.append(copy)

    def half_wait(h, o1, o2):
        p = piece_of(h, o1, o2)
        pltpu.make_async_copy(
            kv.at[p, pl.ds(h * half, half)],
            kv.at[p, pl.ds(h * half, half)],
            half_sem.at[h * 16 + o1 * 4 + o2],
        ).wait()

    def spread(h, o1, o2, along):
        o = (o1, o2)[along]
        if o == 0:
            half_send(h, o1, o2, along, 1)
            half_send(h, o1, o2, along, 3)
        elif o == 1:
            half_send(h, o1, o2, along, 1, 0)
        elif o == 3:
            half_send(h, o1, o2, along, 3, 1)

    def arrive(h, o1, o2):
        half_wait(h, o1, o2)
        if o2 == 0:
            spread(h, o1, o2, 0)
        spread(h, o1, o2, 1)

    def pair_send(a, b):
        p = at(-a, -b, 0)
        copy = pltpu.make_async_remote_copy(
            src_ref=kv.at[p],
            dst_ref=kv.at[p],
            send_sem=send_sem.at[len(started)],
            recv_sem=pair_sem.at[a * 4 + b],
            device_id=partner,
            device_id_type=MESH,
        )
        copy.start()
        started.append(copy)

    def chunk(c, masked, first):
        piece = [kv.at[2 * c], kv.at[2 * c + 1]]
        if masked:
            key_pos = lax.broadcasted_iota(jnp.int32, (2 * rows, rows), 0)
            query_pos = lax.broadcasted_iota(jnp.int32, (2 * rows, rows), 1) + core * rows
            keep = key_pos <= query_pos
        values = [
            jnp.concatenate(
                [
                    jnp.concatenate(
                        [p[head * 128 : head * 128 + 128, 384:640] for p in piece], axis=1
                    ),
                    ones,
                ],
                axis=0,
            )
            for head in range(2)
        ]

        def scores(h):
            lo = (0, 0, 128, 256)[h]
            keys = jnp.concatenate([p[:, lo : lo + 128] for p in piece], axis=0)
            s = jnp.dot(keys, qt[h], preferred_element_type=F32)
            return jnp.where(keep, s, NEG) if masked else s

        ready = scores(0)
        for h in range(4):
            s = ready
            if h < 3:
                ready = scores(h + 1)
            scale = (64**-0.5, 64**-0.5, 128**-0.5, 128**-0.5)[h]
            best = jnp.max(s, axis=0, keepdims=True)
            if not first:
                old = top[h : h + 1, :]
                best = jnp.maximum(best, old)
            p = jnp.exp((s - best) * scale).astype(BF16)
            add = jnp.dot(values[h // 2], p, preferred_element_type=F32)
            if first:
                acc[h] = add
            else:
                acc[h] = acc[h] * jnp.exp((old - best) * scale) + add
            top[h : h + 1, :] = best

    def chunks(offsets):
        code = 0
        for k, (a, b) in enumerate(offsets):
            code += (a * 4 + b) * 16**k

        def body(k, left):
            o = lax.rem(left, 16)
            a = o // 4
            b = lax.rem(o, 4)
            p = lax.rem(z + 4 - a, 4) * 8 + lax.rem(y + 4 - b, 4) * 2 + 1 - core
            pltpu.make_async_copy(kv.at[p], kv.at[p], pair_sem.at[o]).wait()
            c = p // 2

            @pl.when(c < chip)
            def _():
                chunk(c, False, False)

            return left // 16

        lax.fori_loop(0, len(offsets), body, jnp.int32(code))

    def slot_matrices():
        lane = lax.broadcasted_iota(jnp.int32, (64, 2048), 1)
        quarter = (lane // 4) % 4
        oz, oy, ox, oc = (table_ref[k : k + 1, :] for k in range(4))
        expert = (((z + oz) % 4) * 8 + ((y + oy) % 4) * 2 + (core + oc) % 2) * 4 + (tp + ox) % 4
        named = jnp.zeros((64, 2048), F32)
        mixed = jnp.zeros((64, 2048), F32)
        down = lax.broadcasted_iota(jnp.int32, (64, 64), 0)
        across = lax.broadcasted_iota(jnp.int32, (64, 64), 1)

        def column(row):
            return jnp.sum(jnp.where(down == across, row, jnp.zeros_like(row)), axis=1, keepdims=True)

        for k in range(4):
            same = column(ids_ref[k : k + 1, :]) == expert
            named = named + jnp.where(same, 1.0, 0.0)
            mixed = mixed + jnp.where(same, column(mix_ref[k : k + 1, :]), 0.0)
        before = jnp.where(across < down, 1.0, 0.0).astype(BF16)
        rank = jnp.dot(before, named.astype(BF16), preferred_element_type=F32)
        hit = (named > 0.5) & (jnp.abs(rank - (lane % 4).astype(F32)) < 0.5)
        placed = jnp.where(hit, 1.0, 0.0)
        mixed = jnp.where(hit, mixed, 0.0)
        high = mixed.astype(BF16).astype(F32)
        low = mixed - high
        for j in range(4):
            keep = quarter == j
            combine[j * 64 : j * 64 + 64] = jnp.where(keep, high, 0.0).astype(BF16)
            combine[256 + j * 64 : 256 + j * 64 + 64] = jnp.where(keep, low, 0.0).astype(BF16)
        for k in range(8):
            cols = slice(k * 256, k * 256 + 256)
            block = jnp.concatenate(
                [jnp.where(quarter[:, cols] == j, placed[:, cols], 0.0) for j in range(4)], axis=0
            )
            fill[cols] = block.T.astype(BF16)
        a = lax.broadcasted_iota(jnp.int32, (256, 256), 0)
        b = lax.broadcasted_iota(jnp.int32, (256, 256), 1)
        perm[0] = jnp.where(b == ((a // 4) % 16) * 16 + (a // 64) * 4 + a % 4, 1.0, 0.0).astype(BF16)
        perm[1] = jnp.where(a == ((b // 4) % 16) * 16 + (b // 64) * 4 + b % 4, 1.0, 0.0).astype(BF16)

    for h in range(2):
        spread(h, 0, 0, 0)
    pair_send(0, 0)
    for h in range(2):
        spread(h, 0, 0, 1)
    pltpu.make_async_copy(kv.at[sp], kv.at[sp], pair_sem.at[0]).wait()
    chunk(chip, True, True)

    slot_matrices()

    whole = set()
    for kind, items in STEPS:
        if kind == "c":
            chunks(items)
            continue
        for h, o1, o2 in items:
            arrive(h, o1, o2)
            whole.add((h, o1, o2))
            a, b = (o2, o1) if h == 0 else (o1, o2)
            if (0, b, a) in whole and (1, a, b) in whole:
                pair_send(a, b)

    for head in range(2):
        first = acc[2 * head]
        second = acc[2 * head + 1]
        one = first[0:128] / first[128:129]
        two = second[0:128] / second[128:129]
        differ = one - (la_ref, lb_ref)[head][...] * two
        scale = lax.rsqrt(jnp.mean(differ * differ, axis=0, keepdims=True) + EPSILON)
        done = (differ * scale).T * gain_ref[...] * HEAD_SCALE
        heads[:, :, head * 128 : head * 128 + 128] = done.astype(BF16).reshape(4, rows // 4, 128)
    sends = []
    for k in (1, 2, 3):
        to = tp_at[k]
        copy = pltpu.make_async_remote_copy(
            src_ref=heads.at[to],
            dst_ref=back.at[tp],
            send_sem=tp_send.at[k],
            recv_sem=tp_recv.at[k],
            device_id=(sp, to),
            device_id_type=MESH,
        )
        copy.start()
        sends.append(copy)
    back[tp] = heads[tp]
    for load in loads:
        load.wait()
    for k in (1, 2, 3):
        source = tp_at[4 - k]
        pltpu.make_async_copy(back.at[source], back.at[source], tp_recv.at[k]).wait()

    joined = jnp.concatenate(
        [back[p, :, :128] for p in range(4)] + [back[p, :, 128:] for p in range(4)], axis=1
    )

    def project(n, total):
        cols = pl.ds(pl.multiple_of(n * 512, 512), 512)
        part = jnp.dot(joined, wo[:, cols], preferred_element_type=F32)
        rounded = (resid_ref[:, cols].astype(F32) + part).astype(BF16)
        middle[:, cols] = rounded
        wide = rounded.astype(F32)
        return total + jnp.sum(wide * wide, axis=1, keepdims=True)

    total = lax.fori_loop(0, 4, project, jnp.zeros((64, 1), F32), unroll=True)
    scale = lax.rsqrt(total / 2048.0 + EPSILON)
    normed = (middle[...].astype(F32) * scale * norm_ref[...]).astype(BF16)
    stack = jnp.concatenate([normed[:, j * 512 : j * 512 + 512] for j in range(4)], axis=0)

    def move(source, target, sem_out, sem_in, o, other):
        pltpu.make_async_remote_copy(
            src_ref=source,
            dst_ref=target,
            send_sem=sem_out,
            recv_sem=sem_in,
            device_id=device(o, other),
            device_id_type=MESH,
        ).start()

    def direct(way, source, target, lo, hi):
        sign = 1 - 2 * way
        for k in range(lo, hi):
            g = int(k >= 64)
            move(
                source.at[k],
                target.at[k],
                a2a_send.at[way * 2 + g],
                a2a_recv.at[way * 2 + g],
                [sign * v for v in ORDER[k][:3]],
                ORDER[k][3],
            )

    def arrived(way, target, g):
        part = target.at[pl.ds(g * 64, 64 - g)]
        pltpu.make_async_copy(part, part, a2a_recv.at[way * 2 + g]).wait()

    def fill_units(lo, hi):
        for u in range(lo, hi):
            rows_u = jnp.dot(fill[u * 256 : u * 256 + 256], stack, preferred_element_type=F32)
            send[u * 16 : u * 16 + 16] = rows_u.astype(BF16).reshape(16, 16, 512)

    for u in range(8):
        fill_units(u, u + 1)
        if u > 0:
            direct(0, send, recv, u * 16 - 16, u * 16)
    direct(0, send, recv, 112, 127)
    recv[127] = send[127]

    def shared_hidden(n, carry):
        cols = pl.ds(pl.multiple_of(n * 256, 256), 256)
        gate = jnp.dot(normed, sg[:, cols], preferred_element_type=F32)
        up = jnp.dot(normed, su[:, cols], preferred_element_type=F32)
        hs[0:64, cols] = (gate * jax.nn.sigmoid(gate) * up).astype(BF16)
        return carry

    lax.fori_loop(0, 2, shared_hidden, 0)

    def shared_down(n, carry):
        cols = pl.ds(pl.multiple_of(n * 256, 256), 256)
        shared[:, cols] = jnp.dot(hs[0:64, 0:512], sd[:, cols], preferred_element_type=F32)
        return carry

    lax.fori_loop(0, 8, shared_down, 0)

    def expert(g):
        for u in range(4):
            s0 = (g * 4 + u) * 16
            rows_u = jnp.dot(
                perm[0], recv[s0 : s0 + 16].reshape(256, 512), preferred_element_type=F32
            ).astype(BF16)
            for j in range(4):
                xs[u * 64 : u * 64 + 64, j * 512 : j * 512 + 512] = rows_u[j * 64 : j * 64 + 64]

        def hidden(n, carry):
            cols = pl.ds(pl.multiple_of(n * 256, 256), 256)
            gate = jnp.dot(xs[...], wg[:, cols], preferred_element_type=F32)
            up = jnp.dot(xs[...], wu[:, cols], preferred_element_type=F32)
            hs[:, cols] = (gate * jax.nn.sigmoid(gate) * up).astype(BF16)
            return carry

        lax.fori_loop(0, 4, hidden, 0)

        def down(n, carry):
            cols = pl.ds(pl.multiple_of(n * 256, 256), 256)
            rs[:, cols] = jnp.dot(hs[...], wd[:, cols], preferred_element_type=F32).astype(BF16)
            return carry

        lax.fori_loop(0, 8, down, 0)
        for u in range(4):
            s0 = (g * 4 + u) * 16
            block = jnp.concatenate(
                [rs[u * 64 : u * 64 + 64, j * 512 : j * 512 + 512] for j in range(4)], axis=0
            )
            rows_u = jnp.dot(perm[1], block, preferred_element_type=F32)
            res[s0 : s0 + 16] = rows_u.astype(BF16).reshape(16, 16, 512)
            if u > 0:
                direct(1, res, ret, s0 - 16, s0)
        direct(1, res, ret, g * 64 + 48, g * 64 + 64 - g)

    arrived(0, recv, 0)
    expert(0)
    arrived(0, recv, 1)
    expert(1)
    ret[127] = res[127]

    for g in range(2):
        arrived(1, ret, g)
        for half_cols in range(2):
            cols = slice(half_cols * 256, half_cols * 256 + 256)
            part = jnp.dot(
                combine[:, g * 1024 : g * 1024 + 1024],
                ret[g * 64 : g * 64 + 64].reshape(1024, 512)[:, cols],
                preferred_element_type=F32,
            )
            if g == 0:
                routed[:, cols] = part
            else:
                routed[:, cols] = routed[:, cols] + part
    for j in range(4):
        cols = slice(j * 512, j * 512 + 512)
        rows_j = routed[j * 64 : j * 64 + 64] + routed[256 + j * 64 : 256 + j * 64 + 64]
        out_ref[:, cols] = (middle[:, cols].astype(F32) + shared[:, cols] + rows_j).astype(BF16)

    for copy in started + sends:
        copy.wait_send()
    for way, buffer in enumerate((send, res)):
        for g in range(2):
            part = buffer.at[pl.ds(g * 64, 64 - g)]
            pltpu.make_async_copy(part, part, a2a_send.at[way * 2 + g]).wait()


def layer(qkv, lambdas, gain, resid, norm, ids, mix, weights):
    rows = qkv[0].shape[0]
    tokens, width = resid.shape
    table = np.zeros((8, 2048), np.int32)
    table[:4] = np.repeat(np.array(ORDER, np.int32).T, 16, axis=1)
    vmem = pl.BlockSpec(memory_space=pltpu.VMEM)
    slots = pltpu.VMEM((128, 16, 512), BF16)
    return pl.pallas_call(
        layer_kernel,
        out_shape=jax.ShapeDtypeStruct((tokens, width), BF16),
        in_specs=[vmem] * 14 + [pl.BlockSpec(memory_space=pl.ANY)] * 7,
        out_specs=vmem,
        scratch_shapes=[
            pltpu.VMEM((4, 128, rows), BF16),
            pltpu.VMEM((32, rows, 640), BF16),
            pltpu.VMEM((4, rows // 4, 256), BF16),
            pltpu.VMEM((4, rows // 4, 256), BF16),
            pltpu.VMEM((4, 136, rows), F32),
            pltpu.VMEM((8, rows), F32),
        ]
        + [pltpu.VMEM(weights[k].shape, BF16) for k in (0, 1, 2, 3, 4, 5, 6)]
        + [
            pltpu.VMEM((2048, 256), BF16),
            pltpu.VMEM((512, 2048), BF16),
            pltpu.VMEM((2, 256, 256), BF16),
            pltpu.VMEM((tokens, width), BF16),
            pltpu.VMEM((tokens, width), F32),
            slots,
            slots,
            slots,
            slots,
            pltpu.VMEM((256, width), BF16),
            pltpu.VMEM((256, 1024), BF16),
            pltpu.VMEM((256, width), BF16),
            pltpu.VMEM((512, 512), F32),
            pltpu.SemaphoreType.DMA((64,)),
            pltpu.SemaphoreType.DMA((32,)),
            pltpu.SemaphoreType.DMA((16,)),
            pltpu.SemaphoreType.DMA((4,)),
            pltpu.SemaphoreType.DMA((4,)),
            pltpu.SemaphoreType.DMA((7,)),
            pltpu.SemaphoreType.DMA((4,)),
            pltpu.SemaphoreType.DMA((4,)),
        ],
        compiler_params=pltpu.CompilerParams(
            vmem_limit_bytes=63 * 1024 * 1024, collective_id=0, has_side_effects=True
        ),
    )(*qkv, *lambdas, gain, resid, norm, ids, mix, jnp.asarray(table), *weights)


def per_device(
    resid,
    query_a,
    key_a,
    value_a,
    query_b,
    key_b,
    value_b,
    lambda_a,
    lambda_b,
    head_gain,
    out_weight,
    norm_gain,
    expert_ids,
    expert_mix,
    gate_experts,
    up_experts,
    down_experts,
    shared_gate,
    shared_up,
    shared_down,
):
    weights = (
        out_weight,
        gate_experts[0],
        up_experts[0],
        down_experts[0],
        shared_gate,
        shared_up,
        shared_down,
    )
    qkv = [a[:, 0] for a in (query_a, key_a, value_a, query_b, key_b, value_b)]
    return layer(
        qkv,
        (lambda_a[None, :], lambda_b[None, :]),
        head_gain[None, :],
        resid,
        norm_gain[None, :],
        expert_ids.T,
        expert_mix.T,
        weights,
    )


def solution(mesh):
    in_specs = (
        P(("sp", "tp"), None),
        P("sp", "tp", None),
        P("sp", "tp", None),
        P("sp", "tp", None),
        P("sp", "tp", None),
        P("sp", "tp", None),
        P("sp", "tp", None),
        P("tp"),
        P("tp"),
        P(),
        P(),
        P(),
        P(("sp", "tp"), None),
        P(("sp", "tp"), None),
        P(("sp", "tp"), None, None),
        P(("sp", "tp"), None, None),
        P(("sp", "tp"), None, None),
        P(),
        P(),
        P(),
    )
    return jax.shard_map(
        per_device,
        mesh=mesh,
        in_specs=in_specs,
        out_specs=P(("sp", "tp"), None),
        check_vma=False,
    )
```

```python
import itertools

import jax
import jax.numpy as jnp
import numpy as np
from jax import lax
from jax.experimental import pallas as pl
from jax.experimental.pallas import tpu as pltpu
from jax.sharding import PartitionSpec as P

EPSILON = 1e-05
HEAD_SCALE = 0.8
NEG = -1e30
BF16 = jnp.bfloat16
F32 = jnp.float32


MESH = pl.DeviceIdType.MESH
SIDE = 4


def flows():
    every = np.array([o for o in itertools.product(range(SIDE), range(SIDE), range(SIDE), (0, 1)) if any(o)])
    mixed = every[np.random.RandomState(1).permutation(len(every))]
    hops = np.minimum(mixed[:, :3], SIDE - mixed[:, :3]).sum(axis=1)
    mixed = mixed[np.argsort(-hops, kind="stable")]
    for part in (mixed[:64], mixed[64:]):
        best = None
        for seed in range(200):
            trial = part[np.random.RandomState(seed).permutation(len(part))]
            load = np.zeros((len(part), 7))
            for k, o in enumerate(trial):
                for d in range(3):
                    v = o[d]
                    if v == 2:
                        load[k, 2 * d] += 1
                        load[k, 2 * d + 1] += 1
                    elif v:
                        load[k, 2 * d + (v == 3)] += 1
            run = np.cumsum(load[:, :6], axis=0)
            ideal = np.arange(1, len(part) + 1)[:, None] * run[-1] / len(part)
            score = np.abs(run - ideal).mean()
            if best is None or score < best[0]:
                best = (score, trial)
        part[:] = best[1]
    return [tuple(int(v) for v in o) for o in mixed] + [(0, 0, 0, 0)]


ORDER = flows()


STEPS = (
    ("a", [(1, 1, 0), (1, 3, 0), (0, 3, 0), (0, 0, 1), (0, 0, 3)]),
    ("c", [(3, 0), (1, 0)]),
    ("a", [(1, 0, 3), (0, 1, 0), (1, 0, 1), (0, 3, 3), (0, 0, 2), (1, 1, 3), (1, 1, 1), (0, 3, 1), (1, 2, 0)]),
    ("c", [(0, 1), (0, 3)]),
    ("a", [(0, 2, 0), (1, 3, 3)]),
    ("c", [(2, 0)]),
    ("a", [(0, 1, 3), (1, 0, 2), (0, 1, 1), (1, 3, 1)]),
    ("c", [(1, 3), (3, 3), (0, 2), (1, 1)]),
    ("a", [(1, 1, 2), (0, 2, 1), (1, 2, 1), (0, 3, 2), (1, 2, 3), (0, 2, 3)]),
    ("c", [(3, 1)]),
    ("a", [(1, 3, 2), (0, 1, 2)]),
    ("c", [(1, 2), (2, 3)]),
    ("a", [(1, 2, 2), (0, 2, 2)]),
    ("c", [(2, 1), (3, 2), (2, 2)]),
)


def layer_kernel(
    qa_ref,
    ka_ref,
    va_ref,
    qb_ref,
    kb_ref,
    vb_ref,
    la_ref,
    lb_ref,
    gain_ref,
    resid_ref,
    norm_ref,
    ids_ref,
    mix_ref,
    table_ref,
    wo_hbm,
    wg_hbm,
    wu_hbm,
    wd_hbm,
    sg_hbm,
    su_hbm,
    sd_hbm,
    out_ref,
    qt,
    kv,
    heads,
    back,
    acc,
    top,
    wo,
    wg,
    wu,
    wd,
    sg,
    su,
    sd,
    fill,
    combine,
    perm,
    middle,
    shared,
    send,
    recv,
    res,
    ret,
    xs,
    hs,
    rs,
    routed,
    send_sem,
    half_sem,
    pair_sem,
    tp_send,
    tp_recv,
    load_sem,
    a2a_send,
    a2a_recv,
):
    sp = lax.axis_index("sp")
    tp = lax.axis_index("tp")
    core = sp % 2
    chip = sp // 2
    z = chip // SIDE
    y = chip % SIDE
    rows = qa_ref.shape[0]
    half = rows // 2
    ones = jnp.ones((8, 2 * rows), BF16)

    z_at = [lax.rem(z + k, SIDE) * (SIDE * 2) for k in range(SIDE)]
    y_at = [lax.rem(y + k, SIDE) * 2 for k in range(SIDE)]
    core_at = [core, 1 - core]
    tp_at = [lax.rem(tp + k, SIDE) for k in range(SIDE)]

    def at(dz, dy, other):
        return z_at[dz % SIDE] + y_at[dy % SIDE] + core_at[other]

    def device(o, other):
        return (at(o[0], o[1], other), tp_at[o[2] % SIDE])

    def neighbour(dim, step):
        return (at(step, 0, 0), tp) if dim == 0 else (at(0, step, 0), tp)

    partner = (at(0, 0, 1), tp)
    loads = [
        pltpu.make_async_copy(source, target, load_sem.at[k])
        for k, (source, target) in enumerate(
            [(wo_hbm, wo), (sg_hbm, sg), (su_hbm, su), (sd_hbm, sd), (wg_hbm, wg), (wu_hbm, wu), (wd_hbm, wd)]
        )
    ]
    for load in loads:
        load.start()
    barrier = pltpu.get_barrier_semaphore()
    peers = [neighbour(d, k) for d in (0, 1) for k in (1, 3)] + [partner]
    peers += [(sp, tp_at[k]) for k in (1, 2, 3)]
    for peer in peers:
        pl.semaphore_signal(barrier, inc=1, device_id=peer, device_id_type=MESH)

    turned = qa_ref[...].astype(F32).T.astype(BF16)
    nothing = jnp.zeros((64, rows), BF16)
    qt[0] = jnp.concatenate([turned[:64], nothing], axis=0)
    qt[1] = jnp.concatenate([nothing, turned[64:]], axis=0)
    qt[2] = qb_ref[:, :128].astype(F32).T.astype(BF16)
    qt[3] = qb_ref[:, 128:].astype(F32).T.astype(BF16)
    kv[sp, :, 0:128] = ka_ref[...]
    kv[sp, :, 128:384] = kb_ref[...]
    kv[sp, 0:128, 384:640] = va_ref[...].astype(F32).T.astype(BF16)
    kv[sp, 128:256, 384:640] = vb_ref[...].astype(F32).T.astype(BF16)
    pl.semaphore_wait(barrier, len(peers))

    started = []

    def dims(h):
        return (1, 0) if h == 0 else (0, 1)

    def piece_of(h, o1, o2):
        return at(-o2, -o1, 0) if h == 0 else at(-o1, -o2, 0)

    def half_send(h, o1, o2, along, step, part=None):
        dim = dims(h)[along]
        new = [o1, o2]
        new[along] = (new[along] + step) % SIDE
        lo, size = (h * half, half) if part is None else (h * half + part * half // 2, half // 2)
        p = piece_of(h, o1, o2)
        copy = pltpu.make_async_remote_copy(
            src_ref=kv.at[p, pl.ds(lo, size)],
            dst_ref=kv.at[p, pl.ds(lo, size)],
            send_sem=send_sem.at[len(started)],
            recv_sem=half_sem.at[h * 16 + new[0] * 4 + new[1]],
            device_id=neighbour(dim, step),
            device_id_type=MESH,
        )
        copy.start()
        started.append(copy)

    def half_wait(h, o1, o2):
        p = piece_of(h, o1, o2)
        pltpu.make_async_copy(
            kv.at[p, pl.ds(h * half, half)],
            kv.at[p, pl.ds(h * half, half)],
            half_sem.at[h * 16 + o1 * 4 + o2],
        ).wait()

    def spread(h, o1, o2, along):
        o = (o1, o2)[along]
        if o == 0:
            half_send(h, o1, o2, along, 1)
            half_send(h, o1, o2, along, 3)
        elif o == 1:
            half_send(h, o1, o2, along, 1, 0)
        elif o == 3:
            half_send(h, o1, o2, along, 3, 1)

    def arrive(h, o1, o2):
        half_wait(h, o1, o2)
        if o2 == 0:
            spread(h, o1, o2, 0)
        spread(h, o1, o2, 1)

    def pair_send(a, b):
        p = at(-a, -b, 0)
        copy = pltpu.make_async_remote_copy(
            src_ref=kv.at[p],
            dst_ref=kv.at[p],
            send_sem=send_sem.at[len(started)],
            recv_sem=pair_sem.at[a * 4 + b],
            device_id=partner,
            device_id_type=MESH,
        )
        copy.start()
        started.append(copy)

    def chunk(c, masked, first):
        piece = [kv.at[2 * c], kv.at[2 * c + 1]]
        if masked:
            key_pos = lax.broadcasted_iota(jnp.int32, (2 * rows, rows), 0)
            query_pos = lax.broadcasted_iota(jnp.int32, (2 * rows, rows), 1) + core * rows
            keep = key_pos <= query_pos
        values = [
            jnp.concatenate(
                [
                    jnp.concatenate(
                        [p[head * 128 : head * 128 + 128, 384:640] for p in piece], axis=1
                    ),
                    ones,
                ],
                axis=0,
            )
            for head in range(2)
        ]

        def scores(h):
            lo = (0, 0, 128, 256)[h]
            keys = jnp.concatenate([p[:, lo : lo + 128] for p in piece], axis=0)
            s = jnp.dot(keys, qt[h], preferred_element_type=F32)
            return jnp.where(keep, s, NEG) if masked else s

        ready = scores(0)
        for h in range(4):
            s = ready
            if h < 3:
                ready = scores(h + 1)
            scale = (64**-0.5, 64**-0.5, 128**-0.5, 128**-0.5)[h]
            best = jnp.max(s, axis=0, keepdims=True)
            if not first:
                old = top[h : h + 1, :]
                best = jnp.maximum(best, old)
            p = jnp.exp((s - best) * scale).astype(BF16)
            add = jnp.dot(values[h // 2], p, preferred_element_type=F32)
            if first:
                acc[h] = add
            else:
                acc[h] = acc[h] * jnp.exp((old - best) * scale) + add
            top[h : h + 1, :] = best

    def chunks(offsets):
        code = 0
        for k, (a, b) in enumerate(offsets):
            code += (a * 4 + b) * 16**k

        def body(k, left):
            o = lax.rem(left, 16)
            a = o // 4
            b = lax.rem(o, 4)
            p = lax.rem(z + 4 - a, 4) * 8 + lax.rem(y + 4 - b, 4) * 2 + 1 - core
            pltpu.make_async_copy(kv.at[p], kv.at[p], pair_sem.at[o]).wait()
            c = p // 2

            @pl.when(c < chip)
            def _():
                chunk(c, False, False)

            return left // 16

        lax.fori_loop(0, len(offsets), body, jnp.int32(code))

    def slot_matrices():
        lane = lax.broadcasted_iota(jnp.int32, (64, 2048), 1)
        quarter = (lane // 4) % 4
        oz, oy, ox, oc = (table_ref[k : k + 1, :] for k in range(4))
        expert = (((z + oz) % 4) * 8 + ((y + oy) % 4) * 2 + (core + oc) % 2) * 4 + (tp + ox) % 4
        named = jnp.zeros((64, 2048), F32)
        mixed = jnp.zeros((64, 2048), F32)
        down = lax.broadcasted_iota(jnp.int32, (64, 64), 0)
        across = lax.broadcasted_iota(jnp.int32, (64, 64), 1)

        def column(row):
            return jnp.sum(jnp.where(down == across, row, jnp.zeros_like(row)), axis=1, keepdims=True)

        for k in range(4):
            same = column(ids_ref[k : k + 1, :]) == expert
            named = named + jnp.where(same, 1.0, 0.0)
            mixed = mixed + jnp.where(same, column(mix_ref[k : k + 1, :]), 0.0)
        before = jnp.where(across < down, 1.0, 0.0).astype(BF16)
        rank = jnp.dot(before, named.astype(BF16), preferred_element_type=F32)
        hit = (named > 0.5) & (jnp.abs(rank - (lane % 4).astype(F32)) < 0.5)
        placed = jnp.where(hit, 1.0, 0.0)
        mixed = jnp.where(hit, mixed, 0.0)
        high = mixed.astype(BF16).astype(F32)
        low = mixed - high
        for j in range(4):
            keep = quarter == j
            combine[j * 64 : j * 64 + 64] = jnp.where(keep, high, 0.0).astype(BF16)
            combine[256 + j * 64 : 256 + j * 64 + 64] = jnp.where(keep, low, 0.0).astype(BF16)
        for k in range(8):
            cols = slice(k * 256, k * 256 + 256)
            block = jnp.concatenate(
                [jnp.where(quarter[:, cols] == j, placed[:, cols], 0.0) for j in range(4)], axis=0
            )
            fill[cols] = block.T.astype(BF16)
        a = lax.broadcasted_iota(jnp.int32, (256, 256), 0)
        b = lax.broadcasted_iota(jnp.int32, (256, 256), 1)
        perm[0] = jnp.where(b == ((a // 4) % 16) * 16 + (a // 64) * 4 + a % 4, 1.0, 0.0).astype(BF16)
        perm[1] = jnp.where(a == ((b // 4) % 16) * 16 + (b // 64) * 4 + b % 4, 1.0, 0.0).astype(BF16)

    for h in range(2):
        spread(h, 0, 0, 0)
    pair_send(0, 0)
    for h in range(2):
        spread(h, 0, 0, 1)
    pltpu.make_async_copy(kv.at[sp], kv.at[sp], pair_sem.at[0]).wait()
    chunk(chip, True, True)

    slot_matrices()

    whole = set()
    for kind, items in STEPS:
        if kind == "c":
            chunks(items)
            continue
        for h, o1, o2 in items:
            arrive(h, o1, o2)
            whole.add((h, o1, o2))
            a, b = (o2, o1) if h == 0 else (o1, o2)
            if (0, b, a) in whole and (1, a, b) in whole:
                pair_send(a, b)

    for head in range(2):
        first = acc[2 * head]
        second = acc[2 * head + 1]
        one = first[0:128] / first[128:129]
        two = second[0:128] / second[128:129]
        differ = one - (la_ref, lb_ref)[head][...] * two
        scale = lax.rsqrt(jnp.mean(differ * differ, axis=0, keepdims=True) + EPSILON)
        done = (differ * scale).T * gain_ref[...] * HEAD_SCALE
        heads[:, :, head * 128 : head * 128 + 128] = done.astype(BF16).reshape(4, rows // 4, 128)
    sends = []
    for k in (1, 2, 3):
        to = tp_at[k]
        copy = pltpu.make_async_remote_copy(
            src_ref=heads.at[to],
            dst_ref=back.at[tp],
            send_sem=tp_send.at[k],
            recv_sem=tp_recv.at[k],
            device_id=(sp, to),
            device_id_type=MESH,
        )
        copy.start()
        sends.append(copy)
    back[tp] = heads[tp]
    for load in loads:
        load.wait()
    for k in (1, 2, 3):
        source = tp_at[4 - k]
        pltpu.make_async_copy(back.at[source], back.at[source], tp_recv.at[k]).wait()

    joined = jnp.concatenate(
        [back[p, :, :128] for p in range(4)] + [back[p, :, 128:] for p in range(4)], axis=1
    )

    def project(n, total):
        cols = pl.ds(pl.multiple_of(n * 512, 512), 512)
        part = jnp.dot(joined, wo[:, cols], preferred_element_type=F32)
        rounded = (resid_ref[:, cols].astype(F32) + part).astype(BF16)
        middle[:, cols] = rounded
        wide = rounded.astype(F32)
        return total + jnp.sum(wide * wide, axis=1, keepdims=True)

    total = lax.fori_loop(0, 4, project, jnp.zeros((64, 1), F32), unroll=True)
    scale = lax.rsqrt(total / 2048.0 + EPSILON)
    normed = (middle[...].astype(F32) * scale * norm_ref[...]).astype(BF16)
    stack = jnp.concatenate([normed[:, j * 512 : j * 512 + 512] for j in range(4)], axis=0)

    def move(source, target, sem_out, sem_in, o, other):
        pltpu.make_async_remote_copy(
            src_ref=source,
            dst_ref=target,
            send_sem=sem_out,
            recv_sem=sem_in,
            device_id=device(o, other),
            device_id_type=MESH,
        ).start()

    def direct(way, source, target, lo, hi):
        sign = 1 - 2 * way
        for k in range(lo, hi):
            g = int(k >= 64)
            move(
                source.at[k],
                target.at[k],
                a2a_send.at[way * 2 + g],
                a2a_recv.at[way * 2 + g],
                [sign * v for v in ORDER[k][:3]],
                ORDER[k][3],
            )

    def arrived(way, target, g):
        part = target.at[pl.ds(g * 64, 64 - g)]
        pltpu.make_async_copy(part, part, a2a_recv.at[way * 2 + g]).wait()

    def fill_units(lo, hi):
        for u in range(lo, hi):
            rows_u = jnp.dot(fill[u * 256 : u * 256 + 256], stack, preferred_element_type=F32)
            send[u * 16 : u * 16 + 16] = rows_u.astype(BF16).reshape(16, 16, 512)

    for u in range(8):
        fill_units(u, u + 1)
        if u > 0:
            direct(0, send, recv, u * 16 - 16, u * 16)
    direct(0, send, recv, 112, 127)
    recv[127] = send[127]

    def shared_hidden(n, carry):
        cols = pl.ds(pl.multiple_of(n * 256, 256), 256)
        gate = jnp.dot(normed, sg[:, cols], preferred_element_type=F32)
        up = jnp.dot(normed, su[:, cols], preferred_element_type=F32)
        hs[0:64, cols] = (gate * jax.nn.sigmoid(gate) * up).astype(BF16)
        return carry

    lax.fori_loop(0, 2, shared_hidden, 0)

    def shared_down(n, carry):
        cols = pl.ds(pl.multiple_of(n * 256, 256), 256)
        shared[:, cols] = jnp.dot(hs[0:64, 0:512], sd[:, cols], preferred_element_type=F32)
        return carry

    lax.fori_loop(0, 8, shared_down, 0)

    def expert(g):
        for u in range(4):
            s0 = (g * 4 + u) * 16
            rows_u = jnp.dot(
                perm[0], recv[s0 : s0 + 16].reshape(256, 512), preferred_element_type=F32
            ).astype(BF16)
            for j in range(4):
                xs[u * 64 : u * 64 + 64, j * 512 : j * 512 + 512] = rows_u[j * 64 : j * 64 + 64]

        def hidden(n, carry):
            cols = pl.ds(pl.multiple_of(n * 256, 256), 256)
            gate = jnp.dot(xs[...], wg[:, cols], preferred_element_type=F32)
            up = jnp.dot(xs[...], wu[:, cols], preferred_element_type=F32)
            hs[:, cols] = (gate * jax.nn.sigmoid(gate) * up).astype(BF16)
            return carry

        lax.fori_loop(0, 4, hidden, 0, unroll=2)

        def down(n, carry):
            cols = pl.ds(pl.multiple_of(n * 256, 256), 256)
            rs[:, cols] = jnp.dot(hs[...], wd[:, cols], preferred_element_type=F32).astype(BF16)
            return carry

        lax.fori_loop(0, 8, down, 0, unroll=2)
        for u in range(4):
            s0 = (g * 4 + u) * 16
            block = jnp.concatenate(
                [rs[u * 64 : u * 64 + 64, j * 512 : j * 512 + 512] for j in range(4)], axis=0
            )
            rows_u = jnp.dot(perm[1], block, preferred_element_type=F32)
            res[s0 : s0 + 16] = rows_u.astype(BF16).reshape(16, 16, 512)
            if u > 0:
                direct(1, res, ret, s0 - 16, s0)
        direct(1, res, ret, g * 64 + 48, g * 64 + 64 - g)

    arrived(0, recv, 0)
    expert(0)
    arrived(0, recv, 1)
    expert(1)
    ret[127] = res[127]

    for g in range(2):
        arrived(1, ret, g)
        for half_cols in range(2):
            cols = slice(half_cols * 256, half_cols * 256 + 256)
            part = jnp.dot(
                combine[:, g * 1024 : g * 1024 + 1024],
                ret[g * 64 : g * 64 + 64].reshape(1024, 512)[:, cols],
                preferred_element_type=F32,
            )
            if g == 0:
                routed[:, cols] = part
            else:
                routed[:, cols] = routed[:, cols] + part
    for j in range(4):
        cols = slice(j * 512, j * 512 + 512)
        rows_j = routed[j * 64 : j * 64 + 64] + routed[256 + j * 64 : 256 + j * 64 + 64]
        out_ref[:, cols] = (middle[:, cols].astype(F32) + shared[:, cols] + rows_j).astype(BF16)

    for copy in started + sends:
        copy.wait_send()
    for way, buffer in enumerate((send, res)):
        for g in range(2):
            part = buffer.at[pl.ds(g * 64, 64 - g)]
            pltpu.make_async_copy(part, part, a2a_send.at[way * 2 + g]).wait()


def layer(qkv, lambdas, gain, resid, norm, ids, mix, weights):
    rows = qkv[0].shape[0]
    tokens, width = resid.shape
    table = np.zeros((8, 2048), np.int32)
    table[:4] = np.repeat(np.array(ORDER, np.int32).T, 16, axis=1)
    vmem = pl.BlockSpec(memory_space=pltpu.VMEM)
    slots = pltpu.VMEM((128, 16, 512), BF16)
    return pl.pallas_call(
        layer_kernel,
        out_shape=jax.ShapeDtypeStruct((tokens, width), BF16),
        in_specs=[vmem] * 14 + [pl.BlockSpec(memory_space=pl.ANY)] * 7,
        out_specs=vmem,
        scratch_shapes=[
            pltpu.VMEM((4, 128, rows), BF16),
            pltpu.VMEM((32, rows, 640), BF16),
            pltpu.VMEM((4, rows // 4, 256), BF16),
            pltpu.VMEM((4, rows // 4, 256), BF16),
            pltpu.VMEM((4, 136, rows), F32),
            pltpu.VMEM((8, rows), F32),
        ]
        + [pltpu.VMEM(weights[k].shape, BF16) for k in (0, 1, 2, 3, 4, 5, 6)]
        + [
            pltpu.VMEM((2048, 256), BF16),
            pltpu.VMEM((512, 2048), BF16),
            pltpu.VMEM((2, 256, 256), BF16),
            pltpu.VMEM((tokens, width), BF16),
            pltpu.VMEM((tokens, width), F32),
            slots,
            slots,
            slots,
            slots,
            pltpu.VMEM((256, width), BF16),
            pltpu.VMEM((256, 1024), BF16),
            pltpu.VMEM((256, width), BF16),
            pltpu.VMEM((512, 512), F32),
            pltpu.SemaphoreType.DMA((64,)),
            pltpu.SemaphoreType.DMA((32,)),
            pltpu.SemaphoreType.DMA((16,)),
            pltpu.SemaphoreType.DMA((4,)),
            pltpu.SemaphoreType.DMA((4,)),
            pltpu.SemaphoreType.DMA((7,)),
            pltpu.SemaphoreType.DMA((4,)),
            pltpu.SemaphoreType.DMA((4,)),
        ],
        compiler_params=pltpu.CompilerParams(
            vmem_limit_bytes=63 * 1024 * 1024, collective_id=0, has_side_effects=True
        ),
    )(*qkv, *lambdas, gain, resid, norm, ids, mix, jnp.asarray(table), *weights)


def per_device(
    resid,
    query_a,
    key_a,
    value_a,
    query_b,
    key_b,
    value_b,
    lambda_a,
    lambda_b,
    head_gain,
    out_weight,
    norm_gain,
    expert_ids,
    expert_mix,
    gate_experts,
    up_experts,
    down_experts,
    shared_gate,
    shared_up,
    shared_down,
):
    weights = (
        out_weight,
        gate_experts[0],
        up_experts[0],
        down_experts[0],
        shared_gate,
        shared_up,
        shared_down,
    )
    qkv = [a[:, 0] for a in (query_a, key_a, value_a, query_b, key_b, value_b)]
    return layer(
        qkv,
        (lambda_a[None, :], lambda_b[None, :]),
        head_gain[None, :],
        resid,
        norm_gain[None, :],
        expert_ids.T,
        expert_mix.T,
        weights,
    )


def solution(mesh):
    in_specs = (
        P(("sp", "tp"), None),
        P("sp", "tp", None),
        P("sp", "tp", None),
        P("sp", "tp", None),
        P("sp", "tp", None),
        P("sp", "tp", None),
        P("sp", "tp", None),
        P("tp"),
        P("tp"),
        P(),
        P(),
        P(),
        P(("sp", "tp"), None),
        P(("sp", "tp"), None),
        P(("sp", "tp"), None, None),
        P(("sp", "tp"), None, None),
        P(("sp", "tp"), None, None),
        P(),
        P(),
        P(),
    )
    return jax.shard_map(
        per_device,
        mesh=mesh,
        in_specs=in_specs,
        out_specs=P(("sp", "tp"), None),
        check_vma=False,
    )
```

```python
import itertools

import jax
import jax.numpy as jnp
import numpy as np
from jax import lax
from jax.experimental import pallas as pl
from jax.experimental.pallas import tpu as pltpu
from jax.sharding import PartitionSpec as P

EPSILON = 1e-05
HEAD_SCALE = 0.8
NEG = -1e30
BF16 = jnp.bfloat16
F32 = jnp.float32


MESH = pl.DeviceIdType.MESH
SIDE = 4


def flows():
    every = np.array([o for o in itertools.product(range(SIDE), range(SIDE), range(SIDE), (0, 1)) if any(o)])
    mixed = every[np.random.RandomState(1).permutation(len(every))]
    hops = np.minimum(mixed[:, :3], SIDE - mixed[:, :3]).sum(axis=1)
    mixed = mixed[np.argsort(-hops, kind="stable")]
    for part in (mixed[:64], mixed[64:]):
        best = None
        for seed in range(200):
            trial = part[np.random.RandomState(seed).permutation(len(part))]
            load = np.zeros((len(part), 7))
            for k, o in enumerate(trial):
                for d in range(3):
                    v = o[d]
                    if v == 2:
                        load[k, 2 * d] += 1
                        load[k, 2 * d + 1] += 1
                    elif v:
                        load[k, 2 * d + (v == 3)] += 1
            run = np.cumsum(load[:, :6], axis=0)
            ideal = np.arange(1, len(part) + 1)[:, None] * run[-1] / len(part)
            score = np.abs(run - ideal).mean()
            if best is None or score < best[0]:
                best = (score, trial)
        part[:] = best[1]
    return [tuple(int(v) for v in o) for o in mixed] + [(0, 0, 0, 0)]


ORDER = flows()


STEPS = (
    ("a", [(1, 1, 0), (1, 3, 0), (0, 3, 0), (0, 0, 1), (0, 0, 3)]),
    ("c", [(3, 0), (1, 0)]),
    ("a", [(1, 0, 3), (0, 1, 0), (1, 0, 1), (0, 3, 3), (0, 0, 2), (1, 1, 3), (1, 1, 1), (0, 3, 1), (1, 2, 0)]),
    ("c", [(0, 1), (0, 3)]),
    ("a", [(0, 2, 0), (1, 3, 3)]),
    ("c", [(2, 0)]),
    ("a", [(0, 1, 3), (1, 0, 2), (0, 1, 1), (1, 3, 1)]),
    ("c", [(1, 3), (3, 3), (0, 2), (1, 1)]),
    ("a", [(1, 1, 2), (0, 2, 1), (1, 2, 1), (0, 3, 2), (1, 2, 3), (0, 2, 3)]),
    ("c", [(3, 1)]),
    ("a", [(1, 3, 2), (0, 1, 2)]),
    ("c", [(1, 2), (2, 3)]),
    ("a", [(1, 2, 2), (0, 2, 2)]),
    ("c", [(2, 1), (3, 2), (2, 2)]),
)


def layer_kernel(
    qa_ref,
    ka_ref,
    va_ref,
    qb_ref,
    kb_ref,
    vb_ref,
    la_ref,
    lb_ref,
    gain_ref,
    resid_ref,
    norm_ref,
    ids_ref,
    mix_ref,
    table_ref,
    wo_hbm,
    wg_hbm,
    wu_hbm,
    wd_hbm,
    sg_hbm,
    su_hbm,
    sd_hbm,
    out_ref,
    qt,
    kv,
    heads,
    back,
    acc,
    top,
    wo,
    wg,
    wu,
    wd,
    sg,
    su,
    sd,
    fill,
    combine,
    perm,
    middle,
    shared,
    send,
    recv,
    res,
    ret,
    xs,
    hs,
    rs,
    routed,
    send_sem,
    half_sem,
    pair_sem,
    tp_send,
    tp_recv,
    load_sem,
    a2a_send,
    a2a_recv,
):
    sp = lax.axis_index("sp")
    tp = lax.axis_index("tp")
    core = sp % 2
    chip = sp // 2
    z = chip // SIDE
    y = chip % SIDE
    rows = qa_ref.shape[0]
    half = rows // 2
    ones = jnp.ones((8, 2 * rows), BF16)

    z_at = [lax.rem(z + k, SIDE) * (SIDE * 2) for k in range(SIDE)]
    y_at = [lax.rem(y + k, SIDE) * 2 for k in range(SIDE)]
    core_at = [core, 1 - core]
    tp_at = [lax.rem(tp + k, SIDE) for k in range(SIDE)]

    def at(dz, dy, other):
        return z_at[dz % SIDE] + y_at[dy % SIDE] + core_at[other]

    def device(o, other):
        return (at(o[0], o[1], other), tp_at[o[2] % SIDE])

    def neighbour(dim, step):
        return (at(step, 0, 0), tp) if dim == 0 else (at(0, step, 0), tp)

    partner = (at(0, 0, 1), tp)
    loads = [
        pltpu.make_async_copy(source, target, load_sem.at[k])
        for k, (source, target) in enumerate(
            [(wo_hbm, wo), (sg_hbm, sg), (su_hbm, su), (sd_hbm, sd), (wg_hbm, wg), (wu_hbm, wu), (wd_hbm, wd)]
        )
    ]
    for load in loads:
        load.start()
    barrier = pltpu.get_barrier_semaphore()
    peers = [neighbour(d, k) for d in (0, 1) for k in (1, 3)] + [partner]
    peers += [(sp, tp_at[k]) for k in (1, 2, 3)]
    for peer in peers:
        pl.semaphore_signal(barrier, inc=1, device_id=peer, device_id_type=MESH)

    turned = qa_ref[...].astype(F32).T.astype(BF16)
    nothing = jnp.zeros((64, rows), BF16)
    qt[0] = jnp.concatenate([turned[:64], nothing], axis=0)
    qt[1] = jnp.concatenate([nothing, turned[64:]], axis=0)
    qt[2] = qb_ref[:, :128].astype(F32).T.astype(BF16)
    qt[3] = qb_ref[:, 128:].astype(F32).T.astype(BF16)
    kv[sp, :, 0:128] = ka_ref[...]
    kv[sp, :, 128:384] = kb_ref[...]
    kv[sp, 0:128, 384:640] = va_ref[...].astype(F32).T.astype(BF16)
    kv[sp, 128:256, 384:640] = vb_ref[...].astype(F32).T.astype(BF16)
    pl.semaphore_wait(barrier, len(peers))

    started = []

    def dims(h):
        return (1, 0) if h == 0 else (0, 1)

    def piece_of(h, o1, o2):
        return at(-o2, -o1, 0) if h == 0 else at(-o1, -o2, 0)

    def half_send(h, o1, o2, along, step, part=None):
        dim = dims(h)[along]
        new = [o1, o2]
        new[along] = (new[along] + step) % SIDE
        lo, size = (h * half, half) if part is None else (h * half + part * half // 2, half // 2)
        p = piece_of(h, o1, o2)
        copy = pltpu.make_async_remote_copy(
            src_ref=kv.at[p, pl.ds(lo, size)],
            dst_ref=kv.at[p, pl.ds(lo, size)],
            send_sem=send_sem.at[len(started)],
            recv_sem=half_sem.at[h * 16 + new[0] * 4 + new[1]],
            device_id=neighbour(dim, step),
            device_id_type=MESH,
        )
        copy.start()
        started.append(copy)

    def half_wait(h, o1, o2):
        p = piece_of(h, o1, o2)
        pltpu.make_async_copy(
            kv.at[p, pl.ds(h * half, half)],
            kv.at[p, pl.ds(h * half, half)],
            half_sem.at[h * 16 + o1 * 4 + o2],
        ).wait()

    def spread(h, o1, o2, along):
        o = (o1, o2)[along]
        if o == 0:
            half_send(h, o1, o2, along, 1)
            half_send(h, o1, o2, along, 3)
        elif o == 1:
            half_send(h, o1, o2, along, 1, 0)
        elif o == 3:
            half_send(h, o1, o2, along, 3, 1)

    def arrive(h, o1, o2):
        half_wait(h, o1, o2)
        if o2 == 0:
            spread(h, o1, o2, 0)
        spread(h, o1, o2, 1)

    def pair_send(a, b):
        p = at(-a, -b, 0)
        copy = pltpu.make_async_remote_copy(
            src_ref=kv.at[p],
            dst_ref=kv.at[p],
            send_sem=send_sem.at[len(started)],
            recv_sem=pair_sem.at[a * 4 + b],
            device_id=partner,
            device_id_type=MESH,
        )
        copy.start()
        started.append(copy)

    def chunk(c, masked, first):
        piece = [kv.at[2 * c], kv.at[2 * c + 1]]
        if masked:
            key_pos = lax.broadcasted_iota(jnp.int32, (2 * rows, rows), 0)
            query_pos = lax.broadcasted_iota(jnp.int32, (2 * rows, rows), 1) + core * rows
            keep = key_pos <= query_pos
        values = [
            jnp.concatenate(
                [
                    jnp.concatenate(
                        [p[head * 128 : head * 128 + 128, 384:640] for p in piece], axis=1
                    ),
                    ones,
                ],
                axis=0,
            )
            for head in range(2)
        ]

        def scores(h):
            lo = (0, 0, 128, 256)[h]
            keys = jnp.concatenate([p[:, lo : lo + 128] for p in piece], axis=0)
            s = jnp.dot(keys, qt[h], preferred_element_type=F32)
            return jnp.where(keep, s, NEG) if masked else s

        ready = scores(0)
        for h in range(4):
            s = ready
            if h < 3:
                ready = scores(h + 1)
            scale = (64**-0.5, 64**-0.5, 128**-0.5, 128**-0.5)[h]
            best = jnp.max(s, axis=0, keepdims=True)
            if not first:
                old = top[h : h + 1, :]
                best = jnp.maximum(best, old)
            p = jnp.exp((s - best) * scale).astype(BF16)
            add = jnp.dot(values[h // 2], p, preferred_element_type=F32)
            if first:
                acc[h] = add
            else:
                acc[h] = acc[h] * jnp.exp((old - best) * scale) + add
            top[h : h + 1, :] = best

    def chunks(offsets):
        code = 0
        for k, (a, b) in enumerate(offsets):
            code += (a * 4 + b) * 16**k

        def body(k, left):
            o = lax.rem(left, 16)
            a = o // 4
            b = lax.rem(o, 4)
            p = lax.rem(z + 4 - a, 4) * 8 + lax.rem(y + 4 - b, 4) * 2 + 1 - core
            pltpu.make_async_copy(kv.at[p], kv.at[p], pair_sem.at[o]).wait()
            c = p // 2

            @pl.when(c < chip)
            def _():
                chunk(c, False, False)

            return left // 16

        lax.fori_loop(0, len(offsets), body, jnp.int32(code))

    def slot_matrices():
        lane = lax.broadcasted_iota(jnp.int32, (64, 2048), 1)
        quarter = (lane // 4) % 4
        oz, oy, ox, oc = (table_ref[k : k + 1, :] for k in range(4))
        expert = (((z + oz) % 4) * 8 + ((y + oy) % 4) * 2 + (core + oc) % 2) * 4 + (tp + ox) % 4
        named = jnp.zeros((64, 2048), F32)
        mixed = jnp.zeros((64, 2048), F32)
        down = lax.broadcasted_iota(jnp.int32, (64, 64), 0)
        across = lax.broadcasted_iota(jnp.int32, (64, 64), 1)

        def column(row):
            return jnp.sum(jnp.where(down == across, row, jnp.zeros_like(row)), axis=1, keepdims=True)

        for k in range(4):
            same = column(ids_ref[k : k + 1, :]) == expert
            named = named + jnp.where(same, 1.0, 0.0)
            mixed = mixed + jnp.where(same, column(mix_ref[k : k + 1, :]), 0.0)
        before = jnp.where(across < down, 1.0, 0.0).astype(BF16)
        rank = jnp.dot(before, named.astype(BF16), preferred_element_type=F32)
        hit = (named > 0.5) & (jnp.abs(rank - (lane % 4).astype(F32)) < 0.5)
        placed = jnp.where(hit, 1.0, 0.0)
        mixed = jnp.where(hit, mixed, 0.0)
        high = mixed.astype(BF16).astype(F32)
        low = mixed - high
        for j in range(4):
            keep = quarter == j
            combine[j * 64 : j * 64 + 64] = jnp.where(keep, high, 0.0).astype(BF16)
            combine[256 + j * 64 : 256 + j * 64 + 64] = jnp.where(keep, low, 0.0).astype(BF16)
        for k in range(8):
            cols = slice(k * 256, k * 256 + 256)
            block = jnp.concatenate(
                [jnp.where(quarter[:, cols] == j, placed[:, cols], 0.0) for j in range(4)], axis=0
            )
            fill[cols] = block.T.astype(BF16)
        a = lax.broadcasted_iota(jnp.int32, (256, 256), 0)
        b = lax.broadcasted_iota(jnp.int32, (256, 256), 1)
        perm[0] = jnp.where(b == ((a // 4) % 16) * 16 + (a // 64) * 4 + a % 4, 1.0, 0.0).astype(BF16)
        perm[1] = jnp.where(a == ((b // 4) % 16) * 16 + (b // 64) * 4 + b % 4, 1.0, 0.0).astype(BF16)

    for h in range(2):
        spread(h, 0, 0, 0)
    pair_send(0, 0)
    for h in range(2):
        spread(h, 0, 0, 1)
    pltpu.make_async_copy(kv.at[sp], kv.at[sp], pair_sem.at[0]).wait()
    chunk(chip, True, True)

    slot_matrices()

    whole = set()
    for kind, items in STEPS:
        if kind == "c":
            chunks(items)
            continue
        for h, o1, o2 in items:
            arrive(h, o1, o2)
            whole.add((h, o1, o2))
            a, b = (o2, o1) if h == 0 else (o1, o2)
            if (0, b, a) in whole and (1, a, b) in whole:
                pair_send(a, b)

    for head in range(2):
        first = acc[2 * head]
        second = acc[2 * head + 1]
        one = first[0:128] / first[128:129]
        two = second[0:128] / second[128:129]
        differ = one - (la_ref, lb_ref)[head][...] * two
        scale = lax.rsqrt(jnp.mean(differ * differ, axis=0, keepdims=True) + EPSILON)
        done = (differ * scale).T * gain_ref[...] * HEAD_SCALE
        heads[:, :, head * 128 : head * 128 + 128] = done.astype(BF16).reshape(4, rows // 4, 128)
    sends = []
    for k in (1, 2, 3):
        to = tp_at[k]
        copy = pltpu.make_async_remote_copy(
            src_ref=heads.at[to],
            dst_ref=back.at[tp],
            send_sem=tp_send.at[k],
            recv_sem=tp_recv.at[k],
            device_id=(sp, to),
            device_id_type=MESH,
        )
        copy.start()
        sends.append(copy)
    back[tp] = heads[tp]
    for load in loads:
        load.wait()
    for k in (1, 2, 3):
        source = tp_at[4 - k]
        pltpu.make_async_copy(back.at[source], back.at[source], tp_recv.at[k]).wait()

    joined = jnp.concatenate(
        [back[p, :, :128] for p in range(4)] + [back[p, :, 128:] for p in range(4)], axis=1
    )

    def project(n, total):
        cols = pl.ds(pl.multiple_of(n * 512, 512), 512)
        part = jnp.dot(joined, wo[:, cols], preferred_element_type=F32)
        rounded = (resid_ref[:, cols].astype(F32) + part).astype(BF16)
        middle[:, cols] = rounded
        wide = rounded.astype(F32)
        return total + jnp.sum(wide * wide, axis=1, keepdims=True)

    total = lax.fori_loop(0, 4, project, jnp.zeros((64, 1), F32), unroll=True)
    scale = lax.rsqrt(total / 2048.0 + EPSILON)
    normed = (middle[...].astype(F32) * scale * norm_ref[...]).astype(BF16)
    stack = jnp.concatenate([normed[:, j * 512 : j * 512 + 512] for j in range(4)], axis=0)

    def move(source, target, sem_out, sem_in, o, other):
        pltpu.make_async_remote_copy(
            src_ref=source,
            dst_ref=target,
            send_sem=sem_out,
            recv_sem=sem_in,
            device_id=device(o, other),
            device_id_type=MESH,
        ).start()

    def direct(way, source, target, lo, hi):
        sign = 1 - 2 * way
        for k in range(lo, hi):
            g = int(k >= 64)
            move(
                source.at[k],
                target.at[k],
                a2a_send.at[way * 2 + g],
                a2a_recv.at[way * 2 + g],
                [sign * v for v in ORDER[k][:3]],
                ORDER[k][3],
            )

    def arrived(way, target, g):
        part = target.at[pl.ds(g * 64, 64 - g)]
        pltpu.make_async_copy(part, part, a2a_recv.at[way * 2 + g]).wait()

    def fill_units(lo, hi):
        for u in range(lo, hi):
            rows_u = jnp.dot(fill[u * 256 : u * 256 + 256], stack, preferred_element_type=F32)
            send[u * 16 : u * 16 + 16] = rows_u.astype(BF16).reshape(16, 16, 512)

    for u in range(8):
        fill_units(u, u + 1)
        if u > 0:
            direct(0, send, recv, u * 16 - 16, u * 16)
    direct(0, send, recv, 112, 127)
    recv[127] = send[127]

    def shared_hidden(n, carry):
        cols = pl.ds(pl.multiple_of(n * 256, 256), 256)
        gate = jnp.dot(normed, sg[:, cols], preferred_element_type=F32)
        up = jnp.dot(normed, su[:, cols], preferred_element_type=F32)
        hs[0:64, cols] = (gate * jax.nn.sigmoid(gate) * up).astype(BF16)
        return carry

    lax.fori_loop(0, 2, shared_hidden, 0)

    def shared_down(n, carry):
        cols = pl.ds(pl.multiple_of(n * 256, 256), 256)
        shared[:, cols] = jnp.dot(hs[0:64, 0:512], sd[:, cols], preferred_element_type=F32)
        return carry

    lax.fori_loop(0, 8, shared_down, 0)

    def expert(g):
        for u in range(4):
            s0 = (g * 4 + u) * 16
            rows_u = jnp.dot(
                perm[0], recv[s0 : s0 + 16].reshape(256, 512), preferred_element_type=F32
            ).astype(BF16)
            for j in range(4):
                xs[u * 64 : u * 64 + 64, j * 512 : j * 512 + 512] = rows_u[j * 64 : j * 64 + 64]

        def hidden(n, carry):
            cols = pl.ds(pl.multiple_of(n * 256, 256), 256)
            gate = jnp.dot(xs[...], wg[:, cols], preferred_element_type=F32)
            up = jnp.dot(xs[...], wu[:, cols], preferred_element_type=F32)
            hs[:, cols] = (gate * jax.nn.sigmoid(gate) * up).astype(BF16)
            return carry

        lax.fori_loop(0, 4, hidden, 0, unroll=4)

        def down(n, carry):
            cols = pl.ds(pl.multiple_of(n * 256, 256), 256)
            rs[:, cols] = jnp.dot(hs[...], wd[:, cols], preferred_element_type=F32).astype(BF16)
            return carry

        lax.fori_loop(0, 8, down, 0, unroll=4)
        for u in range(4):
            s0 = (g * 4 + u) * 16
            block = jnp.concatenate(
                [rs[u * 64 : u * 64 + 64, j * 512 : j * 512 + 512] for j in range(4)], axis=0
            )
            rows_u = jnp.dot(perm[1], block, preferred_element_type=F32)
            res[s0 : s0 + 16] = rows_u.astype(BF16).reshape(16, 16, 512)
            if u > 0:
                direct(1, res, ret, s0 - 16, s0)
        direct(1, res, ret, g * 64 + 48, g * 64 + 64 - g)

    arrived(0, recv, 0)
    expert(0)
    arrived(0, recv, 1)
    expert(1)
    ret[127] = res[127]

    for g in range(2):
        arrived(1, ret, g)
        for half_cols in range(2):
            cols = slice(half_cols * 256, half_cols * 256 + 256)
            part = jnp.dot(
                combine[:, g * 1024 : g * 1024 + 1024],
                ret[g * 64 : g * 64 + 64].reshape(1024, 512)[:, cols],
                preferred_element_type=F32,
            )
            if g == 0:
                routed[:, cols] = part
            else:
                routed[:, cols] = routed[:, cols] + part
    for j in range(4):
        cols = slice(j * 512, j * 512 + 512)
        rows_j = routed[j * 64 : j * 64 + 64] + routed[256 + j * 64 : 256 + j * 64 + 64]
        out_ref[:, cols] = (middle[:, cols].astype(F32) + shared[:, cols] + rows_j).astype(BF16)

    for copy in started + sends:
        copy.wait_send()
    for way, buffer in enumerate((send, res)):
        for g in range(2):
            part = buffer.at[pl.ds(g * 64, 64 - g)]
            pltpu.make_async_copy(part, part, a2a_send.at[way * 2 + g]).wait()


def layer(qkv, lambdas, gain, resid, norm, ids, mix, weights):
    rows = qkv[0].shape[0]
    tokens, width = resid.shape
    table = np.zeros((8, 2048), np.int32)
    table[:4] = np.repeat(np.array(ORDER, np.int32).T, 16, axis=1)
    vmem = pl.BlockSpec(memory_space=pltpu.VMEM)
    slots = pltpu.VMEM((128, 16, 512), BF16)
    return pl.pallas_call(
        layer_kernel,
        out_shape=jax.ShapeDtypeStruct((tokens, width), BF16),
        in_specs=[vmem] * 14 + [pl.BlockSpec(memory_space=pl.ANY)] * 7,
        out_specs=vmem,
        scratch_shapes=[
            pltpu.VMEM((4, 128, rows), BF16),
            pltpu.VMEM((32, rows, 640), BF16),
            pltpu.VMEM((4, rows // 4, 256), BF16),
            pltpu.VMEM((4, rows // 4, 256), BF16),
            pltpu.VMEM((4, 136, rows), F32),
            pltpu.VMEM((8, rows), F32),
        ]
        + [pltpu.VMEM(weights[k].shape, BF16) for k in (0, 1, 2, 3, 4, 5, 6)]
        + [
            pltpu.VMEM((2048, 256), BF16),
            pltpu.VMEM((512, 2048), BF16),
            pltpu.VMEM((2, 256, 256), BF16),
            pltpu.VMEM((tokens, width), BF16),
            pltpu.VMEM((tokens, width), F32),
            slots,
            slots,
            slots,
            slots,
            pltpu.VMEM((256, width), BF16),
            pltpu.VMEM((256, 1024), BF16),
            pltpu.VMEM((256, width), BF16),
            pltpu.VMEM((512, 512), F32),
            pltpu.SemaphoreType.DMA((64,)),
            pltpu.SemaphoreType.DMA((32,)),
            pltpu.SemaphoreType.DMA((16,)),
            pltpu.SemaphoreType.DMA((4,)),
            pltpu.SemaphoreType.DMA((4,)),
            pltpu.SemaphoreType.DMA((7,)),
            pltpu.SemaphoreType.DMA((4,)),
            pltpu.SemaphoreType.DMA((4,)),
        ],
        compiler_params=pltpu.CompilerParams(
            vmem_limit_bytes=63 * 1024 * 1024, collective_id=0, has_side_effects=True
        ),
    )(*qkv, *lambdas, gain, resid, norm, ids, mix, jnp.asarray(table), *weights)


def per_device(
    resid,
    query_a,
    key_a,
    value_a,
    query_b,
    key_b,
    value_b,
    lambda_a,
    lambda_b,
    head_gain,
    out_weight,
    norm_gain,
    expert_ids,
    expert_mix,
    gate_experts,
    up_experts,
    down_experts,
    shared_gate,
    shared_up,
    shared_down,
):
    weights = (
        out_weight,
        gate_experts[0],
        up_experts[0],
        down_experts[0],
        shared_gate,
        shared_up,
        shared_down,
    )
    qkv = [a[:, 0] for a in (query_a, key_a, value_a, query_b, key_b, value_b)]
    return layer(
        qkv,
        (lambda_a[None, :], lambda_b[None, :]),
        head_gain[None, :],
        resid,
        norm_gain[None, :],
        expert_ids.T,
        expert_mix.T,
        weights,
    )


def solution(mesh):
    in_specs = (
        P(("sp", "tp"), None),
        P("sp", "tp", None),
        P("sp", "tp", None),
        P("sp", "tp", None),
        P("sp", "tp", None),
        P("sp", "tp", None),
        P("sp", "tp", None),
        P("tp"),
        P("tp"),
        P(),
        P(),
        P(),
        P(("sp", "tp"), None),
        P(("sp", "tp"), None),
        P(("sp", "tp"), None, None),
        P(("sp", "tp"), None, None),
        P(("sp", "tp"), None, None),
        P(),
        P(),
        P(),
    )
    return jax.shard_map(
        per_device,
        mesh=mesh,
        in_specs=in_specs,
        out_specs=P(("sp", "tp"), None),
        check_vma=False,
    )
```
